256 devices in a mesh: ep: 128 (over z, y, x), tp: 2 (over core).
Axes of the slice: x: 4, y: 4, z: 8, core: 2. Of those that a mesh axis runs over, the one named last changes fastest.
Arguments:
- tokens: bfloat16 [16384, 2048], P('ep'), may hold values from -24 to 24
- cotangent: bfloat16 [16384, 2048], P('ep'), may hold values from -0.625 to 0.625
- routes: int32 [16384, 2], P('ep'), may hold values from 0 to 127, as said below
- router_group: bfloat16 [2048, 4], replicated, may hold values from -0.125 to 0.125
- router_expert: bfloat16 [2048, 128], replicated, may hold values from -0.125 to 0.125
- gate_proj: bfloat16 [128, 2048, 512], P('ep', None, 'tp'), may hold values from -0.125 to 0.125
- up_proj: bfloat16 [128, 2048, 512], P('ep', None, 'tp'), may hold values from -0.125 to 0.125
- down_proj: bfloat16 [128, 512, 2048], P('ep', 'tp'), may hold values from -0.25 to 0.25
Outputs:
- token_grad: bfloat16 [16384, 2048], P('ep', 'tp')
- gate_grad: bfloat16 [128, 2048, 512], P('ep', None, 'tp')
- up_grad: bfloat16 [128, 2048, 512], P('ep', None, 'tp')
- down_grad: bfloat16 [128, 512, 2048], P('ep', 'tp')
- gate_rows: float32 [128, 2048], P('ep')
- up_rows: float32 [128, 2048], P('ep')
- down_rows: float32 [128, 512], P('ep', 'tp')
- router_expert_grad: float32 [2048, 128], P(('ep', 'tp'))
- router_group_grad: float32 [2048, 4], P(('ep', 'tp'))
- router_rows: float32 [2048], P(('ep', 'tp'))
The draws below stay inside these ranges and needn't reach their ends.
Inputs may be any that keep to these rules, and one draw needn't show every extreme that they name: `routes`: the 2 entries of a row are different experts of one group: their quotients by 32 are equal. Among the rows of one device no expert is named more than 4 times, and the experts of one group, the same for all devices, are each named exactly 4 times by the rows of every device.
All inputs are finite; a program needn't handle non-finite values.
Results may differ from the reference program's by a relative error of at most 0.014.
Values may be sent and summed in bfloat16 or wider, within the bound.
No kernel may reach another device: no remote copies, remote signals or barrier semaphores. Data moves between devices by JAX's collectives and lax.ppermute only.
A program may use at most 64 MiB of HBM per device.

```python
import jax
import jax.numpy as jnp
from jax import lax

D = 2048
FF = 512
TOK_DEV = 128
GROUPS = 4
TOP = 2
EXPERTS = 128
GROUP_SIZE = 32
TOKENS = 16384
N_TP = 2


def draw_routes(key, part):
    blocks = TOKENS // TOK_DEV
    half_rows = TOK_DEV // 2
    others_rows = TOK_DEV - half_rows
    favored = jax.random.randint(jax.random.fold_in(key, 11), (), 0, GROUPS)
    group_ids = jnp.arange(GROUPS, dtype=jnp.int32)
    is_favored = group_ids[None, :] == favored
    shares = jax.random.randint(jax.random.fold_in(key, 12), (blocks, GROUPS), 2, 5)
    shares = jnp.where(is_favored, 0, shares)
    base_rows = others_rows * shares // jnp.sum(shares, axis=1, keepdims=True)
    leftover = others_rows - jnp.sum(base_rows, axis=1, keepdims=True)
    other_rank = jnp.cumsum(jnp.where(is_favored, 0, 1), axis=1) - 1
    extra_rows = jnp.where(jnp.logical_and(jnp.logical_not(is_favored), other_rank < leftover), 1, 0)
    counts = base_rows + extra_rows + jnp.where(is_favored, half_rows, 0)
    group_end = jnp.cumsum(counts, axis=1)
    group_start = group_end - counts
    position = jnp.arange(TOK_DEV, dtype=jnp.int32)
    labels = jnp.sum((group_end[:, None, :] <= position[None, :, None]).astype(jnp.int32), axis=2)
    within = position[None, :] - jnp.take_along_axis(group_start, labels, axis=1)
    rotate = jax.random.randint(jax.random.fold_in(key, 13), (blocks, GROUPS), 0, GROUP_SIZE)
    offset = jax.random.randint(jax.random.fold_in(key, 14), (blocks, GROUPS), 0, GROUP_SIZE - 1)
    first_pick = (within + jnp.take_along_axis(rotate, labels, axis=1)) % GROUP_SIZE
    turned = (jnp.take_along_axis(offset, labels, axis=1) + within // GROUP_SIZE) % (GROUP_SIZE - 1)
    second_pick = (first_pick + 1 + turned) % GROUP_SIZE
    chosen = jnp.stack([labels * GROUP_SIZE + first_pick, labels * GROUP_SIZE + second_pick], axis=2)
    block_keys = jax.random.split(jax.random.fold_in(key, 15), blocks)
    shuffles = jax.vmap(lambda subkey: jax.random.permutation(subkey, TOK_DEV))(block_keys)
    chosen = jnp.take_along_axis(chosen, shuffles[:, :, None], axis=1)
    return chosen.reshape(TOKENS, TOP).astype(jnp.int32)


def spiked(values, rng, source, target, blocks, factor):
    def block_of(axis_at):
        return (jnp.arange(values.shape[axis_at]) // (values.shape[axis_at] // blocks)).reshape((-1,) + (1,) * (values.ndim - 1 - axis_at))

    first = jax.random.permutation(rng, blocks)[block_of(target)]
    other_side = (block_of(target) + blocks // 2) % blocks
    return jnp.where((block_of(source) == first) | (block_of(source) == other_side), factor * values, values)


def level_of(key, shape, cuts, low, high):
    def one(dim, shards_of):
        heights = jax.random.uniform(jax.random.fold_in(jax.random.fold_in(key, 6), dim), (shards_of,), jnp.float32, low / len(cuts), high / len(cuts))
        return jnp.repeat(jnp.exp(heights), shape[dim] // shards_of).reshape((-1,) + (1,) * (len(shape) - dim - 1))

    factor_of = one(*cuts[0])
    for cut in cuts[1:]:
        factor_of = factor_of * one(*cut)
    return factor_of


def noise(key, shape, width, most, pieces=(), kind=jnp.bfloat16):
    loudness = level_of(key, shape, pieces, -0.22, 0.18) if pieces else 1.0
    result = jax.random.normal(key, shape, jnp.float32) * width * loudness
    return jnp.minimum(jnp.maximum(result, -most), most).astype(kind)


def heavy_noise(rng, extent, width, reach, pieces, heavy, kind=jnp.bfloat16):
    array = width * jax.random.normal(rng, extent, jnp.float32)
    if pieces:
        array = array * level_of(rng, extent, pieces, -0.22, 0.18)
    return jnp.clip(spiked(array, jax.random.fold_in(rng, 3), *heavy), -reach, reach).astype(kind)


def setup_inputs(seed: int = 0) -> dict:
    keys = jax.random.split(jax.random.key(seed), 9)
    tokens = heavy_noise(keys[0], (TOKENS, D), 1.0, 24.0, ((0, 128),), (0, 1, 128, 5.5))
    cotangent = noise(keys[1], (TOKENS, D), 0.1, 0.625, ((0, 128),))
    routes = draw_routes(jax.random.fold_in(keys[8], 71), 0)
    router_group = noise(keys[3], (D, GROUPS), D ** -0.5, 0.125)
    router_expert = noise(keys[4], (D, EXPERTS), D ** -0.5, 0.125)
    gate_proj = noise(keys[5], (EXPERTS, D, FF), D ** -0.5, 0.125, ((0, 128), (2, 2)))
    up_proj = noise(keys[6], (EXPERTS, D, FF), D ** -0.5, 0.125, ((0, 128), (2, 2)))
    down_proj = noise(keys[7], (EXPERTS, FF, D), FF ** -0.5, 0.25, ((0, 128), (1, 2)))
    return dict(tokens=tokens, cotangent=cotangent, routes=routes, router_group=router_group, router_expert=router_expert, gate_proj=gate_proj, up_proj=up_proj, down_proj=down_proj)


tile_rows = 128


def contract_rows(left_side, right_side):
    return lax.dot_general(left_side, right_side, (((0,), (0,)), ((), ())), preferred_element_type=jnp.float32)


def contract_cols(left_side, right_side):
    return lax.dot_general(left_side, right_side, (((1,), (1,)), ((), ())), preferred_element_type=jnp.float32)


def router_forward(tokens, routes, router_group, router_expert):
    groups = router_group.shape[1]
    experts = router_expert.shape[1]
    group_logits = jnp.dot(tokens, router_group, preferred_element_type=jnp.float32)
    expert_logits = jnp.dot(tokens, router_expert, preferred_element_type=jnp.float32)
    group_exp = jnp.exp(group_logits)
    group_prob = group_exp / jnp.sum(group_exp, axis=1, keepdims=True)
    chosen_group = routes[:, 0] // (experts // groups)
    group_onehot = (chosen_group[:, None] == jnp.arange(groups, dtype=jnp.int32)[None, :]).astype(jnp.float32)
    picked = jnp.sum(group_prob * group_onehot, axis=1)
    chosen_logits = jnp.take_along_axis(expert_logits, routes, axis=1)
    paired_exp = jnp.exp(chosen_logits)
    paired = paired_exp / jnp.sum(paired_exp, axis=1, keepdims=True)
    return group_prob, group_onehot, picked, paired


def router_backward(dweight, routes, group_prob, group_onehot, picked, paired, experts):
    dpicked = jnp.sum(dweight * paired, axis=1)
    dpaired = dweight * picked[:, None]
    dchosen = paired * (dpaired - jnp.sum(paired * dpaired, axis=1, keepdims=True))
    dgroup = ((dpicked * picked)[:, None] * (group_onehot - group_prob)).astype(jnp.bfloat16)
    expert_onehot = (routes[:, :, None] == jnp.arange(experts, dtype=jnp.int32)[None, None, :]).astype(jnp.float32)
    dexpert = jnp.sum(dchosen[:, :, None] * expert_onehot, axis=1).astype(jnp.bfloat16)
    return dgroup, dexpert


def reference(tokens, cotangent, routes, router_group, router_expert, gate_proj, up_proj, down_proj):
    group_prob, group_onehot, picked, paired = router_forward(tokens, routes, router_group, router_expert)
    weights = (picked[:, None] * paired).astype(jnp.bfloat16)
    assigned = TOKENS * TOP
    flat_ids = routes.reshape(assigned).astype(jnp.int32)
    counts = jnp.zeros((EXPERTS,), jnp.int32).at[flat_ids].add(1)
    tile_count = ((counts + (tile_rows - 1)) // tile_rows).astype(jnp.int32)
    tile_end = jnp.cumsum(tile_count).astype(jnp.int32)
    tile_begin = (tile_end - tile_count).astype(jnp.int32)
    count_begin = (jnp.cumsum(counts).astype(jnp.int32) - counts).astype(jnp.int32)
    ordering = jnp.argsort(flat_ids, stable=True).astype(jnp.int32)
    sorted_ids = flat_ids[ordering]
    ranking = jnp.arange(assigned, dtype=jnp.int32) - count_begin[sorted_ids]
    padded_pos = (tile_begin[sorted_ids] * tile_rows + ranking).astype(jnp.int32)
    tile_total = (assigned + tile_rows - 1) // tile_rows + EXPERTS
    owners = jnp.full((tile_total * tile_rows,), assigned, jnp.int32).at[padded_pos].set(ordering)
    tile_marks = jnp.arange(tile_total, dtype=jnp.int32)[:, None]
    tile_expert = jnp.minimum(jnp.sum((tile_end[None, :] <= tile_marks).astype(jnp.int32), axis=1), EXPERTS - 1).astype(jnp.int32)
    flat_weights = weights.reshape(assigned)
    piece_width = FF // N_TP

    def tile_step(totals, tile_index):
        grad_gate, grad_up, grad_down = totals
        expert = tile_expert[tile_index]
        members = lax.dynamic_slice_in_dim(owners, tile_index * tile_rows, tile_rows)
        source_rows = members // TOP
        inputs = jnp.take(tokens, source_rows, axis=0, mode="fill", fill_value=0)
        upstream = jnp.take(cotangent, source_rows, axis=0, mode="fill", fill_value=0)
        slot_scale = jnp.take(flat_weights, members, axis=0, mode="fill", fill_value=0).astype(jnp.float32)
        gate_mat = gate_proj[expert]
        up_mat = up_proj[expert]
        down_mat = down_proj[expert]
        gate_pre = jnp.dot(inputs, gate_mat, preferred_element_type=jnp.float32)
        up_pre = jnp.dot(inputs, up_mat, preferred_element_type=jnp.float32)
        sigmoid_gate = jax.nn.sigmoid(gate_pre)
        hidden = (gate_pre * sigmoid_gate * up_pre).astype(jnp.bfloat16)
        pulled = contract_cols(upstream, down_mat)
        weight_part = jnp.sum(pulled * hidden.astype(jnp.float32), axis=1)
        dhidden = slot_scale[:, None] * pulled
        gate_delta = (dhidden * up_pre * sigmoid_gate * (1.0 + gate_pre * (1.0 - sigmoid_gate))).astype(jnp.bfloat16)
        up_delta = (dhidden * gate_pre * sigmoid_gate).astype(jnp.bfloat16)
        scaled_cot = (slot_scale[:, None] * upstream.astype(jnp.float32)).astype(jnp.bfloat16)
        grad_gate = grad_gate.at[expert].add(contract_rows(inputs, gate_delta))
        grad_up = grad_up.at[expert].add(contract_rows(inputs, up_delta))
        grad_down = grad_down.at[expert].add(contract_rows(hidden, scaled_cot))
        token_total = jnp.zeros((tile_rows, D), jnp.float32)
        for piece_index in range(N_TP):
            first_col = piece_index * piece_width
            last_col = first_col + piece_width
            piece_term = contract_cols(gate_delta[:, first_col:last_col], gate_mat[:, first_col:last_col])
            piece_term = piece_term + contract_cols(up_delta[:, first_col:last_col], up_mat[:, first_col:last_col])
            token_total = token_total + piece_term.astype(jnp.bfloat16).astype(jnp.float32)
        return (grad_gate, grad_up, grad_down), (token_total.astype(jnp.bfloat16), weight_part)

    start_totals = (jnp.zeros((EXPERTS, D, FF), jnp.float32), jnp.zeros((EXPERTS, D, FF), jnp.float32),
                    jnp.zeros((EXPERTS, FF, D), jnp.float32))
    totals, tile_outputs = lax.scan(tile_step, start_totals, jnp.arange(tile_total, dtype=jnp.int32))
    grad_gate, grad_up, grad_down = totals
    token_tiles, weight_tiles = tile_outputs
    position = jnp.zeros((assigned,), jnp.int32).at[ordering].set(padded_pos)
    token_rows = token_tiles.reshape(tile_total * tile_rows, D)[position]
    expert_part = jnp.sum(token_rows.reshape(TOKENS, TOP, D).astype(jnp.float32), axis=1)
    dweight = weight_tiles.reshape(tile_total * tile_rows)[position].astype(jnp.bfloat16).astype(jnp.float32)
    dweight = dweight.reshape(TOKENS, TOP)
    dgroup, dexpert = router_backward(dweight, routes, group_prob, group_onehot, picked, paired, EXPERTS)
    router_part = contract_cols(dgroup, router_group) + contract_cols(dexpert, router_expert)
    token_grad = (expert_part + router_part).astype(jnp.bfloat16)
    router_expert_grad = contract_rows(tokens, dexpert)
    router_group_grad = contract_rows(tokens, dgroup)
    router_rows = jnp.sum(router_expert_grad * router_expert_grad, axis=1) + jnp.sum(router_group_grad * router_group_grad, axis=1)
    gate_rows = jnp.sum(grad_gate * grad_gate, axis=2)
    up_rows = jnp.sum(grad_up * grad_up, axis=2)
    down_rows = jnp.sum(grad_down * grad_down, axis=2)
    return (token_grad, grad_gate.astype(jnp.bfloat16), grad_up.astype(jnp.bfloat16), grad_down.astype(jnp.bfloat16),
            gate_rows, up_rows, down_rows, router_expert_grad, router_group_grad, router_rows)
```

```python
import jax
import jax.numpy as jnp
from jax import lax
from jax.sharding import PartitionSpec as P

BF = jnp.bfloat16
F32 = jnp.float32
GROUP_LANE = 32
U_LANE = 40
LOW_LANE = 64
EXTRA = 128


def mm(a, b):
    return lax.dot_general(a, b, (((1,), (0,)), ((), ())), preferred_element_type=F32)


def nt(a, b):
    return lax.dot_general(a, b, (((1,), (1,)), ((), ())), preferred_element_type=F32)


def tn(a, b):
    return lax.dot_general(a, b, (((0,), (0,)), ((), ())), preferred_element_type=F32)


def iota(shape, dim):
    return lax.broadcasted_iota(jnp.int32, shape, dim)


def slot_hits(rt, experts, slot_of_row):
    tok = rt.shape[1]
    row = iota((experts * 8, tok), 0)
    hit0 = rt[0:1] == (row >> 3)
    hit1 = rt[1:2] == (row >> 3)
    named = jnp.where(hit0 | hit1, 1.0, 0.0).astype(BF)
    before = jnp.where(iota((tok, tok), 0) < iota((tok, tok), 1), 1.0, 0.0).astype(BF)
    rank = mm(named, before)
    match = rank == slot_of_row(row & 7).astype(F32)
    return row & 7, hit0 & match, hit1 & match


def send_tokens_fn(tp, rt, tokens, experts):
    width = tokens.shape[1] // 4
    sub, h0, h1 = slot_hits(rt, experts, lambda s: 2 * tp + (s & 1))
    hit = h0 | h1
    total = None
    for c in range(4):
        sel = jnp.where(hit & ((sub >> 1) == c), 1.0, 0.0).astype(BF)
        term = mm(sel, tokens[:, c * width : (c + 1) * width])
        total = term if total is None else total + term
    return total.astype(BF)


def router_fn(tp, rt, tokens, cot, rgt, rex):
    tok, dm = tokens.shape
    experts = rex.shape[1]
    groups = rgt.shape[0]
    gw = experts // groups
    width = dm // 4
    r0, r1 = rt[0:1], rt[1:2]
    group_exp = jnp.exp(nt(rgt, tokens))
    group_prob = group_exp / jnp.sum(group_exp, axis=0, keepdims=True)
    logits = jnp.transpose(mm(tokens, rex))
    ei = iota((experts, tok), 0)
    l0 = jnp.sum(jnp.where(ei == r0, logits, 0.0), axis=0, keepdims=True)
    l1 = jnp.sum(jnp.where(ei == r1, logits, 0.0), axis=0, keepdims=True)
    x0, x1 = jnp.exp(l0), jnp.exp(l1)
    p0, p1 = x0 / (x0 + x1), x1 / (x0 + x1)
    chosen = r0 // gw
    gi = iota((groups, tok), 0)
    picked = jnp.sum(jnp.where(gi == chosen, group_prob, 0.0), axis=0, keepdims=True)
    w0 = (picked * p0).astype(BF).astype(F32)
    w1 = (picked * p1).astype(BF).astype(F32)
    sub, h0, h1 = slot_hits(rt, experts, lambda s: 2 * tp + (s & 1))
    scale = jnp.where(h0, w0, jnp.where(h1, w1, 0.0))
    total = None
    for c in range(4):
        sel = jnp.where((sub >> 1) == c, scale, 0.0).astype(BF)
        term = mm(sel, cot[:, c * width : (c + 1) * width])
        total = term if total is None else total + term
    li = iota((EXTRA, tok), 0) & (LOW_LANE - 1)
    base = r0 - chosen * gw
    other = r1 - chosen * gw
    diff = jnp.where(li == base, 1.0, 0.0) - jnp.where(li == other, 1.0, 0.0)
    group_side = jnp.where(li == GROUP_LANE + chosen, 1.0, 0.0)
    for j in range(groups):
        group_side = group_side - jnp.where(li == GROUP_LANE + j, group_prob[j : j + 1], 0.0)
    z0 = (p1 * diff + group_side).astype(BF)
    z1 = (group_side - p0 * diff).astype(BF)
    first = (sub >> 1) == 0
    m0 = jnp.where(h0 & first, 1.0, 0.0).astype(BF)
    m1 = jnp.where(h1 & first, 1.0, 0.0).astype(BF)
    side = nt(m0, z0) + nt(m1, z1)
    return total.astype(BF), side.astype(BF), p0, p1, group_prob


def split_rows(got, parts):
    rows, width = got.shape
    src = rows // 8
    slots = 8 // parts
    return got.reshape(src, parts, slots, width).transpose(0, 2, 1, 3).reshape(src * slots, parts * width)


def body(tokens, cotangent, routes, router_group, router_expert, gate_proj, up_proj, down_proj):
    tok, dm = tokens.shape
    experts = router_expert.shape[1]
    groups = router_group.shape[1]
    gw = experts // groups
    width = dm // 4
    half = dm // 2
    tp = lax.axis_index("tp")
    swap = [(0, 1), (1, 0)]
    rt = routes.T
    rgt = router_group.T
    gate, up, down = gate_proj[0], up_proj[0], down_proj[0]

    def exchange(x):
        n = x.shape[1]
        y = lax.all_to_all(x.reshape(experts, 8, n), "ep", split_axis=0, concat_axis=0, tiled=True)
        return y.reshape(experts * 8, n)

    def partner(x):
        return lax.ppermute(x, "tp", swap)

    got_tok = exchange(send_tokens_fn(tp, rt, tokens, experts))
    send_cot, side, p0, p1, group_prob = router_fn(tp, rt, tokens, cotangent, rgt, router_expert)
    got_cot = exchange(jnp.concatenate([send_cot, side], axis=1))
    toks = (got_tok, partner(got_tok))
    cots = (got_cot, partner(got_cot))
    xs, gds, uds, hids, scs, zs, us, terms = [], [], [], [], [], [], [], []
    for part in range(2):
        x = split_rows(toks[part], 4)
        gp, upre = mm(x, gate), mm(x, up)
        sig = jax.nn.sigmoid(gp)
        hid = (gp * sig * upre).astype(BF)
        sc = split_rows(cots[part][:, :width], 4)
        z = cots[part][:, width:].reshape(experts, 8, EXTRA)[:, :2].reshape(experts * 2, EXTRA)
        pulled = nt(sc, down)
        us.append(jnp.sum(pulled * hid.astype(F32), axis=1, keepdims=True))
        gd = (pulled * (upre * sig * (1.0 + gp * (1.0 - sig)))).astype(BF)
        ud = (pulled * (gp * sig)).astype(BF)
        terms.append((nt(gd, gate) + nt(ud, up)).astype(BF))
        xs.append(x), gds.append(gd), uds.append(ud), hids.append(hid), scs.append(sc), zs.append(z)
    mine, theirs = [], []
    lane = iota((experts * 2, EXTRA), 1)
    for part in range(2):
        mine.append(lax.dynamic_slice_in_dim(terms[part], tp * half, half, 1))
        high = us[part].astype(BF)
        low = (us[part] - high.astype(F32)).astype(BF)
        tail = jnp.where(lane == 0, high, jnp.where(lane == 1, low, jnp.zeros_like(high)))
        theirs.append(
            jnp.concatenate([lax.dynamic_slice_in_dim(terms[part], (1 - tp) * half, half, 1), tail], axis=1)
        )
    came = (partner(theirs[1]), partner(theirs[0]))
    rets, ulanes, rc = [], [], None
    for part in range(2):
        rets.append((mine[part].astype(F32) + came[part][:, :half].astype(F32)).astype(BF))
        u = us[part] + came[part][:, half : half + 1].astype(F32) + came[part][:, half + 1 : half + 2].astype(F32)
        ulanes.append(jnp.where(lane == U_LANE, u, 0.0))
        term = tn(xs[part], (u * zs[part].astype(F32)).astype(BF))
        rc = term if rc is None else rc + term
    rc = rc.reshape(experts, 16, EXTRA)
    rc = lax.dynamic_slice_in_dim(rc, tp * 8, 8, 1)
    ret = jnp.stack([r.reshape(experts, 2, 2, half // 2) for r in rets], axis=1)
    ret = ret.transpose(0, 3, 1, 2, 4).reshape(experts, 8, half // 2)
    uu = jnp.concatenate([v.reshape(experts, 2, EXTRA) for v in ulanes], axis=1)
    uu = jnp.pad(uu, ((0, 0), (0, 4), (0, 0)))
    high = rc.astype(BF)
    elane = iota((1, 1, EXTRA), 2)
    extra = (jnp.where(elane < LOW_LANE, high.astype(F32), rc - high.astype(F32)) + uu).astype(BF)
    back = exchange(jnp.concatenate([ret, extra], axis=2).reshape(experts * 8, half // 2 + EXTRA))
    gate_total = tn(xs[0], gds[0]) + tn(xs[1], gds[1])
    up_total = tn(xs[0], uds[0]) + tn(xs[1], uds[1])
    down_total = tn(hids[0], scs[0]) + tn(hids[1], scs[1])
    sq = jnp.stack([jnp.sum(gate_total * gate_total, axis=1), jnp.sum(up_total * up_total, axis=1)])
    sq = sq + partner(sq)
    down_sq = jnp.sum(down_total * down_total, axis=1)
    back_tok, back_extra = back[:, : half // 2], back[:, half // 2 :]
    sub, h0, h1 = slot_hits(rt, experts, lambda s: (2 * tp + (s & 3)) & 3)
    parts = []
    for c in range(2):
        sel = jnp.where((h0 | h1) & ((sub >> 2) == c), 1.0, 0.0).astype(BF)
        parts.append(tn(sel, back_tok))
    expert_part = jnp.concatenate(parts, axis=1)
    first = (sub >> 2) == 0
    u0 = tn(jnp.where(h0 & first, 1.0, 0.0).astype(BF), back_extra)[:, U_LANE : U_LANE + 1]
    u1 = tn(jnp.where(h1 & first, 1.0, 0.0).astype(BF), back_extra)[:, U_LANE : U_LANE + 1]
    lean = p1.T * u0 - p0.T * u1
    total_u = u0 + u1
    own_group = lax.dynamic_slice_in_dim(rgt, tp * half, half, 1)
    own_expert = lax.dynamic_slice_in_dim(router_expert, tp * half, half, 0)
    er = iota((tok, experts), 1)
    dexpert = (jnp.where(er == routes[:, 0:1], lean, 0.0) - jnp.where(er == routes[:, 1:2], lean, 0.0)).astype(BF)
    gr = iota((tok, groups), 1)
    onehot = jnp.where(gr == routes[:, 0:1] // gw, 1.0, 0.0)
    dgroup = (total_u * (onehot - group_prob.T)).astype(BF)
    token_grad = (expert_part + (mm(dgroup, own_group) + nt(dexpert, own_expert))).astype(BF)
    sums = jnp.sum(back_extra.reshape(groups, gw, 8, EXTRA).astype(F32), axis=1)
    sums = sums[:, :, :LOW_LANE] + sums[:, :, LOW_LANE:]
    rex_grad = jnp.concatenate([sums[g, :, :gw] for g in range(groups)], axis=1)
    rg_grad = jnp.sum(sums[:, :, GROUP_LANE : GROUP_LANE + groups], axis=0)
    rows = jnp.sum(rex_grad * rex_grad, axis=1) + jnp.sum(rg_grad * rg_grad, axis=1)
    return (
        token_grad,
        gate_total.astype(BF)[None],
        up_total.astype(BF)[None],
        down_total.astype(BF)[None],
        sq[0:1],
        sq[1:2],
        down_sq[None],
        rex_grad,
        rg_grad,
        rows,
    )


def solution(mesh):
    return jax.shard_map(
        body,
        mesh=mesh,
        in_specs=(
            P("ep", None),
            P("ep", None),
            P("ep", None),
            P(),
            P(),
            P("ep", None, "tp"),
            P("ep", None, "tp"),
            P("ep", "tp", None),
        ),
        out_specs=(
            P("ep", "tp"),
            P("ep", None, "tp"),
            P("ep", None, "tp"),
            P("ep", "tp", None),
            P("ep", None),
            P("ep", None),
            P("ep", "tp"),
            P(("ep", "tp"), None),
            P(("ep", "tp"), None),
            P(("ep", "tp")),
        ),
        check_vma=False,
    )
```

```python
import jax
import jax.numpy as jnp
from jax import lax
from jax.experimental import pallas as pl
from jax.experimental.pallas import tpu as pltpu
from jax.sharding import PartitionSpec as P

BF = jnp.bfloat16
F32 = jnp.float32
GROUP_LANE = 32
U_LANE = 40
LOW_LANE = 64
EXTRA = 128


def mm(a, b):
    return lax.dot_general(a, b, (((1,), (0,)), ((), ())), preferred_element_type=F32)


def nt(a, b):
    return lax.dot_general(a, b, (((1,), (1,)), ((), ())), preferred_element_type=F32)


def tn(a, b):
    return lax.dot_general(a, b, (((0,), (0,)), ((), ())), preferred_element_type=F32)


def iota(shape, dim):
    return lax.broadcasted_iota(jnp.int32, shape, dim)


def call(kernel, name, flops, outs, scalars, arrays):
    smem = pl.BlockSpec(memory_space=pltpu.SMEM)
    vmem = pl.BlockSpec(memory_space=pltpu.VMEM)
    return pl.pallas_call(
        kernel,
        name=name,
        out_shape=[jax.ShapeDtypeStruct(shape, dtype) for shape, dtype in outs],
        in_specs=[smem] * len(scalars) + [vmem] * len(arrays),
        out_specs=[vmem] * len(outs),
        cost_estimate=pl.CostEstimate(flops=flops, bytes_accessed=4 << 20, transcendentals=0),
        compiler_params=pltpu.CompilerParams(vmem_limit_bytes=56 << 20),
    )(*scalars, *arrays)


def ones_where(mask):
    return jnp.where(mask, 1.0, 0.0).astype(BF)


def pre_kernel(tp_ref, rt_ref, tok_ref, cot_ref, rgt_ref, rex_ref, send_ref, aux_ref):
    tp = tp_ref[0]
    tok, dm = tok_ref.shape
    experts = rex_ref.shape[1]
    groups = rgt_ref.shape[0]
    gw = experts // groups
    width = dm // 4
    r0, r1 = rt_ref[0:1, :], rt_ref[1:2, :]
    group_exp = jnp.exp(nt(rgt_ref[...], tok_ref[...]))
    group_prob = group_exp / jnp.sum(group_exp, axis=0, keepdims=True)
    logits = jnp.transpose(mm(tok_ref[...], rex_ref[...]))
    ei = iota((experts, tok), 0)
    l0 = jnp.sum(jnp.where(ei == r0, logits, 0.0), axis=0, keepdims=True)
    l1 = jnp.sum(jnp.where(ei == r1, logits, 0.0), axis=0, keepdims=True)
    x0, x1 = jnp.exp(l0), jnp.exp(l1)
    p0, p1 = x0 / (x0 + x1), x1 / (x0 + x1)
    chosen = r0 // gw
    gi = iota((groups, tok), 0)
    picked = jnp.sum(jnp.where(gi == chosen, group_prob, 0.0), axis=0, keepdims=True)
    w0 = (picked * p0).astype(BF).astype(F32)
    w1 = (picked * p1).astype(BF).astype(F32)
    li = iota((EXTRA, tok), 0) & (LOW_LANE - 1)
    diff = jnp.where(li == r0 - chosen * gw, 1.0, 0.0) - jnp.where(li == r1 - chosen * gw, 1.0, 0.0)
    group_side = jnp.where(li == GROUP_LANE + chosen, 1.0, 0.0)
    for j in range(groups):
        group_side = group_side - jnp.where(li == GROUP_LANE + j, group_prob[j : j + 1, :], 0.0)
    z0 = (p1 * diff + group_side).astype(BF)
    z1 = (group_side - p0 * diff).astype(BF)
    row = iota((EXTRA, tok), 0)
    aux = jnp.where(row == 0, p0, jnp.where(row == 1, p1, 0.0))
    for j in range(groups):
        aux = jnp.where(row == 2 + j, group_prob[j : j + 1, :], aux)
    aux_ref[...] = jnp.transpose(aux)
    before = ones_where(iota((tok, tok), 0) < iota((tok, tok), 1))
    blk = 128

    def step(b, carry):
        sub = iota((blk, tok), 0) & 7
        expert = b * 16 + (iota((blk, tok), 0) >> 3)
        hit0 = r0 == expert
        hit1 = r1 == expert
        rank = mm(ones_where(hit0 | hit1), before)
        match = rank == (2 * tp + (sub & 1)).astype(F32)
        one0 = jnp.where(hit0 & match, 1.0, 0.0)
        one1 = jnp.where(hit1 & match, 1.0, 0.0)
        one = one0 + one1
        scale = one0 * w0 + one1 * w1
        rows = pl.ds(pl.multiple_of(b * blk, blk), blk)
        got_tok, got_cot = None, None
        for c in range(4):
            here = (sub >> 1) == c
            cols = slice(c * width, (c + 1) * width)
            a = mm(jnp.where(here, one, 0.0).astype(BF), tok_ref[:, cols])
            d = mm(jnp.where(here, scale, 0.0).astype(BF), cot_ref[:, cols])
            got_tok = a if c == 0 else got_tok + a
            got_cot = d if c == 0 else got_cot + d
        send_ref[rows, 0:width] = got_tok.astype(BF)
        send_ref[rows, width : 2 * width] = got_cot.astype(BF)
        head = (sub >> 1) == 0
        side = nt(jnp.where(head, one0, 0.0).astype(BF), z0) + nt(jnp.where(head, one1, 0.0).astype(BF), z1)
        send_ref[rows, 2 * width :] = side.astype(BF)
        return carry

    lax.fori_loop(0, experts * 8 // blk, step, 0)


def expert_kernel(
    tp_ref, got_ref, gate_ref, up_ref, down_ref,
    x_ref, sc_ref, z_ref, gd_ref, ud_ref, hid_ref, u_ref, mine_ref, theirs_ref,
):
    tp = tp_ref[0]
    dm = gate_ref.shape[0]
    width, half = dm // 4, dm // 2
    o, i = iota((128, 128), 0), iota((128, 128), 1)
    perm = ones_where(i == ((o & 31) >> 1) * 8 + (o >> 5) * 2 + (o & 1))
    for b in range(got_ref.shape[0] // 128):
        block = slice(b * 128, (b + 1) * 128)
        rows = slice(b * 32, (b + 1) * 32)
        y = mm(perm, got_ref[block, 0 : 2 * width]).astype(BF)
        for c in range(4):
            cols = slice(c * width, (c + 1) * width)
            x_ref[rows, cols] = y[c * 32 : (c + 1) * 32, 0:width]
            sc_ref[rows, cols] = y[c * 32 : (c + 1) * 32, width:]
        z_ref[rows, :] = mm(perm[0:32], got_ref[block, 2 * width :]).astype(BF)
    gp = mm(x_ref[...], gate_ref[...])
    upre = mm(x_ref[...], up_ref[...])
    pulled = nt(sc_ref[...], down_ref[...])
    sig = 1.0 / (1.0 + jnp.exp(-gp))
    act = gp * sig
    hid = (act * upre).astype(BF)
    hid_ref[...] = hid
    u = jnp.sum(pulled * hid.astype(F32), axis=1, keepdims=True)
    gd = (pulled * (upre * sig * (1.0 + gp * (1.0 - sig)))).astype(BF)
    ud = (pulled * act).astype(BF)
    gd_ref[...] = gd
    ud_ref[...] = ud
    n = x_ref.shape[0]
    u_ref[...] = jnp.broadcast_to(u, (n, EXTRA))
    high = u.astype(BF).astype(F32)
    lane = iota((n, EXTRA), 1)
    theirs_ref[:, half:] = jnp.where(lane == 0, high, jnp.where(lane == 1, u - high, 0.0)).astype(BF)
    far = pl.ds(pl.multiple_of((1 - tp) * half, half), half)
    theirs_ref[:, 0:half] = (nt(gd, gate_ref[far, :]) + nt(ud, up_ref[far, :])).astype(BF)
    near = pl.ds(pl.multiple_of(tp * half, half), half)
    mine_ref[...] = (nt(gd, gate_ref[near, :]) + nt(ud, up_ref[near, :])).astype(BF)


def pack_kernel(tp_ref, *refs):
    tp = tp_ref[0]
    mine, came, us, zs, xs = refs[0:2], refs[2:4], refs[4:6], refs[6:8], refs[8:10]
    ret_ref, y0_ref, y1_ref, ul_ref = refs[10:14]
    n, half = mine[0].shape
    width = half // 2
    lane = iota((n, EXTRA), 1)
    for p, y_ref in ((0, y0_ref), (1, y1_ref)):
        u = us[p][...] + came[p][:, half : half + 1].astype(F32) + came[p][:, half + 1 : half + 2].astype(F32)
        y_ref[...] = (u * zs[p][...].astype(F32)).astype(BF)
        ul_ref[p * n : (p + 1) * n, :] = jnp.where(lane == U_LANE, u, 0.0).astype(BF)
    o, i = iota((128, 128), 0), iota((128, 128), 1)
    perm = ones_where(i == ((o >> 2) & 1) * 64 + ((o >> 1) & 1) * 32 + (o >> 3) * 2 + (o & 1))
    wide = iota((128, EXTRA), 1) < LOW_LANE
    for b in range(n // 32):
        rows = slice(b * 32, (b + 1) * 32)
        out = slice(b * 128, (b + 1) * 128)
        sums = [(mine[p][rows, :].astype(F32) + came[p][rows, 0:half].astype(F32)).astype(BF) for p in range(2)]
        stack = jnp.concatenate(
            [sums[0][:, 0:width], sums[1][:, 0:width], sums[0][:, width:], sums[1][:, width:]], axis=0
        )
        ret_ref[out, 0:width] = mm(perm, stack).astype(BF)
        ulane = jnp.concatenate([ul_ref[rows, :], ul_ref[n + b * 32 : n + (b + 1) * 32, :]], axis=0)
        base = mm(perm[:, 0:64], ulane)
        pieces = []
        for h in range(2):
            cols = slice(b * 256 + h * 128, b * 256 + (h + 1) * 128)
            rc = tn(xs[0][:, cols], y0_ref[...]) + tn(xs[1][:, cols], y1_ref[...])
            rc = rc.reshape(8, 16, EXTRA)
            pieces.append(jnp.where(tp == 0, rc[:, 0:8, :], rc[:, 8:16, :]).reshape(64, EXTRA))
        rc = jnp.concatenate(pieces, axis=0)
        high = rc.astype(BF).astype(F32)
        ret_ref[out, width:] = (base + jnp.where(wide, high, rc - high)).astype(BF)


def home_kernel(tp_ref, routes_ref, aux_ref, rg_ref, rex_ref, sel_ref, q_ref, h_ref):
    tp = tp_ref[0]
    tok = routes_ref.shape[0]
    half = q_ref.shape[1]
    groups = rg_ref.shape[0]
    experts = rex_ref.shape[1]
    gw = experts // groups
    r0, r1 = routes_ref[:, 0:1], routes_ref[:, 1:2]
    n = experts * 8
    col = iota((tok, n), 1)
    hit0 = r0 == (col >> 3)
    hit1 = r1 == (col >> 3)
    earlier = ones_where(iota((tok, tok), 1) < iota((tok, tok), 0))
    rank = mm(earlier, ones_where(hit0 | hit1))
    match = rank == ((2 * tp + (col & 3)) & 3).astype(F32)
    lower = (col & 4) == 0
    one0 = jnp.where(hit0 & match, 1.0, 0.0)
    one1 = jnp.where(hit1 & match, 1.0, 0.0)
    sel_ref[0] = jnp.where(lower, one0, 0.0).astype(BF)
    sel_ref[1] = jnp.where(lower, one1, 0.0).astype(BF)
    sel_ref[2] = jnp.where(lower, one0 + one1, 0.0).astype(BF)
    sel_ref[3] = jnp.where(lower, 0.0, one0 + one1).astype(BF)
    ei = iota((tok, experts), 1)
    pick = (jnp.where(ei == r0, 1.0, 0.0) - jnp.where(ei == r1, 1.0, 0.0)).astype(BF)
    near = pl.ds(pl.multiple_of(tp * half, half), half)
    q_ref[...] = nt(pick, rex_ref[near, :])
    h = None
    for j in range(groups):
        side = jnp.where(r0 // gw == j, 1.0, 0.0) - aux_ref[:, 2 + j : 3 + j]
        term = side * rg_ref[pl.ds(j, 1), near].astype(F32)
        h = term if j == 0 else h + term
    h_ref[...] = h


def final_kernel(back_ref, sel_ref, aux_ref, q_ref, h_ref, tg_ref, rex_ref, rg_ref, rows_ref):
    width = back_ref.shape[1] - EXTRA
    experts = rex_ref.shape[1]
    groups = rg_ref.shape[1]
    gw = experts // groups
    extra = back_ref[:, width:]
    u0 = mm(sel_ref[0], extra)[:, U_LANE : U_LANE + 1]
    u1 = mm(sel_ref[1], extra)[:, U_LANE : U_LANE + 1]
    lean = aux_ref[:, 1:2] * u0 - aux_ref[:, 0:1] * u1
    both = u0 + u1
    for c in range(2):
        cols = slice(c * width, (c + 1) * width)
        part = mm(sel_ref[2 + c], back_ref[:, 0:width])
        tg_ref[:, cols] = (part + (both * h_ref[:, cols] + lean * q_ref[:, cols])).astype(BF)
    sums = jnp.sum(extra.astype(F32).reshape(groups, gw, 8, EXTRA), axis=1)
    rg = None
    square = None
    for g in range(groups):
        s = sums[g]
        rex = s[:, 0:gw] + s[:, LOW_LANE : LOW_LANE + gw]
        grp = s[:, GROUP_LANE : GROUP_LANE + groups] + s[:, LOW_LANE + GROUP_LANE : LOW_LANE + GROUP_LANE + groups]
        rex_ref[:, g * gw : (g + 1) * gw] = rex
        rg = grp if g == 0 else rg + grp
        sq = jnp.sum(rex * rex, axis=1, keepdims=True)
        square = sq if g == 0 else square + sq
    rg_ref[...] = rg
    rows_ref[...] = square + jnp.sum(rg * rg, axis=1, keepdims=True)


def body(tokens, cotangent, routes, router_group, router_expert, gate_proj, up_proj, down_proj):
    tok, dm = tokens.shape
    experts = router_expert.shape[1]
    groups = router_group.shape[1]
    width, half = dm // 4, dm // 2
    ff = gate_proj.shape[2]
    n = experts * 2
    tp = lax.axis_index("tp").reshape(1)
    swap = [(0, 1), (1, 0)]
    rgt = router_group.T
    gate, up, down = gate_proj[0], up_proj[0], down_proj[0]

    def exchange(x):
        m = x.shape[1]
        y = lax.all_to_all(x.reshape(experts, 8, m), "ep", split_axis=0, concat_axis=0, tiled=True)
        return y.reshape(experts * 8, m)

    def partner(x):
        return lax.ppermute(x, "tp", swap)

    send, aux = call(
        pre_kernel, "pre", 1 << 30,
        [((experts * 8, 2 * width + EXTRA), BF), ((tok, EXTRA), F32)],
        [tp], [routes.T, tokens, cotangent, rgt, router_expert],
    )
    got = exchange(send)
    other = partner(got)
    x, sc, z, gd, ud, hid, u, mine, theirs = [list(v) for v in zip(*[
        call(
            expert_kernel, "expert", 3 << 30,
            [((n, dm), BF), ((n, dm), BF), ((n, EXTRA), BF), ((n, ff), BF), ((n, ff), BF), ((n, ff), BF),
             ((n, EXTRA), F32), ((n, half), BF), ((n, half + EXTRA), BF)],
            [tp], [g, gate, up, down],
        )
        for g in (got, other)
    ])]
    came = [partner(theirs[1]), partner(theirs[0])]
    ret = call_pack(tp, mine, came, u, z, x, experts, width)
    back = exchange(ret)
    sel, q, h = call(
        home_kernel, "home", 1 << 29,
        [((4, tok, experts * 8), BF), ((tok, half), F32), ((tok, half), F32)],
        [tp], [routes, aux, rgt, router_expert],
    )
    gate_total = tn(x[0], gd[0]) + tn(x[1], gd[1])
    up_total = tn(x[0], ud[0]) + tn(x[1], ud[1])
    down_total = tn(hid[0], sc[0]) + tn(hid[1], sc[1])
    sq = jnp.stack([jnp.sum(gate_total * gate_total, axis=1), jnp.sum(up_total * up_total, axis=1)])
    sq = sq + partner(sq)
    down_sq = jnp.sum(down_total * down_total, axis=1)
    token_grad, rex_grad, rg_grad, rows = call(
        final_kernel, "final", 1 << 29,
        [((tok, half), BF), ((8, experts), F32), ((8, groups), F32), ((8, 1), F32)],
        [], [back, sel, aux, q, h],
    )
    return (
        token_grad,
        gate_total.astype(BF)[None],
        up_total.astype(BF)[None],
        down_total.astype(BF)[None],
        sq[0:1],
        sq[1:2],
        down_sq[None],
        rex_grad,
        rg_grad,
        rows[:, 0],
    )


def call_pack(tp, mine, came, u, z, x, experts, width):
    n = mine[0].shape[0]
    vmem = pl.BlockSpec(memory_space=pltpu.VMEM)
    return pl.pallas_call(
        pack_kernel,
        name="pack",
        out_shape=jax.ShapeDtypeStruct((experts * 8, width + EXTRA), BF),
        in_specs=[pl.BlockSpec(memory_space=pltpu.SMEM)] + [vmem] * 10,
        out_specs=vmem,
        scratch_shapes=[pltpu.VMEM((n, EXTRA), BF), pltpu.VMEM((n, EXTRA), BF), pltpu.VMEM((2 * n, EXTRA), BF)],
        cost_estimate=pl.CostEstimate(flops=1 << 29, bytes_accessed=4 << 20, transcendentals=0),
        compiler_params=pltpu.CompilerParams(vmem_limit_bytes=56 << 20),
    )(tp, *mine, *came, *u, *z, *x)


def solution(mesh):
    return jax.shard_map(
        body,
        mesh=mesh,
        in_specs=(
            P("ep", None),
            P("ep", None),
            P("ep", None),
            P(),
            P(),
            P("ep", None, "tp"),
            P("ep", None, "tp"),
            P("ep", "tp", None),
        ),
        out_specs=(
            P("ep", "tp"),
            P("ep", None, "tp"),
            P("ep", None, "tp"),
            P("ep", "tp", None),
            P("ep", None),
            P("ep", None),
            P("ep", "tp"),
            P(("ep", "tp"), None),
            P(("ep", "tp"), None),
            P(("ep", "tp")),
        ),
        check_vma=False,
    )
```

```python
import jax
import jax.numpy as jnp
from jax import lax
from jax.experimental import pallas as pl
from jax.experimental.pallas import tpu as pltpu
from jax.sharding import PartitionSpec as P

BF = jnp.bfloat16
F32 = jnp.float32
GROUP_LANE = 32
U_LANE = 40
LOW_LANE = 64
EXTRA = 128


def mm(a, b):
    return lax.dot_general(a, b, (((1,), (0,)), ((), ())), preferred_element_type=F32)


def nt(a, b):
    return lax.dot_general(a, b, (((1,), (1,)), ((), ())), preferred_element_type=F32)


def tn(a, b):
    return lax.dot_general(a, b, (((0,), (0,)), ((), ())), preferred_element_type=F32)


def iota(shape, dim):
    return lax.broadcasted_iota(jnp.int32, shape, dim)


def call(kernel, name, flops, limit, outs, scalars, arrays, scratch=(), spaces=None):
    smem = pl.BlockSpec(memory_space=pltpu.SMEM)
    vmem = pl.BlockSpec(memory_space=pltpu.VMEM)
    return pl.pallas_call(
        kernel,
        name=name,
        out_shape=[jax.ShapeDtypeStruct(shape, dtype) for shape, dtype in outs],
        in_specs=[smem] * len(scalars) + (spaces or [vmem] * len(arrays)),
        out_specs=[vmem] * len(outs),
        scratch_shapes=list(scratch),
        cost_estimate=pl.CostEstimate(flops=flops, bytes_accessed=4 << 20, transcendentals=0),
        compiler_params=pltpu.CompilerParams(vmem_limit_bytes=limit << 20),
    )(*scalars, *arrays)


def ones_where(mask):
    return jnp.where(mask, 1.0, 0.0).astype(BF)


def pre_kernel(
    tp_ref, rt_ref, rgt_ref, tok_hbm, cot_hbm, rex_hbm,
    send_ref, aux_ref, tok_ref, cot_ref, rex_ref, one_ref, sems,
):
    tp = tp_ref[0]
    tok, dm = tok_ref.shape
    experts = rex_ref.shape[1]
    groups = rgt_ref.shape[0]
    gw = experts // groups
    width = dm // 4
    loads = [
        pltpu.make_async_copy(src, dst, sems.at[k])
        for k, (src, dst) in enumerate(((tok_hbm, tok_ref), (rex_hbm, rex_ref), (cot_hbm, cot_ref)))
    ]
    for load in loads:
        load.start()
    r0, r1 = rt_ref[0:1, :], rt_ref[1:2, :]
    before = ones_where(iota((tok, tok), 0) < iota((tok, tok), 1))
    blk = min(256, experts * 8)
    blocks = experts * 8 // blk
    row = iota((blk, tok), 0)
    sub = row & 7
    want = (2 * tp + (sub & 1)).astype(F32)
    part = sub >> 1
    for b in range(blocks):
        rows = slice(b * blk, (b + 1) * blk)
        expert = b * (blk // 8) + (row >> 3)
        hit0 = r0 == expert
        hit1 = r1 == expert
        match = mm(ones_where(hit0 | hit1), before) == want
        one_ref[0, rows, :] = ones_where(hit0 & match)
        one_ref[1, rows, :] = ones_where(hit1 & match)

    def spread(sel):
        return jnp.concatenate([jnp.where(part == c, sel, 0.0).astype(BF) for c in range(4)], axis=1)

    def stacked(ref):
        return jnp.concatenate([ref[:, c * width : (c + 1) * width] for c in range(4)], axis=0)

    loads[0].wait()
    stack = stacked(tok_ref)
    for b in range(blocks):
        rows = slice(b * blk, (b + 1) * blk)
        one = one_ref[0, rows, :].astype(F32) + one_ref[1, rows, :].astype(F32)
        send_ref[rows, 0:width] = mm(spread(one), stack).astype(BF)
    loads[1].wait()
    group_exp = jnp.exp(nt(rgt_ref[...], tok_ref[...]))
    group_prob = group_exp / jnp.sum(group_exp, axis=0, keepdims=True)
    logits = jnp.transpose(mm(tok_ref[...], rex_ref[...]))
    ei = iota((experts, tok), 0)
    l0 = jnp.sum(jnp.where(ei == r0, logits, 0.0), axis=0, keepdims=True)
    l1 = jnp.sum(jnp.where(ei == r1, logits, 0.0), axis=0, keepdims=True)
    x0, x1 = jnp.exp(l0), jnp.exp(l1)
    p0, p1 = x0 / (x0 + x1), x1 / (x0 + x1)
    chosen = r0 // gw
    gi = iota((groups, tok), 0)
    picked = jnp.sum(jnp.where(gi == chosen, group_prob, 0.0), axis=0, keepdims=True)
    w0 = (picked * p0).astype(BF).astype(F32)
    w1 = (picked * p1).astype(BF).astype(F32)
    li = iota((EXTRA, tok), 0) & (LOW_LANE - 1)
    diff = jnp.where(li == r0 - chosen * gw, 1.0, 0.0) - jnp.where(li == r1 - chosen * gw, 1.0, 0.0)
    group_side = jnp.where(li == GROUP_LANE + chosen, 1.0, 0.0)
    for j in range(groups):
        group_side = group_side - jnp.where(li == GROUP_LANE + j, group_prob[j : j + 1, :], 0.0)
    side_t = jnp.concatenate([(p1 * diff + group_side).astype(BF), (group_side - p0 * diff).astype(BF)], axis=1)
    arow = iota((EXTRA, tok), 0)
    aux = jnp.where(arow == 0, p0, jnp.where(arow == 1, p1, 0.0))
    for j in range(groups):
        aux = jnp.where(arow == 2 + j, group_prob[j : j + 1, :], aux)
    aux = jnp.where(arow == 6, r0.astype(F32), jnp.where(arow == 7, r1.astype(F32), aux))
    aux_ref[...] = jnp.transpose(aux)
    loads[2].wait()
    stack = stacked(cot_ref)
    for b in range(blocks):
        rows = slice(b * blk, (b + 1) * blk)
        one0, one1 = one_ref[0, rows, :].astype(F32), one_ref[1, rows, :].astype(F32)
        send_ref[rows, width : 2 * width] = mm(spread(one0 * w0 + one1 * w1), stack).astype(BF)
        head = part == 0
        both = jnp.concatenate(
            [jnp.where(head, one0, 0.0).astype(BF), jnp.where(head, one1, 0.0).astype(BF)], axis=1
        )
        send_ref[rows, 2 * width :] = nt(both, side_t).astype(BF)


def expert_kernel(
    tp_ref, got_ref, gate_ref, up_ref, down_ref,
    x_ref, sc_ref, z_ref, gd_ref, ud_ref, hid_ref, u_ref, mine_ref, theirs_ref,
):
    tp = tp_ref[0]
    dm = gate_ref.shape[0]
    width, half = dm // 4, dm // 2
    blk = min(256, got_ref.shape[0])
    n4 = blk // 4
    shift = n4.bit_length() - 1
    o, i = iota((blk, blk), 0), iota((blk, blk), 1)
    perm = ones_where(i == ((o & (n4 - 1)) >> 1) * 8 + (o >> shift) * 2 + (o & 1))
    for b in range(got_ref.shape[0] // blk):
        block = slice(b * blk, (b + 1) * blk)
        rows = slice(b * n4, (b + 1) * n4)
        y = mm(perm, got_ref[block, 0 : 2 * width]).astype(BF)
        for c in range(4):
            cols = slice(c * width, (c + 1) * width)
            x_ref[rows, cols] = y[c * n4 : (c + 1) * n4, 0:width]
            sc_ref[rows, cols] = y[c * n4 : (c + 1) * n4, width:]
        z_ref[rows, :] = mm(perm[0:n4], got_ref[block, 2 * width :]).astype(BF)
    gp = mm(x_ref[...], gate_ref[...])
    upre = mm(x_ref[...], up_ref[...])
    pulled = nt(sc_ref[...], down_ref[...])
    sig = 1.0 / (1.0 + jnp.exp(-gp))
    act = gp * sig
    hid = (act * upre).astype(BF)
    hid_ref[...] = hid
    u = jnp.sum(pulled * hid.astype(F32), axis=1, keepdims=True)
    gd = (pulled * (upre * sig * (1.0 + gp * (1.0 - sig)))).astype(BF)
    ud = (pulled * act).astype(BF)
    gd_ref[...] = gd
    ud_ref[...] = ud
    n = x_ref.shape[0]
    u_ref[...] = jnp.broadcast_to(u, (n, EXTRA))
    high = u.astype(BF).astype(F32)
    lane = iota((n, EXTRA), 1)
    theirs_ref[:, half:] = jnp.where(lane == 0, high, jnp.where(lane == 1, u - high, 0.0)).astype(BF)
    far = pl.ds(pl.multiple_of((1 - tp) * half, half), half)
    theirs_ref[:, 0:half] = (nt(gd, gate_ref[far, :]) + nt(ud, up_ref[far, :])).astype(BF)
    near = pl.ds(pl.multiple_of(tp * half, half), half)
    mine_ref[...] = (nt(gd, gate_ref[near, :]) + nt(ud, up_ref[near, :])).astype(BF)


def pack_kernel(tp_ref, *refs):
    tp = tp_ref[0]
    mine, came, us, zs, xs = refs[0:2], refs[2:4], refs[4:6], refs[6:8], refs[8:10]
    ret_ref, y0_ref, y1_ref, ul_ref = refs[10:14]
    n, half = mine[0].shape
    width = half // 2
    lane = iota((n, EXTRA), 1)
    for p, y_ref in ((0, y0_ref), (1, y1_ref)):
        u = us[p][...] + came[p][:, half : half + 1].astype(F32) + came[p][:, half + 1 : half + 2].astype(F32)
        y_ref[...] = (u * zs[p][...].astype(F32)).astype(BF)
        ul_ref[p * n : (p + 1) * n, :] = jnp.where(lane == U_LANE, u, 0.0).astype(BF)
    blk = min(256, n * 4)
    bs = blk // 8
    o, i = iota((blk, blk), 0), iota((blk, blk), 1)
    perm = ones_where(i == ((o >> 2) & 1) * (4 * bs) + ((o >> 1) & 1) * (2 * bs) + (o >> 3) * 2 + (o & 1))
    wide = iota((blk, EXTRA), 1) < LOW_LANE
    for b in range(n // (2 * bs)):
        rows = slice(b * 2 * bs, (b + 1) * 2 * bs)
        out = slice(b * blk, (b + 1) * blk)
        sums = [(mine[p][rows, :].astype(F32) + came[p][rows, 0:half].astype(F32)).astype(BF) for p in range(2)]
        stack = jnp.concatenate(
            [sums[0][:, 0:width], sums[1][:, 0:width], sums[0][:, width:], sums[1][:, width:]], axis=0
        )
        ret_ref[out, 0:width] = mm(perm, stack).astype(BF)
        ulane = jnp.concatenate([ul_ref[rows, :], ul_ref[n + b * 2 * bs : n + (b + 1) * 2 * bs, :]], axis=0)
        base = mm(perm[:, 0 : 4 * bs], ulane)
        cols = slice(b * 16 * bs, (b + 1) * 16 * bs)
        rc = tn(xs[0][:, cols], y0_ref[...]) + tn(xs[1][:, cols], y1_ref[...])
        rc = rc.reshape(bs, 16, EXTRA)
        rc = jnp.where(tp == 0, rc[:, 0:8, :], rc[:, 8:16, :]).reshape(blk, EXTRA)
        high = rc.astype(BF).astype(F32)
        ret_ref[out, width:] = (base + jnp.where(wide, high, rc - high)).astype(BF)


def grads_kernel(*refs):
    x, sc, gd, ud, hid = (refs[2 * k : 2 * k + 2] for k in range(5))
    gate_ref, up_ref, down_ref, sq_ref, down_sq_ref, acc_ref = refs[10:]
    dm, ff = gate_ref.shape
    blk = 128
    wide = 512 if dm % 512 == 0 else 128

    def as_row(col):
        return jnp.transpose(jnp.broadcast_to(col, (col.shape[0], 128)))[0:1, :]

    def step(b, carry):
        cols = pl.ds(pl.multiple_of(b * blk, blk), blk)
        for k, (delta, out_ref) in enumerate(((gd, gate_ref), (ud, up_ref))):
            full = tn(x[0][:, cols], delta[0][...]) + tn(x[1][:, cols], delta[1][...])
            out_ref[cols, :] = full.astype(BF)
            sq_ref[k : k + 1, cols] = as_row(jnp.sum(full * full, axis=1, keepdims=True))
        return carry

    lax.fori_loop(0, dm // blk, step, 0)
    acc_ref[...] = jnp.zeros_like(acc_ref)

    def down_step(b, carry):
        cols = pl.ds(pl.multiple_of(b * wide, wide), wide)
        full = tn(hid[0][...], sc[0][:, cols]) + tn(hid[1][...], sc[1][:, cols])
        down_ref[:, cols] = full.astype(BF)
        acc_ref[...] += jnp.broadcast_to(jnp.sum(full * full, axis=1, keepdims=True), acc_ref.shape)
        return carry

    lax.fori_loop(0, dm // wide, down_step, 0)
    down_sq_ref[...] = jnp.transpose(acc_ref[...])[0:1, :]


def home_kernel(tp_ref, aux_ref, rg_ref, rex_ref, sel_ref, q_ref, h_ref):
    tp = tp_ref[0]
    tok = aux_ref.shape[0]
    half = q_ref.shape[1]
    groups = rg_ref.shape[0]
    experts = rex_ref.shape[1]
    gw = experts // groups
    r0, r1 = aux_ref[:, 6:7].astype(jnp.int32), aux_ref[:, 7:8].astype(jnp.int32)
    n = experts * 8
    col = iota((tok, n), 1)
    hit0 = r0 == (col >> 3)
    hit1 = r1 == (col >> 3)
    earlier = ones_where(iota((tok, tok), 1) < iota((tok, tok), 0))
    rank = mm(earlier, ones_where(hit0 | hit1))
    match = rank == ((2 * tp + (col & 3)) & 3).astype(F32)
    lower = (col & 4) == 0
    one0 = jnp.where(hit0 & match, 1.0, 0.0)
    one1 = jnp.where(hit1 & match, 1.0, 0.0)
    sel_ref[0] = jnp.where(lower, one0, 0.0).astype(BF)
    sel_ref[1] = jnp.where(lower, one1, 0.0).astype(BF)
    sel_ref[2] = jnp.where(lower, one0 + one1, 0.0).astype(BF)
    sel_ref[3] = jnp.where(lower, 0.0, one0 + one1).astype(BF)
    ei = iota((tok, experts), 1)
    pick = (jnp.where(ei == r0, 1.0, 0.0) - jnp.where(ei == r1, 1.0, 0.0)).astype(BF)
    near = pl.ds(pl.multiple_of(tp * half, half), half)
    q_ref[...] = nt(pick, rex_ref[near, :])
    h = None
    for j in range(groups):
        side = jnp.where(r0 // gw == j, 1.0, 0.0) - aux_ref[:, 2 + j : 3 + j]
        term = side * rg_ref[pl.ds(j, 1), near].astype(F32)
        h = term if j == 0 else h + term
    h_ref[...] = h


def final_kernel(
    back_ref, sel_ref, aux_ref, q_ref, h_ref, sq_ref, sqo_ref,
    tg_ref, rex_ref, rg_ref, rows_ref, gate_sq_ref, up_sq_ref,
):
    gate_sq_ref[...] = sq_ref[0:1, :] + sqo_ref[0:1, :]
    up_sq_ref[...] = sq_ref[1:2, :] + sqo_ref[1:2, :]
    width = back_ref.shape[1] - EXTRA
    experts = rex_ref.shape[1]
    groups = rg_ref.shape[0]
    gw = experts // groups
    extra = back_ref[:, width:]
    u0 = mm(sel_ref[0], extra)[:, U_LANE : U_LANE + 1]
    u1 = mm(sel_ref[1], extra)[:, U_LANE : U_LANE + 1]
    lean = aux_ref[:, 1:2] * u0 - aux_ref[:, 0:1] * u1
    both = u0 + u1
    for c in range(2):
        cols = slice(c * width, (c + 1) * width)
        part = mm(sel_ref[2 + c], back_ref[:, 0:width])
        tg_ref[:, cols] = (part + (both * h_ref[:, cols] + lean * q_ref[:, cols])).astype(BF)
    sums = jnp.sum(extra.astype(F32).reshape(groups, gw, 8, EXTRA), axis=1)
    rg = None
    square = None
    lane = iota((8, EXTRA), 1)
    for g in range(groups):
        s = sums[g]
        s = s + jnp.concatenate([s[:, LOW_LANE:], s[:, 0:LOW_LANE]], axis=1)
        rex = s[:, 0:gw]
        rex_ref[:, g * gw : (g + 1) * gw] = rex
        rg = s if g == 0 else rg + s
        sq = jnp.sum(rex * rex, axis=1, keepdims=True)
        square = sq if g == 0 else square + sq
    grp = rg[:, GROUP_LANE : GROUP_LANE + groups]
    square = square + jnp.sum(grp * grp, axis=1, keepdims=True)
    rest = jnp.transpose(jnp.where(lane == GROUP_LANE + groups, square, rg))
    rg_ref[...] = rest[GROUP_LANE : GROUP_LANE + groups, :]
    rows_ref[...] = rest[GROUP_LANE + groups : GROUP_LANE + groups + 1, :]


def body(tokens, cotangent, routes, router_group, router_expert, gate_proj, up_proj, down_proj):
    tok, dm = tokens.shape
    experts = router_expert.shape[1]
    groups = router_group.shape[1]
    width, half = dm // 4, dm // 2
    ff = gate_proj.shape[2]
    n = experts * 2
    tp = lax.axis_index("tp").reshape(1)
    swap = [(0, 1), (1, 0)]
    rgt = router_group.T
    gate, up, down = gate_proj[0], up_proj[0], down_proj[0]

    def exchange(x):
        m = x.shape[1]
        y = lax.all_to_all(x.reshape(experts, 8, m), "ep", split_axis=0, concat_axis=0, tiled=True)
        return y.reshape(experts * 8, m)

    def partner(x):
        return lax.ppermute(x, "tp", swap)

    send, aux = call(
        pre_kernel, "pre", 1 << 30, 20,
        [((experts * 8, 2 * width + EXTRA), BF), ((tok, EXTRA), F32)],
        [tp], [routes.T, rgt, tokens, cotangent, router_expert],
        scratch=[
            pltpu.VMEM((tok, dm), BF), pltpu.VMEM((tok, dm), BF), pltpu.VMEM((dm, experts), BF),
            pltpu.VMEM((2, experts * 8, tok), BF), pltpu.SemaphoreType.DMA((3,)),
        ],
        spaces=[pl.BlockSpec(memory_space=pltpu.VMEM)] * 2 + [pl.BlockSpec(memory_space=pl.ANY)] * 3,
    )
    got = exchange(send)
    other = partner(got)
    x, sc, z, gd, ud, hid, u, mine, theirs = [list(v) for v in zip(*[
        call(
            expert_kernel, "expert", 3 << 30, 18,
            [((n, dm), BF), ((n, dm), BF), ((n, EXTRA), BF), ((n, ff), BF), ((n, ff), BF), ((n, ff), BF),
             ((n, EXTRA), F32), ((n, half), BF), ((n, half + EXTRA), BF)],
            [tp], [g, gate, up, down],
        )
        for g in (got, other)
    ])]
    came = [partner(theirs[1]), partner(theirs[0])]
    ret = call_pack(tp, mine, came, u, z, x, experts, width)
    back = exchange(ret)
    sel, q, h = call(
        home_kernel, "home", 1 << 29, 8,
        [((4, tok, experts * 8), BF), ((tok, half), F32), ((tok, half), F32)],
        [tp], [aux, rgt, router_expert],
    )
    gate_grad, up_grad, down_grad, sq, down_sq = call(
        grads_kernel, "grads", 3 << 30, 20,
        [((dm, ff), BF), ((dm, ff), BF), ((ff, dm), BF), ((2, dm), F32), ((1, ff), F32)],
        [], [*x, *sc, *gd, *ud, *hid], scratch=[pltpu.VMEM((ff, 128), F32)],
    )
    sq_other = partner(sq)
    token_grad, rex_grad, rg_grad, rows, gate_sq, up_sq = call(
        final_kernel, "final", 1 << 29, 10,
        [((tok, half), BF), ((8, experts), F32), ((groups, 8), F32), ((1, 8), F32),
         ((1, dm), F32), ((1, dm), F32)],
        [], [back, sel, aux, q, h, sq, sq_other],
    )
    return (
        token_grad,
        gate_grad[None],
        up_grad[None],
        down_grad[None],
        gate_sq,
        up_sq,
        down_sq,
        rex_grad,
        rg_grad.T,
        rows[0],
    )


def call_pack(tp, mine, came, u, z, x, experts, width):
    n = mine[0].shape[0]
    vmem = pl.BlockSpec(memory_space=pltpu.VMEM)
    return pl.pallas_call(
        pack_kernel,
        name="pack",
        out_shape=jax.ShapeDtypeStruct((experts * 8, width + EXTRA), BF),
        in_specs=[pl.BlockSpec(memory_space=pltpu.SMEM)] + [vmem] * 10,
        out_specs=vmem,
        scratch_shapes=[pltpu.VMEM((n, EXTRA), BF), pltpu.VMEM((n, EXTRA), BF), pltpu.VMEM((2 * n, EXTRA), BF)],
        cost_estimate=pl.CostEstimate(flops=1 << 29, bytes_accessed=4 << 20, transcendentals=0),
        compiler_params=pltpu.CompilerParams(vmem_limit_bytes=16 << 20),
    )(tp, *mine, *came, *u, *z, *x)


def solution(mesh):
    return jax.shard_map(
        body,
        mesh=mesh,
        in_specs=(
            P("ep", None),
            P("ep", None),
            P("ep", None),
            P(),
            P(),
            P("ep", None, "tp"),
            P("ep", None, "tp"),
            P("ep", "tp", None),
        ),
        out_specs=(
            P("ep", "tp"),
            P("ep", None, "tp"),
            P("ep", None, "tp"),
            P("ep", "tp", None),
            P("ep", None),
            P("ep", None),
            P("ep", "tp"),
            P(("ep", "tp"), None),
            P(("ep", "tp"), None),
            P(("ep", "tp")),
        ),
        check_vma=False,
    )
```

```python
import functools

import jax
import jax.numpy as jnp
from jax import lax
from jax.experimental import pallas as pl
from jax.experimental.pallas import tpu as pltpu
from jax.sharding import PartitionSpec as P

BF = jnp.bfloat16
F32 = jnp.float32
GROUP_LANE = 32
EXTRA = 128


def mm(a, b):
    return lax.dot_general(a, b, (((1,), (0,)), ((), ())), preferred_element_type=F32)


def nt(a, b):
    return lax.dot_general(a, b, (((1,), (1,)), ((), ())), preferred_element_type=F32)


def tn(a, b):
    return lax.dot_general(a, b, (((0,), (0,)), ((), ())), preferred_element_type=F32)


def iota(shape, dim):
    return lax.broadcasted_iota(jnp.int32, shape, dim)


VM = pl.BlockSpec(memory_space=pltpu.VMEM)
HB = pl.BlockSpec(memory_space=pltpu.HBM)


def far(x):
    return pltpu.with_memory_space_constraint(x, pltpu.HBM)


def call(kernel, name, flops, limit, outs, scalars, arrays, scratch=(), spaces=None, out_spaces=None):
    smem = pl.BlockSpec(memory_space=pltpu.SMEM)
    vmem = pl.BlockSpec(memory_space=pltpu.VMEM)
    return pl.pallas_call(
        kernel,
        name=name,
        out_shape=[
            pltpu.HBM(shape, dtype) if out_spaces and out_spaces[k] is HB else jax.ShapeDtypeStruct(shape, dtype)
            for k, (shape, dtype) in enumerate(outs)
        ],
        in_specs=[smem] * len(scalars) + (spaces or [vmem] * len(arrays)),
        out_specs=out_spaces or [vmem] * len(outs),
        scratch_shapes=list(scratch),
        cost_estimate=pl.CostEstimate(flops=flops, bytes_accessed=4 << 20, transcendentals=0),
        compiler_params=pltpu.CompilerParams(vmem_limit_bytes=limit << 20),
    )(*scalars, *arrays)


def ones_where(mask):
    return jnp.where(mask, 1.0, 0.0).astype(BF)


def pre_kernel(
    ep_ref, tp_ref, rt_hbm, rgt_hbm, tok_hbm, cot_hbm, rex_hbm,
    send_ref, aux_ref, rt_ref, rgt_ref, tok_ref, cot_ref, rex_ref, one_ref, sems,
):
    tp = tp_ref[0]
    tok, dm = tok_ref.shape
    experts = rex_ref.shape[1]
    groups = rgt_ref.shape[0]
    gw = experts // groups
    width = dm // 4
    loads = [
        pltpu.make_async_copy(src, dst, sems.at[k])
        for k, (src, dst) in enumerate(
            ((rt_hbm, rt_ref), (tok_hbm, tok_ref), (rgt_hbm, rgt_ref), (rex_hbm, rex_ref), (cot_hbm, cot_ref))
        )
    ]
    for load in loads:
        load.start()
    loads[0].wait()
    r0, r1 = rt_ref[0:1, :], rt_ref[1:2, :]
    before = ones_where(iota((tok, tok), 0) < iota((tok, tok), 1))
    blk = min(256, experts * 8)
    blocks = experts * 8 // blk
    row = iota((blk, tok), 0)
    sub = row & 7
    want = (2 * tp + (sub & 1)).astype(F32)
    part = sub >> 1
    for b in range(blocks):
        rows = slice(b * blk, (b + 1) * blk)
        expert = b * (blk // 8) + (row >> 3)
        hit0 = r0 == expert
        hit1 = r1 == expert
        match = mm(ones_where(hit0 | hit1), before) == want
        one_ref[0, rows, :] = ones_where(hit0 & match)
        one_ref[1, rows, :] = ones_where(hit1 & match)

    def spread(sel):
        return jnp.concatenate([jnp.where(part == c, sel, 0.0).astype(BF) for c in range(4)], axis=1)

    def stacked(ref):
        return jnp.concatenate([ref[:, c * width : (c + 1) * width] for c in range(4)], axis=0)

    loads[1].wait()
    stack = stacked(tok_ref)
    for b in range(blocks):
        rows = slice(b * blk, (b + 1) * blk)
        one = one_ref[0, rows, :].astype(F32) + one_ref[1, rows, :].astype(F32)
        send_ref[rows, 0:width] = mm(spread(one), stack).astype(BF)
    loads[2].wait()
    loads[3].wait()
    group_exp = jnp.exp(nt(rgt_ref[...], tok_ref[...]))
    group_prob = group_exp / jnp.sum(group_exp, axis=0, keepdims=True)
    logits = jnp.transpose(mm(tok_ref[...], rex_ref[...]))
    ei = iota((experts, tok), 0)
    l0 = jnp.sum(jnp.where(ei == r0, logits, 0.0), axis=0, keepdims=True)
    l1 = jnp.sum(jnp.where(ei == r1, logits, 0.0), axis=0, keepdims=True)
    x0, x1 = jnp.exp(l0), jnp.exp(l1)
    p0, p1 = x0 / (x0 + x1), x1 / (x0 + x1)
    chosen = r0 // gw
    gi = iota((groups, tok), 0)
    picked = jnp.sum(jnp.where(gi == chosen, group_prob, 0.0), axis=0, keepdims=True)
    w0 = (picked * p0).astype(BF).astype(F32)
    w1 = (picked * p1).astype(BF).astype(F32)
    li = iota((EXTRA, tok), 0)
    diff = jnp.where(li == r0 - chosen * gw, 1.0, 0.0) - jnp.where(li == r1 - chosen * gw, 1.0, 0.0)
    group_side = jnp.where(li == GROUP_LANE + chosen, 1.0, 0.0)
    for j in range(groups):
        group_side = group_side - jnp.where(li == GROUP_LANE + j, group_prob[j : j + 1, :], 0.0)
    side_t = jnp.concatenate([(p1 * diff + group_side).astype(BF), (group_side - p0 * diff).astype(BF)], axis=1)
    arow = iota((EXTRA, tok), 0)
    aux = jnp.where(arow == 0, p0, jnp.where(arow == 1, p1, 0.0))
    for j in range(groups):
        aux = jnp.where(arow == 2 + j, group_prob[j : j + 1, :], aux)
    aux = jnp.where(arow == 6, r0.astype(F32), jnp.where(arow == 7, r1.astype(F32), aux))
    aux_ref[...] = jnp.transpose(aux)
    loads[4].wait()
    stack = stacked(cot_ref)
    for b in range(blocks):
        rows = slice(b * blk, (b + 1) * blk)
        one0, one1 = one_ref[0, rows, :].astype(F32), one_ref[1, rows, :].astype(F32)
        send_ref[rows, width : 2 * width] = mm(spread(one0 * w0 + one1 * w1), stack).astype(BF)
        head = part == 0
        both = jnp.concatenate(
            [jnp.where(head, one0, 0.0).astype(BF), jnp.where(head, one1, 0.0).astype(BF)], axis=1
        )
        send_ref[rows, 2 * width :] = nt(both, side_t).astype(BF)


def expert_kernel(
    tp_ref, got_ref, gate_ref, up_ref, down_ref,
    u_ref, z_ref, mine_ref, theirs_ref, x_out, sc_out, gd_out, ud_out, hid_out,
    x_ref, sc_ref, gd_ref, ud_ref, hid_ref, sems,
):
    tp = tp_ref[0]
    dm = gate_ref.shape[0]
    width, half = dm // 4, dm // 2
    blk = min(256, got_ref.shape[0])
    n4 = blk // 4
    shift = n4.bit_length() - 1
    o, i = iota((blk, blk), 0), iota((blk, blk), 1)
    perm = ones_where(i == ((o & (n4 - 1)) >> 1) * 8 + (o >> shift) * 2 + (o & 1))
    for b in range(got_ref.shape[0] // blk):
        block = slice(b * blk, (b + 1) * blk)
        rows = slice(b * n4, (b + 1) * n4)
        y = mm(perm, got_ref[block, 0 : 2 * width]).astype(BF)
        for c in range(4):
            cols = slice(c * width, (c + 1) * width)
            x_ref[rows, cols] = y[c * n4 : (c + 1) * n4, 0:width]
            sc_ref[rows, cols] = y[c * n4 : (c + 1) * n4, width:]
        z_ref[rows, :] = mm(perm[0:n4], got_ref[block, 2 * width :]).astype(BF)
    saves = [
        pltpu.make_async_copy(src, dst, sems.at[k])
        for k, (src, dst) in enumerate(
            ((x_ref, x_out), (sc_ref, sc_out), (gd_ref, gd_out), (ud_ref, ud_out), (hid_ref, hid_out))
        )
    ]
    saves[0].start()
    saves[1].start()
    gp = mm(x_ref[...], gate_ref[...])
    upre = mm(x_ref[...], up_ref[...])
    pulled = nt(sc_ref[...], down_ref[...])
    sig = 1.0 / (1.0 + jnp.exp(-gp))
    act = gp * sig
    hid = (act * upre).astype(BF)
    hid_ref[...] = hid
    u = jnp.sum(pulled * hid.astype(F32), axis=1, keepdims=True)
    gd = (pulled * (upre * sig * (1.0 + gp * (1.0 - sig)))).astype(BF)
    ud = (pulled * act).astype(BF)
    gd_ref[...] = gd
    ud_ref[...] = ud
    for save in saves[2:]:
        save.start()
    n = x_ref.shape[0]
    u_ref[...] = jnp.broadcast_to(u, (n, EXTRA))
    high = u.astype(BF).astype(F32)
    lane = iota((n, EXTRA), 1)
    theirs_ref[:, half:] = jnp.where(lane == 0, high, jnp.where(lane == 1, u - high, 0.0)).astype(BF)
    far = pl.ds(pl.multiple_of((1 - tp) * half, half), half)
    theirs_ref[:, 0:half] = (nt(gd, gate_ref[far, :]) + nt(ud, up_ref[far, :])).astype(BF)
    near = pl.ds(pl.multiple_of(tp * half, half), half)
    mine_ref[...] = (nt(gd, gate_ref[near, :]) + nt(ud, up_ref[near, :])).astype(BF)
    for save in saves:
        save.wait()


def pack_kernel(ep_ref, tp_ref, *refs):
    tp = tp_ref[0]
    mine, came, us, zs = refs[0:2], refs[2:4], refs[4:6], refs[6:8]
    rgt_hbm, rex_hbm, ret_out, y0_out, y1_out, sum_ref, ret_ref, y_ref, rgt_ref, rex_ref, sems = refs[8:19]
    n, half = mine[0].shape
    width = half // 2
    experts, groups = rex_ref.shape[1], rgt_ref.shape[0]
    gw = experts // groups
    group = ep_ref[0] // gw
    near = pl.ds(pl.multiple_of(tp * half, half), half)
    loads = [
        pltpu.make_async_copy(rex_hbm.at[near, :], rex_ref, sems.at[6]),
        pltpu.make_async_copy(rgt_hbm.at[:, near], rgt_ref, sems.at[7]),
    ]
    for load in loads:
        load.start()
    li, ei = iota((EXTRA, experts), 0), iota((EXTRA, experts), 1)
    to_expert = ones_where((ei == group * gw + li) & (li < gw))
    to_group = ones_where(iota((EXTRA, groups), 0) == GROUP_LANE + iota((EXTRA, groups), 1))
    saves = []
    for p, y_out in ((0, y0_out), (1, y1_out)):
        u = us[p][...] + came[p][:, half : half + 1].astype(F32) + came[p][:, half + 1 : half + 2].astype(F32)
        y = (u * zs[p][...].astype(F32)).astype(BF)
        y_ref[p] = y
        saves.append(pltpu.make_async_copy(y_ref.at[p], y_out, sems.at[p]))
        saves[-1].start()
    for load in loads:
        load.wait()
    for p in range(2):
        y = y_ref[p]
        route = nt(mm(y, to_expert).astype(BF), rex_ref[...])
        route = route + mm(mm(y, to_group).astype(BF), rgt_ref[...])
        sum_ref[p] = (mine[p][...].astype(F32) + came[p][:, 0:half].astype(F32) + route).astype(BF)
    blk = min(256, n * 4)
    bs = blk // 8
    o, i = iota((blk, blk), 0), iota((blk, blk), 1)
    perm = ones_where(i == ((o >> 2) & 1) * (4 * bs) + ((o >> 1) & 1) * (2 * bs) + (o >> 3) * 2 + (o & 1))
    for b in range(n // (2 * bs)):
        rows = slice(b * 2 * bs, (b + 1) * 2 * bs)
        stack = jnp.concatenate(
            [sum_ref[0, rows, 0:width], sum_ref[1, rows, 0:width], sum_ref[0, rows, width:], sum_ref[1, rows, width:]],
            axis=0,
        )
        out = pl.ds(b * blk, blk)
        ret_ref[out, :] = mm(perm, stack).astype(BF)
        saves.append(pltpu.make_async_copy(ret_ref.at[out, :], ret_out.at[out, :], sems.at[2 + b]))
        saves[-1].start()
    for save in saves:
        save.wait()


def rc_x_kernel(ep_ref, tp_ref, x0_ref, x1_ref, y0_ref, y1_ref, own_ref, s1_ref, s2_ref, s3_ref, all_ref):
    x, tp = ep_ref[0] & 3, tp_ref[0]
    planes = x0_ref.shape[1] // 256
    for b in range(planes):
        cols = slice(b * 256, (b + 1) * 256)
        rc = tn(x0_ref[:, cols], y0_ref[...]) + tn(x1_ref[:, cols], y1_ref[...])
        rc = rc.reshape(16, 16, EXTRA)
        all_ref[b * 16 : (b + 1) * 16] = jnp.where(tp == 0, rc[:, 0:8, :], rc[:, 8:16, :])
    for d, out_ref in enumerate((own_ref, s1_ref, s2_ref, s3_ref)):
        to = (x + d) & 3
        for q in range(planes * 4):
            out_ref[q * 8 : (q + 1) * 8, :] = all_ref[q * 4 + to].astype(out_ref.dtype)


def rc_y_kernel(ep_ref, tp_ref, own_ref, a_ref, b_ref, c_ref, o0_ref, o1_ref, o2_ref, o3_ref, all_ref):
    y = (ep_ref[0] >> 2) & 3
    total = own_ref[...]
    for ref in (a_ref, b_ref, c_ref):
        total = total + ref[...].astype(F32)
    all_ref[...] = total.reshape(all_ref.shape)
    for d, out_ref in enumerate((o0_ref, o1_ref, o2_ref, o3_ref)):
        to = (y + d) & 3
        for q in range(all_ref.shape[0] // 4):
            out_ref[q * 8 : (q + 1) * 8, :] = all_ref[q * 4 + to]


def rc_z_kernel(groups, gw, ep_ref, tp_ref, own_ref, a_ref, b_ref, c_ref, *refs):
    outs, all_ref = refs[:-1], refs[-1]
    planes = all_ref.shape[0]
    group, z = ep_ref[0] // gw, ep_ref[0] >> 4
    total = own_ref[...] + a_ref[...] + b_ref[...] + c_ref[...]
    rows = total.shape[0]
    near = total[:, 0:gw]
    placed = None
    for g in range(groups):
        parts = [near if h == g else jnp.zeros((rows, gw), F32) for h in range(groups)]
        spread = jnp.where(group == g, jnp.concatenate(parts, axis=1), 0.0)
        placed = spread if g == 0 else placed + spread
    all_ref[:, :, 0 : groups * gw] = placed.reshape(planes, 8, groups * gw)
    all_ref[:, :, groups * gw :] = total.reshape(planes, 8, EXTRA)
    for d, out_ref in enumerate(outs):
        out_ref[...] = all_ref[(z + d) & (planes - 1)]


def as_row(col):
    return jnp.transpose(jnp.broadcast_to(col, (col.shape[0], 128)))[0:1, :]


def in_grad_kernel(x0_ref, x1_ref, d0_ref, d1_ref, out_ref, sq_ref):
    blk = 128

    def step(b, carry):
        cols = pl.ds(pl.multiple_of(b * blk, blk), blk)
        full = tn(x0_ref[:, cols], d0_ref[...]) + tn(x1_ref[:, cols], d1_ref[...])
        out_ref[cols, :] = full.astype(BF)
        sq_ref[:, cols] = as_row(jnp.sum(full * full, axis=1, keepdims=True))
        return carry

    lax.fori_loop(0, out_ref.shape[0] // blk, step, 0)


def down_grad_kernel(h0_ref, h1_ref, s0_ref, s1_ref, out_ref, sq_ref, acc_ref):
    dm = out_ref.shape[1]
    wide = 512 if dm % 512 == 0 else 128
    acc_ref[...] = jnp.zeros_like(acc_ref)

    def step(b, carry):
        cols = pl.ds(pl.multiple_of(b * wide, wide), wide)
        full = tn(h0_ref[...], s0_ref[:, cols]) + tn(h1_ref[...], s1_ref[:, cols])
        out_ref[:, cols] = full.astype(BF)
        acc_ref[...] += jnp.broadcast_to(jnp.sum(full * full, axis=1, keepdims=True), acc_ref.shape)
        return carry

    lax.fori_loop(0, dm // wide, step, 0)
    sq_ref[...] = jnp.transpose(acc_ref[...])[0:1, :]


def home_kernel(tp_ref, aux_ref, sel_ref):
    tp = tp_ref[0]
    tok = aux_ref.shape[0]
    n = sel_ref.shape[2]
    r0, r1 = aux_ref[:, 6:7].astype(jnp.int32), aux_ref[:, 7:8].astype(jnp.int32)
    col = iota((tok, n), 1)
    hit = jnp.where(r0 == (col >> 3), 1.0, 0.0) + jnp.where(r1 == (col >> 3), 1.0, 0.0)
    earlier = ones_where(iota((tok, tok), 1) < iota((tok, tok), 0))
    rank = mm(earlier, hit.astype(BF))
    one = jnp.where(rank == ((2 * tp + (col & 3)) & 3).astype(F32), hit, 0.0)
    lower = (col & 4) == 0
    sel_ref[0] = jnp.where(lower, one, 0.0).astype(BF)
    sel_ref[1] = jnp.where(lower, 0.0, one).astype(BF)


def final_kernel(blocks, *refs):
    back_ref, sel_ref, g0_ref, g1_ref, u0_ref, u1_ref = refs[0:6]
    rcs = refs[6 : 6 + blocks]
    tg_ref, rex_ref, rg_ref, rows_ref, gate_sq_ref, up_sq_ref = refs[6 + blocks :]
    width = back_ref.shape[1]
    experts, groups = rex_ref.shape[1], rg_ref.shape[0]
    gate_sq_ref[...] = g0_ref[...] + g1_ref[...]
    up_sq_ref[...] = u0_ref[...] + u1_ref[...]
    for c in range(2):
        tg_ref[:, c * width : (c + 1) * width] = mm(sel_ref[c], back_ref[...]).astype(BF)
    total = rcs[0][...]
    for ref in rcs[1:]:
        total = total + ref[...]
    rex = total[:, 0:experts]
    rg = total[:, experts:]
    lane = iota(rg.shape, 1)
    rex_ref[...] = rex
    grp = jnp.where((lane >= GROUP_LANE) & (lane < GROUP_LANE + groups), rg, 0.0)
    square = jnp.sum(rex * rex, axis=1, keepdims=True) + jnp.sum(grp * grp, axis=1, keepdims=True)
    rest = jnp.transpose(jnp.where(lane == GROUP_LANE + groups, square, grp))
    rg_ref[...] = rest[GROUP_LANE : GROUP_LANE + groups, :]
    rows_ref[...] = rest[GROUP_LANE + groups : GROUP_LANE + groups + 1, :]


def body(tokens, cotangent, routes, router_group, router_expert, gate_proj, up_proj, down_proj):
    tok, dm = tokens.shape
    experts = router_expert.shape[1]
    groups = router_group.shape[1]
    width, half = dm // 4, dm // 2
    ff = gate_proj.shape[2]
    n = experts * 2
    tp = lax.axis_index("tp").reshape(1)
    swap = [(0, 1), (1, 0)]
    rgt = router_group.T
    ep = lax.axis_index("ep")
    planes = experts // 16
    idx = [ep.reshape(1), tp]
    gate, up, down = gate_proj[0], up_proj[0], down_proj[0]

    def exchange(x):
        m = x.shape[1]
        y = lax.all_to_all(x.reshape(experts, 8, m), "ep", split_axis=0, concat_axis=0, tiled=True)
        return y.reshape(experts * 8, m)

    def partner(x):
        return lax.ppermute(x, "tp", swap)

    def shift(v, stride, d):
        size = planes if stride == 16 else 4
        pairs = []
        for e in range(experts):
            at = e // stride % size
            pairs.append((e, e + ((at + d) % size - at) * stride))
        return lax.ppermute(v, "ep", pairs)

    send, aux = call(
        pre_kernel, "pre", 1 << 30, 20,
        [((experts * 8, 2 * width + EXTRA), BF), ((tok, EXTRA), F32)],
        idx, [far(routes.T), far(rgt), far(tokens), far(cotangent), far(router_expert)],
        scratch=[
            pltpu.VMEM((2, tok), jnp.int32), pltpu.VMEM((groups, dm), BF),
            pltpu.VMEM((tok, dm), BF), pltpu.VMEM((tok, dm), BF), pltpu.VMEM((dm, experts), BF),
            pltpu.VMEM((2, experts * 8, tok), BF), pltpu.SemaphoreType.DMA((5,)),
        ],
        spaces=[HB] * 5,
    )
    got = exchange(send)
    other = partner(got)
    u, z, mine, theirs, x, sc, gd, ud, hid = [list(v) for v in zip(*[
        call(
            expert_kernel, "expert", 3 << 30, 18,
            [((n, EXTRA), F32), ((n, EXTRA), BF), ((n, half), BF), ((n, half + EXTRA), BF),
             ((n, dm), BF), ((n, dm), BF), ((n, ff), BF), ((n, ff), BF), ((n, ff), BF)],
            [tp], [g, gate, up, down],
            scratch=[pltpu.VMEM((n, w), BF) for w in (dm, dm, ff, ff, ff)] + [pltpu.SemaphoreType.DMA((5,))],
            out_spaces=[VM] * 4 + [HB] * 5,
        )
        for g in (got, other)
    ])]
    came = [partner(theirs[1]), partner(theirs[0])]
    ret, y0, y1 = call(
        pack_kernel, "pack", 1 << 29, 16,
        [((experts * 8, width), BF), ((n, EXTRA), BF), ((n, EXTRA), BF)],
        idx, [*mine, *came, *u, *z, far(rgt), far(router_expert)],
        spaces=[VM] * 8 + [HB] * 2,
        scratch=[pltpu.VMEM((2, n, half), BF), pltpu.VMEM((experts * 8, width), BF), pltpu.VMEM((2, n, EXTRA), BF),
                 pltpu.VMEM((groups, half), BF), pltpu.VMEM((half, experts), BF), pltpu.SemaphoreType.DMA((8,))],
        out_spaces=[HB] * 3,
    )
    back = exchange(ret)
    r = planes * 32
    own, *sends = call(
        rc_x_kernel, "rc_x", 1 << 29, 12,
        [((r, EXTRA), F32)] + [((r, EXTRA), BF)] * 3,
        idx, [*x, y0, y1], scratch=[pltpu.VMEM((experts, 8, EXTRA), F32)],
    )
    came_x = [shift(v, 1, d + 1) for d, v in enumerate(sends)]
    own, *sends = call(
        rc_y_kernel, "rc_y", 1 << 20, 8, [((r // 4, EXTRA), F32)] * 4,
        idx, [own, *came_x], scratch=[pltpu.VMEM((planes * 4, 8, EXTRA), F32)],
    )
    came_y = [shift(v, 4, d + 1) for d, v in enumerate(sends)]
    wide = experts + EXTRA
    own, *sends = call(
        functools.partial(rc_z_kernel, groups, experts // groups), "rc_z", 1 << 20, 8, [((8, wide), F32)] * planes,
        idx, [own, *came_y], scratch=[pltpu.VMEM((planes, 8, wide), F32)],
    )
    rcs = [own] + [shift(v, 16, d + 1) for d, v in enumerate(sends)]
    in_grads = [
        call(
            in_grad_kernel, name, 1 << 30, 12, [((dm, ff), BF), ((1, dm), F32)], [], [*x, *delta],
        )
        for name, delta in (("gate_grad", gd), ("up_grad", ud))
    ]
    (gate_grad, gate_sq), (up_grad, up_sq) = in_grads
    down_grad, down_sq = call(
        down_grad_kernel, "down_grad", 1 << 30, 12, [((ff, dm), BF), ((1, ff), F32)],
        [], [*hid, *sc], scratch=[pltpu.VMEM((ff, 128), F32)],
    )
    (sel,) = call(home_kernel, "home", 1 << 26, 8, [((2, tok, experts * 8), BF)], [tp], [aux])
    token_grad, rex_grad, rg_grad, rows, gate_sq, up_sq = call(
        functools.partial(final_kernel, len(rcs)), "final", 1 << 29, 10,
        [((tok, half), BF), ((8, experts), F32), ((groups, 8), F32), ((1, 8), F32),
         ((1, dm), F32), ((1, dm), F32)],
        [], [back, sel, gate_sq, partner(gate_sq), up_sq, partner(up_sq), *rcs],
    )
    return (
        token_grad,
        gate_grad[None],
        up_grad[None],
        down_grad[None],
        gate_sq,
        up_sq,
        down_sq,
        rex_grad,
        rg_grad.T,
        rows[0],
    )


def solution(mesh):
    return jax.shard_map(
        body,
        mesh=mesh,
        in_specs=(
            P("ep", None),
            P("ep", None),
            P("ep", None),
            P(),
            P(),
            P("ep", None, "tp"),
            P("ep", None, "tp"),
            P("ep", "tp", None),
        ),
        out_specs=(
            P("ep", "tp"),
            P("ep", None, "tp"),
            P("ep", None, "tp"),
            P("ep", "tp", None),
            P("ep", None),
            P("ep", None),
            P("ep", "tp"),
            P(("ep", "tp"), None),
            P(("ep", "tp"), None),
            P(("ep", "tp")),
        ),
        check_vma=False,
    )
```

```python
import functools

import jax
import jax.numpy as jnp
from jax import lax
from jax.experimental import pallas as pl
from jax.experimental.pallas import tpu as pltpu
from jax.sharding import PartitionSpec as P


BF = jnp.bfloat16
F32 = jnp.float32
GROUP_LANE = 32
U_LANE = 40
LOW_LANE = 64
EXTRA = 128


def mm(a, b):
    return lax.dot_general(a, b, (((1,), (0,)), ((), ())), preferred_element_type=F32)


def nt(a, b):
    return lax.dot_general(a, b, (((1,), (1,)), ((), ())), preferred_element_type=F32)


def tn(a, b):
    return lax.dot_general(a, b, (((0,), (0,)), ((), ())), preferred_element_type=F32)


def iota(shape, dim):
    return lax.broadcasted_iota(jnp.int32, shape, dim)


VM = pl.BlockSpec(memory_space=pltpu.VMEM)
HB = pl.BlockSpec(memory_space=pltpu.HBM)


def far(x):
    return pltpu.with_memory_space_constraint(x, pltpu.HBM)


def call(kernel, flops, limit, outs, scalars, arrays, scratch=(), spaces=None, out_spaces=None):
    smem = pl.BlockSpec(memory_space=pltpu.SMEM)
    vmem = pl.BlockSpec(memory_space=pltpu.VMEM)
    return pl.pallas_call(
        kernel,
        out_shape=[
            pltpu.HBM(shape, dtype) if out_spaces and out_spaces[k] is HB else jax.ShapeDtypeStruct(shape, dtype)
            for k, (shape, dtype) in enumerate(outs)
        ],
        in_specs=[smem] * len(scalars) + (spaces or [vmem] * len(arrays)),
        out_specs=out_spaces or [vmem] * len(outs),
        scratch_shapes=list(scratch),
        cost_estimate=pl.CostEstimate(flops=flops, bytes_accessed=4 << 20, transcendentals=0),
        compiler_params=pltpu.CompilerParams(vmem_limit_bytes=limit << 20),
    )(*scalars, *arrays)


def ones_where(mask):
    return jnp.where(mask, 1.0, 0.0).astype(BF)


def pre_kernel(
    ep_ref, tp_ref, rt_hbm, rgt_hbm, tok_hbm, cot_hbm, rex_hbm,
    send_out, aux_ref, send_ref, rt_ref, rgt_ref, tok_ref, cot_ref, rex_ref, one_ref, sems,
):
    tp = tp_ref[0]
    tok, dm = tok_ref.shape
    experts = rex_ref.shape[1]
    groups = rgt_ref.shape[0]
    gw = experts // groups
    width = dm // 4
    loads = [
        pltpu.make_async_copy(src, dst, sems.at[k])
        for k, (src, dst) in enumerate(
            ((rt_hbm, rt_ref), (tok_hbm, tok_ref), (rgt_hbm, rgt_ref), (rex_hbm, rex_ref), (cot_hbm, cot_ref))
        )
    ]
    for load in loads:
        load.start()
    loads[0].wait()
    r0, r1 = rt_ref[0:1, :], rt_ref[1:2, :]
    before = ones_where(iota((tok, tok), 0) < iota((tok, tok), 1))
    blk = min(256, experts * 8)
    blocks = experts * 8 // blk
    row = iota((blk, tok), 0)
    sub = row & 7
    want = (2 * tp + (sub & 1)).astype(F32)
    part = sub >> 1
    for b in range(blocks):
        rows = slice(b * blk, (b + 1) * blk)
        expert = b * (blk // 8) + (row >> 3)
        hit0 = r0 == expert
        hit1 = r1 == expert
        match = mm(ones_where(hit0 | hit1), before) == want
        one_ref[0, rows, :] = ones_where(hit0 & match)
        one_ref[1, rows, :] = ones_where(hit1 & match)

    def spread(sel):
        return jnp.concatenate([jnp.where(part == c, sel, 0.0).astype(BF) for c in range(4)], axis=1)

    def stacked(ref):
        return jnp.concatenate([ref[:, c * width : (c + 1) * width] for c in range(4)], axis=0)

    saves = []

    def save(k, rows, cols):
        saves.append(pltpu.make_async_copy(send_ref.at[rows, cols], send_out.at[rows, cols], sems.at[5 + k]))
        saves[-1].start()

    loads[1].wait()
    stack = stacked(tok_ref)
    for b in range(blocks):
        rows = slice(b * blk, (b + 1) * blk)
        one = one_ref[0, rows, :].astype(F32) + one_ref[1, rows, :].astype(F32)
        send_ref[rows, 0:width] = mm(spread(one), stack).astype(BF)
        save(2 * b, rows, slice(0, width))
    loads[2].wait()
    loads[3].wait()
    group_exp = jnp.exp(nt(rgt_ref[...], tok_ref[...]))
    group_prob = group_exp / jnp.sum(group_exp, axis=0, keepdims=True)
    logits = jnp.transpose(mm(tok_ref[...], rex_ref[...]))
    ei = iota((experts, tok), 0)
    l0 = jnp.sum(jnp.where(ei == r0, logits, 0.0), axis=0, keepdims=True)
    l1 = jnp.sum(jnp.where(ei == r1, logits, 0.0), axis=0, keepdims=True)
    x0, x1 = jnp.exp(l0), jnp.exp(l1)
    p0, p1 = x0 / (x0 + x1), x1 / (x0 + x1)
    chosen = r0 // gw
    gi = iota((groups, tok), 0)
    picked = jnp.sum(jnp.where(gi == chosen, group_prob, 0.0), axis=0, keepdims=True)
    w0 = (picked * p0).astype(BF).astype(F32)
    w1 = (picked * p1).astype(BF).astype(F32)
    arow = iota((EXTRA, tok), 0)
    aux = jnp.where(arow == 0, p0, jnp.where(arow == 1, p1, 0.0))
    for j in range(groups):
        aux = jnp.where(arow == 2 + j, group_prob[j : j + 1, :], aux)
    aux = jnp.where(arow == 6, r0.astype(F32), jnp.where(arow == 7, r1.astype(F32), aux))
    aux_ref[...] = aux
    loads[4].wait()
    stack = stacked(cot_ref)
    for b in range(blocks):
        rows = slice(b * blk, (b + 1) * blk)
        one0, one1 = one_ref[0, rows, :].astype(F32), one_ref[1, rows, :].astype(F32)
        send_ref[rows, width : 2 * width] = mm(spread(one0 * w0 + one1 * w1), stack).astype(BF)
        save(2 * b + 1, rows, slice(width, 2 * width))
    for copy in saves:
        copy.wait()


def pick_rows(outs, rows_in, stride, at):
    n = rows_in.shape[0] // stride
    for d, out_ref in enumerate(outs):
        want = iota((n, n * stride), 0) * stride + ((at + d) & (stride - 1))
        out_ref[...] = mm(ones_where(iota((n, n * stride), 1) == want), rows_in).astype(BF)


def side_x_kernel(groups, ep_ref, aux_ref, *outs):
    tok = aux_ref.shape[1]
    experts = outs[0].shape[0] * 4
    gw = experts // groups
    r0, r1 = aux_ref[6:7, :].astype(jnp.int32), aux_ref[7:8, :].astype(jnp.int32)
    ei = iota((experts, tok), 0)
    one0 = jnp.where(ei == r0, 1.0, 0.0)
    one1 = jnp.where(ei == r1, 1.0, 0.0)
    before = ones_where(iota((tok, tok), 0) < iota((tok, tok), 1))
    rank = mm((one0 + one1).astype(BF), before)
    li = iota((EXTRA, tok), 0)
    base = (r0 // gw) * gw
    shared = jnp.zeros((EXTRA, tok), F32)
    for j in range(groups):
        shared = jnp.where((li & 7) == 2 + j, aux_ref[2 + j : 3 + j, :], shared)
    kinds = []
    for other, prob in ((r1, aux_ref[1:2, :]), (r0, aux_ref[0:1, :])):
        kinds.append(
            jnp.where((li & 7) == 0, (other - base).astype(F32), jnp.where((li & 7) == 1, prob, shared))
        )
    total = None
    for r in range(4):
        for one, kind in ((one0, kinds[0]), (one1, kinds[1])):
            left = jnp.where(rank == float(r), one, 0.0).astype(BF)
            right = jnp.where((li >> 3) == r, kind, 0.0).astype(BF)
            term = nt(left, right)
            total = term if total is None else total + term
    pick_rows(outs, total.astype(BF), 4, ep_ref[0] & 3)


def side_y_kernel(ep_ref, a_ref, b_ref, c_ref, d_ref, *outs):
    rows = jnp.concatenate([a_ref[...], b_ref[...], c_ref[...], d_ref[...]], axis=0)
    pick_rows(outs, rows, 4, (ep_ref[0] >> 2) & 3)


def side_z_kernel(ep_ref, a_ref, b_ref, c_ref, d_ref, *outs):
    rows = jnp.concatenate([a_ref[...], b_ref[...], c_ref[...], d_ref[...]], axis=0)
    pick_rows(outs, rows, len(outs), ep_ref[0] >> 4)


def side_end_kernel(groups, ep_ref, tp_ref, *refs):
    ins, outs = refs[:-2], refs[-2:]
    rows = jnp.concatenate([ref[...] for ref in ins], axis=0)
    experts = rows.shape[0]
    planes = len(ins)
    gw = experts // groups
    e, tp = ep_ref[0], tp_ref[0]
    n = experts * 2
    src = iota((n, experts), 0) >> 1
    dz = ((e >> 4) - (src >> 4)) & (planes - 1)
    dy = ((e >> 2) - (src >> 2)) & 3
    dx = (e - src) & 3
    spread = mm(ones_where(iota((n, experts), 1) == dz * 16 + dy * 4 + dx), rows)
    lane = iota((n, EXTRA), 1)
    li = lane & (LOW_LANE - 1)
    chosen = e // gw
    own = jnp.where(li == e - chosen * gw, 1.0, 0.0)
    mark = jnp.where(li == GROUP_LANE + chosen, 1.0, 0.0)
    for p, out_ref in enumerate(outs):
        slot = 2 * ((tp + p) & 1) + (iota((n, EXTRA), 0) & 1)

        def value(v):
            return jnp.sum(jnp.where(lane == slot * 8 + v, spread, 0.0), axis=1, keepdims=True)

        z = value(1) * (own - jnp.where(li.astype(F32) == value(0), 1.0, 0.0)) + mark
        for j in range(groups):
            z = z - jnp.where(li == GROUP_LANE + j, value(2 + j), 0.0)
        out_ref[...] = z.astype(BF)


def expert_kernel(load, tp_ref, got_ref, *refs):
    tp = tp_ref[0]
    weights, refs = refs[:3], refs[3:]
    u_ref, mine_ref, theirs_ref, x_ref, x_out, sc_out, gd_out, ud_out, hid_out = refs[:9]
    sc_ref, gd_ref, ud_ref, hid_ref, sems = refs[-5:]
    gate_ref, up_ref, down_ref = refs[9:12] if load else weights
    loads = []
    if load:
        loads = [
            pltpu.make_async_copy(src, dst, sems.at[5 + k])
            for k, (src, dst) in enumerate(zip(weights, (gate_ref, up_ref, down_ref)))
        ]
        for copy in loads:
            copy.start()
    dm = gate_ref.shape[0]
    width, half = dm // 4, dm // 2
    blk = min(256, got_ref.shape[0])
    n4 = blk // 4
    shift = n4.bit_length() - 1
    o, i = iota((blk, blk), 0), iota((blk, blk), 1)
    perm = ones_where(i == ((o & (n4 - 1)) >> 1) * 8 + (o >> shift) * 2 + (o & 1))
    for b in range(got_ref.shape[0] // blk):
        block = slice(b * blk, (b + 1) * blk)
        rows = slice(b * n4, (b + 1) * n4)
        y = mm(perm, got_ref[block, 0 : 2 * width]).astype(BF)
        for c in range(4):
            cols = slice(c * width, (c + 1) * width)
            x_ref[rows, cols] = y[c * n4 : (c + 1) * n4, 0:width]
            sc_ref[rows, cols] = y[c * n4 : (c + 1) * n4, width:]
    saves = [
        pltpu.make_async_copy(src, dst, sems.at[k])
        for k, (src, dst) in enumerate(
            ((x_ref, x_out), (sc_ref, sc_out), (gd_ref, gd_out), (ud_ref, ud_out), (hid_ref, hid_out))
        )
    ]
    saves[0].start()
    saves[1].start()
    if load:
        loads[0].wait()
    gp = mm(x_ref[...], gate_ref[...])
    if load:
        loads[1].wait()
    upre = mm(x_ref[...], up_ref[...])
    if load:
        loads[2].wait()
    pulled = nt(sc_ref[...], down_ref[...])
    sig = 1.0 / (1.0 + jnp.exp(-gp))
    act = gp * sig
    hid = (act * upre).astype(BF)
    hid_ref[...] = hid
    u = jnp.sum(pulled * hid.astype(F32), axis=1, keepdims=True)
    gd = (pulled * (upre * sig * (1.0 + gp * (1.0 - sig)))).astype(BF)
    ud = (pulled * act).astype(BF)
    gd_ref[...] = gd
    ud_ref[...] = ud
    for save in saves[2:]:
        save.start()
    n = x_ref.shape[0]
    u_ref[...] = jnp.broadcast_to(u, (n, EXTRA))
    high = u.astype(BF).astype(F32)
    lane = iota((n, EXTRA), 1)
    theirs_ref[:, half:] = jnp.where(lane == 0, high, jnp.where(lane == 1, u - high, 0.0)).astype(BF)
    far = pl.ds(pl.multiple_of((1 - tp) * half, half), half)
    theirs_ref[:, 0:half] = (nt(gd, gate_ref[far, :]) + nt(ud, up_ref[far, :])).astype(BF)
    near = pl.ds(pl.multiple_of(tp * half, half), half)
    mine_ref[...] = (nt(gd, gate_ref[near, :]) + nt(ud, up_ref[near, :])).astype(BF)
    for save in saves:
        save.wait()


def pack_kernel(tp_ref, *refs):
    tp = tp_ref[0]
    mine, came, us, zs, xs = refs[0:2], refs[2:4], refs[4:6], refs[6:8], refs[8:10]
    ret_out, ret_ref, y0_ref, y1_ref, ul_ref, sems = refs[10:16]
    saves = []
    n, half = mine[0].shape
    width = half // 2
    lane = iota((n, EXTRA), 1)
    for p, y_ref in ((0, y0_ref), (1, y1_ref)):
        u = us[p][...] + came[p][:, half : half + 1].astype(F32) + came[p][:, half + 1 : half + 2].astype(F32)
        y_ref[...] = (u * zs[p][...].astype(F32)).astype(BF)
        ul_ref[p * n : (p + 1) * n, :] = jnp.where(lane == U_LANE, u, 0.0).astype(BF)
    blk = min(256, n * 4)
    bs = blk // 8
    o, i = iota((blk, blk), 0), iota((blk, blk), 1)
    perm = ones_where(i == ((o >> 2) & 1) * (4 * bs) + ((o >> 1) & 1) * (2 * bs) + (o >> 3) * 2 + (o & 1))
    wide = iota((blk, EXTRA), 1) < LOW_LANE
    for b in range(n // (2 * bs)):
        rows = slice(b * 2 * bs, (b + 1) * 2 * bs)
        out = slice(b * blk, (b + 1) * blk)
        sums = [(mine[p][rows, :].astype(F32) + came[p][rows, 0:half].astype(F32)).astype(BF) for p in range(2)]
        stack = jnp.concatenate(
            [sums[0][:, 0:width], sums[1][:, 0:width], sums[0][:, width:], sums[1][:, width:]], axis=0
        )
        ret_ref[out, 0:width] = mm(perm, stack).astype(BF)
        ulane = jnp.concatenate([ul_ref[rows, :], ul_ref[n + b * 2 * bs : n + (b + 1) * 2 * bs, :]], axis=0)
        base = mm(perm[:, 0 : 4 * bs], ulane)
        cols = slice(b * 16 * bs, (b + 1) * 16 * bs)
        rc = tn(xs[0][:, cols], y0_ref[...]) + tn(xs[1][:, cols], y1_ref[...])
        rc = rc.reshape(bs, 16, EXTRA)
        rc = jnp.where(tp == 0, rc[:, 0:8, :], rc[:, 8:16, :]).reshape(blk, EXTRA)
        high = rc.astype(BF).astype(F32)
        ret_ref[out, width:] = (base + jnp.where(wide, high, rc - high)).astype(BF)
        saves.append(pltpu.make_async_copy(ret_ref.at[out, :], ret_out.at[out, :], sems.at[b]))
        saves[-1].start()
    for save in saves:
        save.wait()


def grads_kernel(*refs):
    x, sc, gd, ud, hid = (refs[2 * k : 2 * k + 2] for k in range(5))
    gate_ref, up_ref, down_ref, sq_ref, down_sq_ref, acc_ref = refs[10:]
    dm, _ = gate_ref.shape
    blk = 128
    wide = 512 if dm % 512 == 0 else 128

    def as_row(col):
        return jnp.transpose(jnp.broadcast_to(col, (col.shape[0], 128)))[0:1, :]

    def step(b, carry):
        cols = pl.ds(pl.multiple_of(b * blk, blk), blk)
        for k, (delta, out_ref) in enumerate(((gd, gate_ref), (ud, up_ref))):
            full = tn(x[0][:, cols], delta[0][...]) + tn(x[1][:, cols], delta[1][...])
            out_ref[cols, :] = full.astype(BF)
            sq_ref[k : k + 1, cols] = as_row(jnp.sum(full * full, axis=1, keepdims=True))
        return carry

    lax.fori_loop(0, dm // blk, step, 0)
    acc_ref[...] = jnp.zeros_like(acc_ref)

    def down_step(b, carry):
        cols = pl.ds(pl.multiple_of(b * wide, wide), wide)
        full = tn(hid[0][...], sc[0][:, cols]) + tn(hid[1][...], sc[1][:, cols])
        down_ref[:, cols] = full.astype(BF)
        acc_ref[...] += jnp.broadcast_to(jnp.sum(full * full, axis=1, keepdims=True), acc_ref.shape)
        return carry

    lax.fori_loop(0, dm // wide, down_step, 0)
    down_sq_ref[...] = jnp.transpose(acc_ref[...])[0:1, :]


def home_kernel(tp_ref, raux_ref, rg_ref, rex_ref, sel_ref, q_ref, h_ref, aux_ref):
    tp = tp_ref[0]
    aux_ref[...] = jnp.transpose(raux_ref[...])
    tok = aux_ref.shape[0]
    half = q_ref.shape[1]
    groups = rg_ref.shape[0]
    experts = rex_ref.shape[1]
    gw = experts // groups
    r0, r1 = aux_ref[:, 6:7].astype(jnp.int32), aux_ref[:, 7:8].astype(jnp.int32)
    n = experts * 8
    col = iota((tok, n), 1)
    hit0 = r0 == (col >> 3)
    hit1 = r1 == (col >> 3)
    earlier = ones_where(iota((tok, tok), 1) < iota((tok, tok), 0))
    rank = mm(earlier, ones_where(hit0 | hit1))
    match = rank == ((2 * tp + (col & 3)) & 3).astype(F32)
    lower = (col & 4) == 0
    one0 = jnp.where(hit0 & match, 1.0, 0.0)
    one1 = jnp.where(hit1 & match, 1.0, 0.0)
    sel_ref[0] = jnp.where(lower, one0, 0.0).astype(BF)
    sel_ref[1] = jnp.where(lower, one1, 0.0).astype(BF)
    sel_ref[2] = jnp.where(lower, one0 + one1, 0.0).astype(BF)
    sel_ref[3] = jnp.where(lower, 0.0, one0 + one1).astype(BF)
    ei = iota((tok, experts), 1)
    pick = (jnp.where(ei == r0, 1.0, 0.0) - jnp.where(ei == r1, 1.0, 0.0)).astype(BF)
    near = pl.ds(pl.multiple_of(tp * half, half), half)
    q_ref[...] = nt(pick, rex_ref[near, :])
    h = None
    for j in range(groups):
        side = jnp.where(r0 // gw == j, 1.0, 0.0) - aux_ref[:, 2 + j : 3 + j]
        term = side * rg_ref[pl.ds(j, 1), near].astype(F32)
        h = term if j == 0 else h + term
    h_ref[...] = h


def final_kernel(
    back_ref, sel_ref, aux_ref, q_ref, h_ref, sq_ref, sqo_ref,
    tg_ref, rex_ref, rg_ref, rows_ref, gate_sq_ref, up_sq_ref,
):
    gate_sq_ref[...] = sq_ref[0:1, :] + sqo_ref[0:1, :]
    up_sq_ref[...] = sq_ref[1:2, :] + sqo_ref[1:2, :]
    width = back_ref.shape[1] - EXTRA
    experts = rex_ref.shape[1]
    groups = rg_ref.shape[0]
    gw = experts // groups
    extra = back_ref[:, width:]
    u0 = mm(sel_ref[0], extra)[:, U_LANE : U_LANE + 1]
    u1 = mm(sel_ref[1], extra)[:, U_LANE : U_LANE + 1]
    lean = aux_ref[:, 1:2] * u0 - aux_ref[:, 0:1] * u1
    both = u0 + u1
    for c in range(2):
        cols = slice(c * width, (c + 1) * width)
        part = mm(sel_ref[2 + c], back_ref[:, 0:width])
        tg_ref[:, cols] = (part + (both * h_ref[:, cols] + lean * q_ref[:, cols])).astype(BF)
    sums = jnp.sum(extra.astype(F32).reshape(groups, gw, 8, EXTRA), axis=1)
    rg = None
    square = None
    lane = iota((8, EXTRA), 1)
    for g in range(groups):
        s = sums[g]
        s = s + jnp.concatenate([s[:, LOW_LANE:], s[:, 0:LOW_LANE]], axis=1)
        rex = s[:, 0:gw]
        rex_ref[:, g * gw : (g + 1) * gw] = rex
        rg = s if g == 0 else rg + s
        sq = jnp.sum(rex * rex, axis=1, keepdims=True)
        square = sq if g == 0 else square + sq
    grp = rg[:, GROUP_LANE : GROUP_LANE + groups]
    square = square + jnp.sum(grp * grp, axis=1, keepdims=True)
    rest = jnp.transpose(jnp.where(lane == GROUP_LANE + groups, square, rg))
    rg_ref[...] = rest[GROUP_LANE : GROUP_LANE + groups, :]
    rows_ref[...] = rest[GROUP_LANE + groups : GROUP_LANE + groups + 1, :]


def body(tokens, cotangent, routes, router_group, router_expert, gate_proj, up_proj, down_proj):
    tok, dm = tokens.shape
    experts = router_expert.shape[1]
    groups = router_group.shape[1]
    width, half = dm // 4, dm // 2
    ff = gate_proj.shape[2]
    n = experts * 2
    tp = lax.axis_index("tp").reshape(1)
    swap = [(0, 1), (1, 0)]
    rgt = router_group.T
    ep = lax.axis_index("ep")
    planes = experts // 16
    idx = [ep.reshape(1), tp]
    gate, up, down = gate_proj[0], up_proj[0], down_proj[0]

    def exchange(x):
        m = x.shape[1]
        y = lax.all_to_all(x.reshape(experts, 8, m), "ep", split_axis=0, concat_axis=0, tiled=True)
        return y.reshape(experts * 8, m)

    def partner(x):
        return lax.ppermute(x, "tp", swap)

    def shift(v, stride, d):
        size = planes if stride == 16 else 4
        pairs = []
        for e in range(experts):
            at = e // stride % size
            pairs.append((e, e + ((at + d) % size - at) * stride))
        return lax.ppermute(v, "ep", pairs)

    send, aux = call(
        pre_kernel, 1 << 30, 20,
        [((experts * 8, 2 * width), BF), ((EXTRA, tok), F32)],
        idx, [far(routes.T), far(rgt), far(tokens), far(cotangent), far(router_expert)],
        scratch=[
            pltpu.VMEM((experts * 8, 2 * width), BF), pltpu.VMEM((2, tok), jnp.int32), pltpu.VMEM((groups, dm), BF),
            pltpu.VMEM((tok, dm), BF), pltpu.VMEM((tok, dm), BF), pltpu.VMEM((dm, experts), BF),
            pltpu.VMEM((2, experts * 8, tok), BF), pltpu.SemaphoreType.DMA((13,)),
        ],
        spaces=[HB] * 5,
        out_spaces=[HB, VM],
    )
    got = exchange(send)
    sides = call(
        functools.partial(side_x_kernel, groups), 1 << 28, 6,
        [((experts // 4, EXTRA), BF)] * 4, idx[:1], [aux],
    )
    sides = [shift(v, 1, d) if d else v for d, v in enumerate(sides)]
    sides = call(side_y_kernel, 1 << 24, 6, [((experts // 4, EXTRA), BF)] * 4, idx[:1], sides)
    sides = [shift(v, 4, d) if d else v for d, v in enumerate(sides)]
    sides = call(side_z_kernel, 1 << 24, 6, [((16, EXTRA), BF)] * planes, idx[:1], sides)
    sides = [shift(v, 16, d) if d else v for d, v in enumerate(sides)]
    z = call(functools.partial(side_end_kernel, groups), 1 << 24, 6, [((n, EXTRA), BF)] * 2, idx, sides)
    other = partner(got)

    def expert(g, weights, load):
        held = [((dm, ff), BF), ((dm, ff), BF), ((ff, dm), BF)] if load else []
        return call(
            functools.partial(expert_kernel, load), 3 << 30, 18,
            [((n, EXTRA), F32), ((n, half), BF), ((n, half + EXTRA), BF), ((n, dm), BF),
             ((n, dm), BF), ((n, dm), BF), ((n, ff), BF), ((n, ff), BF), ((n, ff), BF)] + held,
            [tp], [g, *weights],
            scratch=[pltpu.VMEM((n, w), BF) for w in (dm, ff, ff, ff)] + [pltpu.SemaphoreType.DMA((8,))],
            spaces=[VM] + [HB if load else VM] * 3,
            out_spaces=[VM] * 4 + [HB] * 5 + [VM] * len(held),
        )

    first = expert(got, [far(gate), far(up), far(down)], True)
    second = expert(other, first[9:], False)
    u, mine, theirs, xv, x, sc, gd, ud, hid = [list(v) for v in zip(first[:9], second)]
    came = [partner(theirs[1]), partner(theirs[0])]
    (ret,) = call(
        pack_kernel, 1 << 29, 16, [((experts * 8, width + EXTRA), BF)],
        [tp], [*mine, *came, *u, *z, *xv],
        scratch=[
            pltpu.VMEM((experts * 8, width + EXTRA), BF), pltpu.VMEM((n, EXTRA), BF), pltpu.VMEM((n, EXTRA), BF),
            pltpu.VMEM((2 * n, EXTRA), BF), pltpu.SemaphoreType.DMA((4,)),
        ],
        out_spaces=[HB],
    )
    back = exchange(ret)
    gate_grad, up_grad, down_grad, sq, down_sq = call(
        grads_kernel, 3 << 30, 20,
        [((dm, ff), BF), ((dm, ff), BF), ((ff, dm), BF), ((2, dm), F32), ((1, ff), F32)],
        [], [*x, *sc, *gd, *ud, *hid], scratch=[pltpu.VMEM((ff, 128), F32)],
    )
    sq_other = partner(sq)
    sel, q, h, aux_cols = call(
        home_kernel, 1 << 29, 8,
        [((4, tok, experts * 8), BF), ((tok, half), F32), ((tok, half), F32), ((tok, EXTRA), F32)],
        [tp], [aux, rgt, router_expert],
    )
    token_grad, rex_grad, rg_grad, rows, gate_sq, up_sq = call(
        final_kernel, 1 << 29, 10,
        [((tok, half), BF), ((8, experts), F32), ((groups, 8), F32), ((1, 8), F32),
         ((1, dm), F32), ((1, dm), F32)],
        [], [back, sel, aux_cols, q, h, sq, sq_other],
    )
    return (
        token_grad,
        gate_grad[None],
        up_grad[None],
        down_grad[None],
        gate_sq,
        up_sq,
        down_sq,
        rex_grad,
        rg_grad.T,
        rows[0],
    )


def solution(mesh):
    return jax.shard_map(
        body,
        mesh=mesh,
        in_specs=(
            P("ep", None),
            P("ep", None),
            P("ep", None),
            P(),
            P(),
            P("ep", None, "tp"),
            P("ep", None, "tp"),
            P("ep", "tp", None),
        ),
        out_specs=(
            P("ep", "tp"),
            P("ep", None, "tp"),
            P("ep", None, "tp"),
            P("ep", "tp", None),
            P("ep", None),
            P("ep", None),
            P("ep", "tp"),
            P(("ep", "tp"), None),
            P(("ep", "tp"), None),
            P(("ep", "tp")),
        ),
        check_vma=False,
    )
```

```python
import functools

import jax
import jax.numpy as jnp
from jax import lax
from jax.experimental import pallas as pl
from jax.experimental.pallas import tpu as pltpu
from jax.sharding import PartitionSpec as P


BF = jnp.bfloat16
F32 = jnp.float32
GROUP_LANE = 32
U_LANE = 40
LOW_LANE = 64
EXTRA = 128


def mm(a, b):
    return lax.dot_general(a, b, (((1,), (0,)), ((), ())), preferred_element_type=F32)


def nt(a, b):
    return lax.dot_general(a, b, (((1,), (1,)), ((), ())), preferred_element_type=F32)


def tn(a, b):
    return lax.dot_general(a, b, (((0,), (0,)), ((), ())), preferred_element_type=F32)


def iota(shape, dim):
    return lax.broadcasted_iota(jnp.int32, shape, dim)


VM = pl.BlockSpec(memory_space=pltpu.VMEM)
HB = pl.BlockSpec(memory_space=pltpu.HBM)


def far(x):
    return pltpu.with_memory_space_constraint(x, pltpu.HBM)


def call(kernel, flops, limit, outs, scalars, arrays, scratch=(), spaces=None, out_spaces=None):
    smem = pl.BlockSpec(memory_space=pltpu.SMEM)
    vmem = pl.BlockSpec(memory_space=pltpu.VMEM)
    return pl.pallas_call(
        kernel,
        out_shape=[
            pltpu.HBM(shape, dtype) if out_spaces and out_spaces[k] is HB else jax.ShapeDtypeStruct(shape, dtype)
            for k, (shape, dtype) in enumerate(outs)
        ],
        in_specs=[smem] * len(scalars) + (spaces or [vmem] * len(arrays)),
        out_specs=out_spaces or [vmem] * len(outs),
        scratch_shapes=list(scratch),
        cost_estimate=pl.CostEstimate(flops=flops, bytes_accessed=4 << 20, transcendentals=0),
        compiler_params=pltpu.CompilerParams(vmem_limit_bytes=limit << 20),
    )(*scalars, *arrays)


def ones_where(mask):
    return jnp.where(mask, 1.0, 0.0).astype(BF)


def pre_kernel(
    ep_ref, tp_ref, rt_hbm, rgt_hbm, tok_hbm, cot_hbm, rex_hbm,
    send_out, aux_ref, send_ref, rt_ref, rgt_ref, tok_ref, cot_ref, rex_ref, one_ref, sems,
):
    tp = tp_ref[0]
    tok, dm = tok_ref.shape
    experts = rex_ref.shape[1]
    groups = rgt_ref.shape[0]
    gw = experts // groups
    width = dm // 4
    loads = [
        pltpu.make_async_copy(src, dst, sems.at[k])
        for k, (src, dst) in enumerate(
            ((rt_hbm, rt_ref), (tok_hbm, tok_ref), (rgt_hbm, rgt_ref), (rex_hbm, rex_ref), (cot_hbm, cot_ref))
        )
    ]
    for load in loads:
        load.start()
    loads[0].wait()
    r0, r1 = rt_ref[0:1, :], rt_ref[1:2, :]
    before = ones_where(iota((tok, tok), 0) < iota((tok, tok), 1))
    blk = min(256, experts * 8)
    blocks = experts * 8 // blk
    row = iota((blk, tok), 0)
    sub = row & 7
    want = (2 * tp + (sub & 1)).astype(F32)
    part = sub >> 1
    for b in range(blocks):
        rows = slice(b * blk, (b + 1) * blk)
        expert = b * (blk // 8) + (row >> 3)
        hit0 = r0 == expert
        hit1 = r1 == expert
        match = mm(ones_where(hit0 | hit1), before) == want
        one_ref[0, rows, :] = ones_where(hit0 & match)
        one_ref[1, rows, :] = ones_where(hit1 & match)

    def spread(sel):
        return jnp.concatenate([jnp.where(part == c, sel, 0.0).astype(BF) for c in range(4)], axis=1)

    def stacked(ref):
        return jnp.concatenate([ref[:, c * width : (c + 1) * width] for c in range(4)], axis=0)

    saves = []

    def save(k, rows, cols):
        saves.append(pltpu.make_async_copy(send_ref.at[rows, cols], send_out.at[rows, cols], sems.at[5 + k]))
        saves[-1].start()

    loads[1].wait()
    stack = stacked(tok_ref)
    for b in range(blocks):
        rows = slice(b * blk, (b + 1) * blk)
        one = one_ref[0, rows, :].astype(F32) + one_ref[1, rows, :].astype(F32)
        send_ref[rows, 0:width] = mm(spread(one), stack).astype(BF)
        save(2 * b, rows, slice(0, width))
    loads[2].wait()
    loads[3].wait()
    group_exp = jnp.exp(nt(rgt_ref[...], tok_ref[...]))
    group_prob = group_exp / jnp.sum(group_exp, axis=0, keepdims=True)
    logits = jnp.transpose(mm(tok_ref[...], rex_ref[...]))
    ei = iota((experts, tok), 0)
    l0 = jnp.sum(jnp.where(ei == r0, logits, 0.0), axis=0, keepdims=True)
    l1 = jnp.sum(jnp.where(ei == r1, logits, 0.0), axis=0, keepdims=True)
    x0, x1 = jnp.exp(l0), jnp.exp(l1)
    p0, p1 = x0 / (x0 + x1), x1 / (x0 + x1)
    chosen = r0 // gw
    gi = iota((groups, tok), 0)
    picked = jnp.sum(jnp.where(gi == chosen, group_prob, 0.0), axis=0, keepdims=True)
    w0 = (picked * p0).astype(BF).astype(F32)
    w1 = (picked * p1).astype(BF).astype(F32)
    arow = iota((EXTRA, tok), 0)
    aux = jnp.where(arow == 0, p0, jnp.where(arow == 1, p1, 0.0))
    for j in range(groups):
        aux = jnp.where(arow == 2 + j, group_prob[j : j + 1, :], aux)
    aux = jnp.where(arow == 6, r0.astype(F32), jnp.where(arow == 7, r1.astype(F32), aux))
    aux_ref[...] = aux
    loads[4].wait()
    stack = stacked(cot_ref)
    for b in range(blocks):
        rows = slice(b * blk, (b + 1) * blk)
        one0, one1 = one_ref[0, rows, :].astype(F32), one_ref[1, rows, :].astype(F32)
        send_ref[rows, width : 2 * width] = mm(spread(one0 * w0 + one1 * w1), stack).astype(BF)
        save(2 * b + 1, rows, slice(width, 2 * width))
    for copy in saves:
        copy.wait()


def pick_rows(outs, rows_in, stride, at):
    n = rows_in.shape[0] // stride
    for d, out_ref in enumerate(outs):
        want = iota((n, n * stride), 0) * stride + ((at + d) & (stride - 1))
        out_ref[...] = mm(ones_where(iota((n, n * stride), 1) == want), rows_in).astype(BF)


def mark_kernel(aux_ref, out_ref):
    out_ref[...] = jnp.transpose(aux_ref[...])


def side_x_kernel(groups, ep_ref, aux_ref, *outs):
    tok = aux_ref.shape[1]
    experts = outs[0].shape[0] * 4
    gw = experts // groups
    r0, r1 = aux_ref[6:7, :].astype(jnp.int32), aux_ref[7:8, :].astype(jnp.int32)
    ei = iota((experts, tok), 0)
    one0 = jnp.where(ei == r0, 1.0, 0.0)
    one1 = jnp.where(ei == r1, 1.0, 0.0)
    before = ones_where(iota((tok, tok), 0) < iota((tok, tok), 1))
    rank = mm((one0 + one1).astype(BF), before)
    li = iota((EXTRA, tok), 0)
    base = (r0 // gw) * gw
    shared = jnp.zeros((EXTRA, tok), F32)
    for j in range(groups):
        shared = jnp.where((li & 7) == 2 + j, aux_ref[2 + j : 3 + j, :], shared)
    kinds = []
    for other, prob in ((r1, aux_ref[1:2, :]), (r0, aux_ref[0:1, :])):
        kinds.append(
            jnp.where((li & 7) == 0, (other - base).astype(F32), jnp.where((li & 7) == 1, prob, shared))
        )
    total = None
    for r in range(4):
        for one, kind in ((one0, kinds[0]), (one1, kinds[1])):
            left = jnp.where(rank == float(r), one, 0.0).astype(BF)
            right = jnp.where((li >> 3) == r, kind, 0.0).astype(BF)
            term = nt(left, right)
            total = term if total is None else total + term
    pick_rows(outs, total.astype(BF), 4, ep_ref[0] & 3)


def side_y_kernel(ep_ref, a_ref, b_ref, c_ref, d_ref, *outs):
    rows = jnp.concatenate([a_ref[...], b_ref[...], c_ref[...], d_ref[...]], axis=0)
    pick_rows(outs, rows, 4, (ep_ref[0] >> 2) & 3)


def side_z_kernel(ep_ref, a_ref, b_ref, c_ref, d_ref, *outs):
    rows = jnp.concatenate([a_ref[...], b_ref[...], c_ref[...], d_ref[...]], axis=0)
    pick_rows(outs, rows, len(outs), ep_ref[0] >> 4)


def side_end_kernel(groups, ep_ref, tp_ref, *refs):
    ins, outs = refs[:-2], refs[-2:]
    rows = jnp.concatenate([ref[...] for ref in ins], axis=0)
    experts = rows.shape[0]
    planes = len(ins)
    gw = experts // groups
    e, tp = ep_ref[0], tp_ref[0]
    n = experts * 2
    src = iota((n, experts), 0) >> 1
    dz = ((e >> 4) - (src >> 4)) & (planes - 1)
    dy = ((e >> 2) - (src >> 2)) & 3
    dx = (e - src) & 3
    spread = mm(ones_where(iota((n, experts), 1) == dz * 16 + dy * 4 + dx), rows)
    lane = iota((n, EXTRA), 1)
    li = lane & (LOW_LANE - 1)
    chosen = e // gw
    own = jnp.where(li == e - chosen * gw, 1.0, 0.0)
    mark = jnp.where(li == GROUP_LANE + chosen, 1.0, 0.0)
    for p, out_ref in enumerate(outs):
        slot = 2 * ((tp + p) & 1) + (iota((n, EXTRA), 0) & 1)

        def value(v):
            return jnp.sum(jnp.where(lane == slot * 8 + v, spread, 0.0), axis=1, keepdims=True)

        z = value(1) * (own - jnp.where(li.astype(F32) == value(0), 1.0, 0.0)) + mark
        for j in range(groups):
            z = z - jnp.where(li == GROUP_LANE + j, value(2 + j), 0.0)
        out_ref[...] = z.astype(BF)


def expert_kernel(load, tp_ref, got_ref, *refs):
    tp = tp_ref[0]
    weights, refs = refs[:3], refs[3:]
    u_ref, mine_ref, theirs_ref, x_ref, x_out, sc_out, gd_out, ud_out, hid_out = refs[:9]
    sc_ref, gd_ref, ud_ref, hid_ref, sems = refs[-5:]
    gate_ref = weights[0]
    up_ref, down_ref = refs[9:11] if load else weights[1:]
    loads = []
    if load:
        loads = [
            pltpu.make_async_copy(src, dst, sems.at[5 + k])
            for k, (src, dst) in enumerate(zip(weights[1:], (up_ref, down_ref)))
        ]
        for copy in loads:
            copy.start()
    dm = gate_ref.shape[0]
    width, half = dm // 4, dm // 2
    blk = min(256, got_ref.shape[0])
    n4 = blk // 4
    shift = n4.bit_length() - 1
    o, i = iota((blk, blk), 0), iota((blk, blk), 1)
    perm = ones_where(i == ((o & (n4 - 1)) >> 1) * 8 + (o >> shift) * 2 + (o & 1))
    for b in range(got_ref.shape[0] // blk):
        block = slice(b * blk, (b + 1) * blk)
        rows = slice(b * n4, (b + 1) * n4)
        y = mm(perm, got_ref[block, 0 : 2 * width]).astype(BF)
        for c in range(4):
            cols = slice(c * width, (c + 1) * width)
            x_ref[rows, cols] = y[c * n4 : (c + 1) * n4, 0:width]
            sc_ref[rows, cols] = y[c * n4 : (c + 1) * n4, width:]
    saves = [
        pltpu.make_async_copy(src, dst, sems.at[k])
        for k, (src, dst) in enumerate(
            ((x_ref, x_out), (sc_ref, sc_out), (gd_ref, gd_out), (ud_ref, ud_out), (hid_ref, hid_out))
        )
    ]
    gp = mm(x_ref[...], gate_ref[...])
    for copy in loads:
        copy.wait()
    saves[0].start()
    saves[1].start()
    upre = mm(x_ref[...], up_ref[...])
    pulled = nt(sc_ref[...], down_ref[...])
    sig = 1.0 / (1.0 + jnp.exp(-gp))
    act = gp * sig
    hid = (act * upre).astype(BF)
    hid_ref[...] = hid
    u = jnp.sum(pulled * hid.astype(F32), axis=1, keepdims=True)
    gd = (pulled * (upre * sig * (1.0 + gp * (1.0 - sig)))).astype(BF)
    ud = (pulled * act).astype(BF)
    gd_ref[...] = gd
    ud_ref[...] = ud
    for save in saves[2:]:
        save.start()
    n = x_ref.shape[0]
    u_ref[...] = jnp.broadcast_to(u, (n, EXTRA))
    high = u.astype(BF).astype(F32)
    lane = iota((n, EXTRA), 1)
    theirs_ref[:, half:] = jnp.where(lane == 0, high, jnp.where(lane == 1, u - high, 0.0)).astype(BF)
    far = pl.ds(pl.multiple_of((1 - tp) * half, half), half)
    theirs_ref[:, 0:half] = (nt(gd, gate_ref[far, :]) + nt(ud, up_ref[far, :])).astype(BF)
    near = pl.ds(pl.multiple_of(tp * half, half), half)
    mine_ref[...] = (nt(gd, gate_ref[near, :]) + nt(ud, up_ref[near, :])).astype(BF)
    for save in saves:
        save.wait()


def pack_kernel(tp_ref, *refs):
    tp = tp_ref[0]
    mine, came, us, zs, xs = refs[0:2], refs[2:4], refs[4:6], refs[6:8], refs[8:10]
    ret_out, ret_ref, y0_ref, y1_ref, ul_ref, sems = refs[10:16]
    saves = []
    n, half = mine[0].shape
    width = half // 2
    lane = iota((n, EXTRA), 1)
    for p, y_ref in ((0, y0_ref), (1, y1_ref)):
        u = us[p][...] + came[p][:, half : half + 1].astype(F32) + came[p][:, half + 1 : half + 2].astype(F32)
        y_ref[...] = (u * zs[p][...].astype(F32)).astype(BF)
        ul_ref[p * n : (p + 1) * n, :] = jnp.where(lane == U_LANE, u, 0.0).astype(BF)
    blk = min(256, n * 4)
    bs = blk // 8
    o, i = iota((blk, blk), 0), iota((blk, blk), 1)
    perm = ones_where(i == ((o >> 2) & 1) * (4 * bs) + ((o >> 1) & 1) * (2 * bs) + (o >> 3) * 2 + (o & 1))
    wide = iota((blk, EXTRA), 1) < LOW_LANE
    for b in range(n // (2 * bs)):
        rows = slice(b * 2 * bs, (b + 1) * 2 * bs)
        out = slice(b * blk, (b + 1) * blk)
        sums = [(mine[p][rows, :].astype(F32) + came[p][rows, 0:half].astype(F32)).astype(BF) for p in range(2)]
        stack = jnp.concatenate(
            [sums[0][:, 0:width], sums[1][:, 0:width], sums[0][:, width:], sums[1][:, width:]], axis=0
        )
        ret_ref[out, 0:width] = mm(perm, stack).astype(BF)
        ulane = jnp.concatenate([ul_ref[rows, :], ul_ref[n + b * 2 * bs : n + (b + 1) * 2 * bs, :]], axis=0)
        base = mm(perm[:, 0 : 4 * bs], ulane)
        cols = slice(b * 16 * bs, (b + 1) * 16 * bs)
        rc = tn(xs[0][:, cols], y0_ref[...]) + tn(xs[1][:, cols], y1_ref[...])
        rc = rc.reshape(bs, 16, EXTRA)
        rc = jnp.where(tp == 0, rc[:, 0:8, :], rc[:, 8:16, :]).reshape(blk, EXTRA)
        high = rc.astype(BF).astype(F32)
        ret_ref[out, width:] = (base + jnp.where(wide, high, rc - high)).astype(BF)
        saves.append(pltpu.make_async_copy(ret_ref.at[out, :], ret_out.at[out, :], sems.at[b]))
        saves[-1].start()
    for save in saves:
        save.wait()


def grads_kernel(*refs):
    x, sc, gd, ud, hid = (refs[2 * k : 2 * k + 2] for k in range(5))
    gate_ref, up_ref, down_ref, sq_ref, down_sq_ref, acc_ref = refs[10:]
    dm, _ = gate_ref.shape
    blk = 128
    wide = 512 if dm % 512 == 0 else 128

    def as_row(col):
        return jnp.transpose(jnp.broadcast_to(col, (col.shape[0], 128)))[0:1, :]

    def step(b, carry):
        cols = pl.ds(pl.multiple_of(b * blk, blk), blk)
        for k, (delta, out_ref) in enumerate(((gd, gate_ref), (ud, up_ref))):
            full = tn(x[0][:, cols], delta[0][...]) + tn(x[1][:, cols], delta[1][...])
            out_ref[cols, :] = full.astype(BF)
            sq_ref[k : k + 1, cols] = as_row(jnp.sum(full * full, axis=1, keepdims=True))
        return carry

    lax.fori_loop(0, dm // blk, step, 0)
    acc_ref[...] = jnp.zeros_like(acc_ref)

    def down_step(b, carry):
        cols = pl.ds(pl.multiple_of(b * wide, wide), wide)
        full = tn(hid[0][...], sc[0][:, cols]) + tn(hid[1][...], sc[1][:, cols])
        down_ref[:, cols] = full.astype(BF)
        acc_ref[...] += jnp.broadcast_to(jnp.sum(full * full, axis=1, keepdims=True), acc_ref.shape)
        return carry

    lax.fori_loop(0, dm // wide, down_step, 0)
    down_sq_ref[...] = jnp.transpose(acc_ref[...])[0:1, :]


def home_kernel(tp_ref, aux_ref, rg_ref, rex_ref, sel_ref, q_ref, h_ref):
    tp = tp_ref[0]
    tok = aux_ref.shape[0]
    half = q_ref.shape[1]
    groups = rg_ref.shape[0]
    experts = rex_ref.shape[1]
    gw = experts // groups
    r0, r1 = aux_ref[:, 6:7].astype(jnp.int32), aux_ref[:, 7:8].astype(jnp.int32)
    n = experts * 8
    col = iota((tok, n), 1)
    hit0 = r0 == (col >> 3)
    hit1 = r1 == (col >> 3)
    earlier = ones_where(iota((tok, tok), 1) < iota((tok, tok), 0))
    rank = mm(earlier, ones_where(hit0 | hit1))
    match = rank == ((2 * tp + (col & 3)) & 3).astype(F32)
    lower = (col & 4) == 0
    one0 = jnp.where(hit0 & match, 1.0, 0.0)
    one1 = jnp.where(hit1 & match, 1.0, 0.0)
    sel_ref[0] = jnp.where(lower, one0, 0.0).astype(BF)
    sel_ref[1] = jnp.where(lower, one1, 0.0).astype(BF)
    sel_ref[2] = jnp.where(lower, one0 + one1, 0.0).astype(BF)
    sel_ref[3] = jnp.where(lower, 0.0, one0 + one1).astype(BF)
    ei = iota((tok, experts), 1)
    pick = (jnp.where(ei == r0, 1.0, 0.0) - jnp.where(ei == r1, 1.0, 0.0)).astype(BF)
    near = pl.ds(pl.multiple_of(tp * half, half), half)
    q_ref[...] = nt(pick, rex_ref[near, :])
    h = None
    for j in range(groups):
        side = jnp.where(r0 // gw == j, 1.0, 0.0) - aux_ref[:, 2 + j : 3 + j]
        term = side * rg_ref[pl.ds(j, 1), near].astype(F32)
        h = term if j == 0 else h + term
    h_ref[...] = h


def final_kernel(
    back_ref, sel_ref, aux_ref, q_ref, h_ref, sq_ref, sqo_ref,
    tg_ref, rex_ref, rg_ref, rows_ref, gate_sq_ref, up_sq_ref,
):
    gate_sq_ref[...] = sq_ref[0:1, :] + sqo_ref[0:1, :]
    up_sq_ref[...] = sq_ref[1:2, :] + sqo_ref[1:2, :]
    width = back_ref.shape[1] - EXTRA
    experts = rex_ref.shape[1]
    groups = rg_ref.shape[0]
    gw = experts // groups
    extra = back_ref[:, width:]
    u0 = mm(sel_ref[0], extra)[:, U_LANE : U_LANE + 1]
    u1 = mm(sel_ref[1], extra)[:, U_LANE : U_LANE + 1]
    lean = aux_ref[:, 1:2] * u0 - aux_ref[:, 0:1] * u1
    both = u0 + u1
    for c in range(2):
        cols = slice(c * width, (c + 1) * width)
        part = mm(sel_ref[2 + c], back_ref[:, 0:width])
        tg_ref[:, cols] = (part + (both * h_ref[:, cols] + lean * q_ref[:, cols])).astype(BF)
    sums = jnp.sum(extra.astype(F32).reshape(groups, gw, 8, EXTRA), axis=1)
    rg = None
    square = None
    lane = iota((8, EXTRA), 1)
    for g in range(groups):
        s = sums[g]
        s = s + jnp.concatenate([s[:, LOW_LANE:], s[:, 0:LOW_LANE]], axis=1)
        rex = s[:, 0:gw]
        rex_ref[:, g * gw : (g + 1) * gw] = rex
        rg = s if g == 0 else rg + s
        sq = jnp.sum(rex * rex, axis=1, keepdims=True)
        square = sq if g == 0 else square + sq
    grp = rg[:, GROUP_LANE : GROUP_LANE + groups]
    square = square + jnp.sum(grp * grp, axis=1, keepdims=True)
    rest = jnp.transpose(jnp.where(lane == GROUP_LANE + groups, square, rg))
    rg_ref[...] = rest[GROUP_LANE : GROUP_LANE + groups, :]
    rows_ref[...] = rest[GROUP_LANE + groups : GROUP_LANE + groups + 1, :]


def body(tokens, cotangent, routes, router_group, router_expert, gate_proj, up_proj, down_proj):
    tok, dm = tokens.shape
    experts = router_expert.shape[1]
    groups = router_group.shape[1]
    width, half = dm // 4, dm // 2
    ff = gate_proj.shape[2]
    n = experts * 2
    tp = lax.axis_index("tp").reshape(1)
    swap = [(0, 1), (1, 0)]
    rgt = router_group.T
    ep = lax.axis_index("ep")
    planes = experts // 16
    idx = [ep.reshape(1), tp]
    gate, up, down = gate_proj[0], up_proj[0], down_proj[0]

    def exchange(x):
        m = x.shape[1]
        y = lax.all_to_all(x.reshape(experts, 8, m), "ep", split_axis=0, concat_axis=0, tiled=True)
        return y.reshape(experts * 8, m)

    def partner(x):
        return lax.ppermute(x, "tp", swap)

    def shift(v, stride, d):
        size = planes if stride == 16 else 4
        pairs = []
        for e in range(experts):
            at = e // stride % size
            pairs.append((e, e + ((at + d) % size - at) * stride))
        return lax.ppermute(v, "ep", pairs)

    send, aux = call(
        pre_kernel, 1 << 30, 20,
        [((experts * 8, 2 * width), BF), ((EXTRA, tok), F32)],
        idx, [far(routes.T), far(rgt), far(tokens), far(cotangent), far(router_expert)],
        scratch=[
            pltpu.VMEM((experts * 8, 2 * width), BF), pltpu.VMEM((2, tok), jnp.int32), pltpu.VMEM((groups, dm), BF),
            pltpu.VMEM((tok, dm), BF), pltpu.VMEM((tok, dm), BF), pltpu.VMEM((dm, experts), BF),
            pltpu.VMEM((2, experts * 8, tok), BF), pltpu.SemaphoreType.DMA((13,)),
        ],
        spaces=[HB] * 5,
        out_spaces=[HB, VM],
    )
    got = exchange(send)
    sides = call(
        functools.partial(side_x_kernel, groups), 1 << 28, 6,
        [((experts // 4, EXTRA), BF)] * 4, idx[:1], [aux],
    )
    sides = [shift(v, 1, d) if d else v for d, v in enumerate(sides)]
    sides = call(side_y_kernel, 1 << 24, 6, [((experts // 4, EXTRA), BF)] * 4, idx[:1], sides)
    sides = [shift(v, 4, d) if d else v for d, v in enumerate(sides)]
    sides = call(side_z_kernel, 1 << 24, 6, [((16, EXTRA), BF)] * planes, idx[:1], sides)
    sides = [shift(v, 16, d) if d else v for d, v in enumerate(sides)]
    (aux_cols,) = call(mark_kernel, 1 << 20, 4, [((tok, EXTRA), F32)], [], [aux])
    z = call(functools.partial(side_end_kernel, groups), 1 << 24, 6, [((n, EXTRA), BF)] * 2, idx, sides)
    other = partner(got)

    def expert(g, weights, load):
        held = [((dm, ff), BF), ((ff, dm), BF)] if load else []
        return call(
            functools.partial(expert_kernel, load), 3 << 30, 18,
            [((n, EXTRA), F32), ((n, half), BF), ((n, half + EXTRA), BF), ((n, dm), BF),
             ((n, dm), BF), ((n, dm), BF), ((n, ff), BF), ((n, ff), BF), ((n, ff), BF)] + held,
            [tp], [g, *weights],
            scratch=[pltpu.VMEM((n, w), BF) for w in (dm, ff, ff, ff)] + [pltpu.SemaphoreType.DMA((8,))],
            spaces=[VM] * 2 + [HB if load else VM] * 2,
            out_spaces=[VM] * 4 + [HB] * 5 + [VM] * len(held),
        )

    first = expert(got, [gate, far(up), far(down)], True)
    second = expert(other, [gate, *first[9:]], False)
    u, mine, theirs, xv, x, sc, gd, ud, hid = [list(v) for v in zip(first[:9], second)]
    came = [partner(theirs[1]), partner(theirs[0])]
    (ret,) = call(
        pack_kernel, 1 << 29, 16, [((experts * 8, width + EXTRA), BF)],
        [tp], [*mine, *came, *u, *z, *xv],
        scratch=[
            pltpu.VMEM((experts * 8, width + EXTRA), BF), pltpu.VMEM((n, EXTRA), BF), pltpu.VMEM((n, EXTRA), BF),
            pltpu.VMEM((2 * n, EXTRA), BF), pltpu.SemaphoreType.DMA((4,)),
        ],
        out_spaces=[HB],
    )
    back = exchange(ret)
    gate_grad, up_grad, down_grad, sq, down_sq = call(
        grads_kernel, 3 << 30, 20,
        [((dm, ff), BF), ((dm, ff), BF), ((ff, dm), BF), ((2, dm), F32), ((1, ff), F32)],
        [], [*x, *sc, *gd, *ud, *hid], scratch=[pltpu.VMEM((ff, 128), F32)],
    )
    sq_other = partner(sq)
    sel, q, h = call(
        home_kernel, 1 << 29, 8,
        [((4, tok, experts * 8), BF), ((tok, half), F32), ((tok, half), F32)],
        [tp], [aux_cols, rgt, router_expert],
    )
    token_grad, rex_grad, rg_grad, rows, gate_sq, up_sq = call(
        final_kernel, 1 << 29, 10,
        [((tok, half), BF), ((8, experts), F32), ((groups, 8), F32), ((1, 8), F32),
         ((1, dm), F32), ((1, dm), F32)],
        [], [back, sel, aux_cols, q, h, sq, sq_other],
    )
    return (
        token_grad,
        gate_grad[None],
        up_grad[None],
        down_grad[None],
        gate_sq,
        up_sq,
        down_sq,
        rex_grad,
        rg_grad.T,
        rows[0],
    )


def solution(mesh):
    return jax.shard_map(
        body,
        mesh=mesh,
        in_specs=(
            P("ep", None),
            P("ep", None),
            P("ep", None),
            P(),
            P(),
            P("ep", None, "tp"),
            P("ep", None, "tp"),
            P("ep", "tp", None),
        ),
        out_specs=(
            P("ep", "tp"),
            P("ep", None, "tp"),
            P("ep", None, "tp"),
            P("ep", "tp", None),
            P("ep", None),
            P("ep", None),
            P("ep", "tp"),
            P(("ep", "tp"), None),
            P(("ep", "tp"), None),
            P(("ep", "tp")),
        ),
        check_vma=False,
    )
```

```python
import functools

import jax
import jax.numpy as jnp
from jax import lax
from jax.experimental import pallas as pl
from jax.experimental.pallas import tpu as pltpu
from jax.sharding import PartitionSpec as P


BF = jnp.bfloat16
F32 = jnp.float32
GROUP_LANE = 32
U_LANE = 40
LOW_LANE = 64
EXTRA = 128


def mm(a, b):
    return lax.dot_general(a, b, (((1,), (0,)), ((), ())), preferred_element_type=F32)


def nt(a, b):
    return lax.dot_general(a, b, (((1,), (1,)), ((), ())), preferred_element_type=F32)


def tn(a, b):
    return lax.dot_general(a, b, (((0,), (0,)), ((), ())), preferred_element_type=F32)


def iota(shape, dim):
    return lax.broadcasted_iota(jnp.int32, shape, dim)


VM = pl.BlockSpec(memory_space=pltpu.VMEM)
HB = pl.BlockSpec(memory_space=pltpu.HBM)


def far(x):
    return pltpu.with_memory_space_constraint(x, pltpu.HBM)


def call(kernel, flops, limit, outs, scalars, arrays, scratch=(), spaces=None, out_spaces=None):
    smem = pl.BlockSpec(memory_space=pltpu.SMEM)
    vmem = pl.BlockSpec(memory_space=pltpu.VMEM)
    return pl.pallas_call(
        kernel,
        out_shape=[
            pltpu.HBM(shape, dtype) if out_spaces and out_spaces[k] is HB else jax.ShapeDtypeStruct(shape, dtype)
            for k, (shape, dtype) in enumerate(outs)
        ],
        in_specs=[smem] * len(scalars) + (spaces or [vmem] * len(arrays)),
        out_specs=out_spaces or [vmem] * len(outs),
        scratch_shapes=list(scratch),
        cost_estimate=pl.CostEstimate(flops=flops, bytes_accessed=4 << 20, transcendentals=0),
        compiler_params=pltpu.CompilerParams(vmem_limit_bytes=limit << 20),
    )(*scalars, *arrays)


def ones_where(mask):
    return jnp.where(mask, 1.0, 0.0).astype(BF)


def pre_kernel(
    ep_ref, tp_ref, rt_hbm, rgt_hbm, tok_hbm, cot_hbm, rex_hbm,
    send_out, aux_ref, send_ref, sel_ref, rt_ref, rgt_ref, tok_ref, cot_ref, rex_ref, one_ref, sems,
):
    tp = tp_ref[0]
    tok, dm = tok_ref.shape
    experts = rex_ref.shape[1]
    groups = rgt_ref.shape[0]
    gw = experts // groups
    width = dm // 4
    loads = [
        pltpu.make_async_copy(src, dst, sems.at[k])
        for k, (src, dst) in enumerate(
            ((rt_hbm, rt_ref), (tok_hbm, tok_ref), (rgt_hbm, rgt_ref), (rex_hbm, rex_ref), (cot_hbm, cot_ref))
        )
    ]
    for load in loads:
        load.start()
    loads[0].wait()
    r0, r1 = rt_ref[0:1, :], rt_ref[1:2, :]
    before = ones_where(iota((tok, tok), 0) < iota((tok, tok), 1))
    blk = min(256, experts * 8)
    blocks = experts * 8 // blk
    row = iota((blk, tok), 0)
    sub = row & 7
    want = (2 * tp + (sub & 1)).astype(F32)
    part = sub >> 1
    for b in range(blocks):
        rows = slice(b * blk, (b + 1) * blk)
        expert = b * (blk // 8) + (row >> 3)
        hit0 = r0 == expert
        hit1 = r1 == expert
        match = mm(ones_where(hit0 | hit1), before) == want
        one_ref[0, rows, :] = ones_where(hit0 & match)
        one_ref[1, rows, :] = ones_where(hit1 & match)

    def spread(sel):
        return jnp.concatenate([jnp.where(part == c, sel, 0.0).astype(BF) for c in range(4)], axis=1)

    def stacked(ref):
        return jnp.concatenate([ref[:, c * width : (c + 1) * width] for c in range(4)], axis=0)

    saves = []

    def save(k, rows, cols):
        saves.append(pltpu.make_async_copy(send_ref.at[rows, cols], send_out.at[rows, cols], sems.at[5 + k]))
        saves[-1].start()

    loads[1].wait()
    stack = stacked(tok_ref)
    for b in range(blocks):
        rows = slice(b * blk, (b + 1) * blk)
        one = one_ref[0, rows, :].astype(F32) + one_ref[1, rows, :].astype(F32)
        sel_ref[rows, :] = spread(one)
        send_ref[rows, 0:width] = mm(sel_ref[rows, :], stack).astype(BF)
        save(2 * b, rows, slice(0, width))
    loads[2].wait()
    loads[3].wait()
    group_exp = jnp.exp(nt(rgt_ref[...], tok_ref[...]))
    group_prob = group_exp / jnp.sum(group_exp, axis=0, keepdims=True)
    logits = jnp.transpose(mm(tok_ref[...], rex_ref[...]))
    ei = iota((experts, tok), 0)
    l0 = jnp.sum(jnp.where(ei == r0, logits, 0.0), axis=0, keepdims=True)
    l1 = jnp.sum(jnp.where(ei == r1, logits, 0.0), axis=0, keepdims=True)
    x0, x1 = jnp.exp(l0), jnp.exp(l1)
    p0, p1 = x0 / (x0 + x1), x1 / (x0 + x1)
    chosen = r0 // gw
    gi = iota((groups, tok), 0)
    picked = jnp.sum(jnp.where(gi == chosen, group_prob, 0.0), axis=0, keepdims=True)
    w0 = (picked * p0).astype(BF).astype(F32)
    w1 = (picked * p1).astype(BF).astype(F32)
    arow = iota((EXTRA, tok), 0)
    aux = jnp.where(arow == 0, p0, jnp.where(arow == 1, p1, 0.0))
    for j in range(groups):
        aux = jnp.where(arow == 2 + j, group_prob[j : j + 1, :], aux)
    aux = jnp.where(arow == 6, r0.astype(F32), jnp.where(arow == 7, r1.astype(F32), aux))
    aux_ref[...] = aux
    loads[4].wait()
    stack = stacked(cot_ref)
    for b in range(blocks):
        rows = slice(b * blk, (b + 1) * blk)
        one0, one1 = one_ref[0, rows, :].astype(F32), one_ref[1, rows, :].astype(F32)
        scale = jnp.sum(one0 * w0 + one1 * w1, axis=1, keepdims=True)
        send_ref[rows, width : 2 * width] = (mm(sel_ref[rows, :], stack) * scale).astype(BF)
        save(2 * b + 1, rows, slice(width, 2 * width))
    for copy in saves:
        copy.wait()


def pick_rows(outs, rows_in, stride, at):
    n = rows_in.shape[0] // stride
    for d, out_ref in enumerate(outs):
        want = iota((n, n * stride), 0) * stride + ((at + d) & (stride - 1))
        out_ref[...] = mm(ones_where(iota((n, n * stride), 1) == want), rows_in).astype(BF)


def mark_kernel(aux_ref, out_ref):
    out_ref[...] = jnp.transpose(aux_ref[...])


def side_x_kernel(groups, ep_ref, aux_ref, *outs):
    tok = aux_ref.shape[1]
    experts = outs[0].shape[0] * 4
    gw = experts // groups
    r0, r1 = aux_ref[6:7, :].astype(jnp.int32), aux_ref[7:8, :].astype(jnp.int32)
    ei = iota((experts, tok), 0)
    one0 = jnp.where(ei == r0, 1.0, 0.0)
    one1 = jnp.where(ei == r1, 1.0, 0.0)
    before = ones_where(iota((tok, tok), 0) < iota((tok, tok), 1))
    rank = mm((one0 + one1).astype(BF), before)
    li = iota((EXTRA, tok), 0)
    base = (r0 // gw) * gw
    shared = jnp.zeros((EXTRA, tok), F32)
    for j in range(groups):
        shared = jnp.where((li & 7) == 2 + j, aux_ref[2 + j : 3 + j, :], shared)
    kinds = []
    for other, prob in ((r1, aux_ref[1:2, :]), (r0, aux_ref[0:1, :])):
        kinds.append(
            jnp.where((li & 7) == 0, (other - base).astype(F32), jnp.where((li & 7) == 1, prob, shared))
        )
    total = None
    for r in range(4):
        for one, kind in ((one0, kinds[0]), (one1, kinds[1])):
            left = jnp.where(rank == float(r), one, 0.0).astype(BF)
            right = jnp.where((li >> 3) == r, kind, 0.0).astype(BF)
            term = nt(left, right)
            total = term if total is None else total + term
    pick_rows(outs, total.astype(BF), 4, ep_ref[0] & 3)


def side_y_kernel(ep_ref, a_ref, b_ref, c_ref, d_ref, *outs):
    rows = jnp.concatenate([a_ref[...], b_ref[...], c_ref[...], d_ref[...]], axis=0)
    pick_rows(outs, rows, 4, (ep_ref[0] >> 2) & 3)


def side_z_kernel(ep_ref, a_ref, b_ref, c_ref, d_ref, *outs):
    rows = jnp.concatenate([a_ref[...], b_ref[...], c_ref[...], d_ref[...]], axis=0)
    pick_rows(outs, rows, len(outs), ep_ref[0] >> 4)


def side_end_kernel(groups, ep_ref, tp_ref, *refs):
    ins, outs = refs[:-2], refs[-2:]
    rows = jnp.concatenate([ref[...] for ref in ins], axis=0)
    experts = rows.shape[0]
    planes = len(ins)
    gw = experts // groups
    e, tp = ep_ref[0], tp_ref[0]
    n = experts * 2
    src = iota((n, experts), 0) >> 1
    dz = ((e >> 4) - (src >> 4)) & (planes - 1)
    dy = ((e >> 2) - (src >> 2)) & 3
    dx = (e - src) & 3
    spread = mm(ones_where(iota((n, experts), 1) == dz * 16 + dy * 4 + dx), rows)
    lane = iota((n, EXTRA), 1)
    li = lane & (LOW_LANE - 1)
    chosen = e // gw
    own = jnp.where(li == e - chosen * gw, 1.0, 0.0)
    mark = jnp.where(li == GROUP_LANE + chosen, 1.0, 0.0)
    for p, out_ref in enumerate(outs):
        slot = 2 * ((tp + p) & 1) + (iota((n, EXTRA), 0) & 1)

        def value(v):
            return jnp.sum(jnp.where(lane == slot * 8 + v, spread, 0.0), axis=1, keepdims=True)

        z = value(1) * (own - jnp.where(li.astype(F32) == value(0), 1.0, 0.0)) + mark
        for j in range(groups):
            z = z - jnp.where(li == GROUP_LANE + j, value(2 + j), 0.0)
        out_ref[...] = z.astype(BF)


def expert_kernel(load, tp_ref, got_ref, *refs):
    tp = tp_ref[0]
    weights, refs = refs[:3], refs[3:]
    u_ref, mine_ref, theirs_ref, x_ref, x_out, sc_out, gd_out, ud_out, hid_out = refs[:9]
    sc_ref, gd_ref, ud_ref, hid_ref, sems = refs[-5:]
    gate_ref = weights[0]
    up_ref, down_ref = refs[9:11] if load else weights[1:]
    loads = []
    if load:
        loads = [
            pltpu.make_async_copy(src, dst, sems.at[5 + k])
            for k, (src, dst) in enumerate(zip(weights[1:], (up_ref, down_ref)))
        ]
        for copy in loads:
            copy.start()
    dm = gate_ref.shape[0]
    width, half = dm // 4, dm // 2
    blk = min(256, got_ref.shape[0])
    n4 = blk // 4
    shift = n4.bit_length() - 1
    o, i = iota((blk, blk), 0), iota((blk, blk), 1)
    perm = ones_where(i == ((o & (n4 - 1)) >> 1) * 8 + (o >> shift) * 2 + (o & 1))
    for b in range(got_ref.shape[0] // blk):
        block = slice(b * blk, (b + 1) * blk)
        rows = slice(b * n4, (b + 1) * n4)
        y = mm(perm, got_ref[block, 0 : 2 * width]).astype(BF)
        for c in range(4):
            cols = slice(c * width, (c + 1) * width)
            x_ref[rows, cols] = y[c * n4 : (c + 1) * n4, 0:width]
            sc_ref[rows, cols] = y[c * n4 : (c + 1) * n4, width:]
    saves = [
        pltpu.make_async_copy(src, dst, sems.at[k])
        for k, (src, dst) in enumerate(
            ((x_ref, x_out), (sc_ref, sc_out), (gd_ref, gd_out), (ud_ref, ud_out), (hid_ref, hid_out))
        )
    ]
    if not load:
        saves[0].start()
        saves[1].start()
    gp = mm(x_ref[...], gate_ref[...])
    if load:
        loads[0].wait()
    upre = mm(x_ref[...], up_ref[...])
    if load:
        loads[1].wait()
        saves[0].start()
        saves[1].start()
    pulled = nt(sc_ref[...], down_ref[...])
    sig = 1.0 / (1.0 + jnp.exp(-gp))
    act = gp * sig
    hid = (act * upre).astype(BF)
    hid_ref[...] = hid
    u = jnp.sum(pulled * hid.astype(F32), axis=1, keepdims=True)
    gd = (pulled * (upre * sig * (1.0 + gp * (1.0 - sig)))).astype(BF)
    ud = (pulled * act).astype(BF)
    gd_ref[...] = gd
    ud_ref[...] = ud
    for save in saves[2:]:
        save.start()
    n = x_ref.shape[0]
    u_ref[...] = jnp.broadcast_to(u, (n, EXTRA))
    high = u.astype(BF).astype(F32)
    lane = iota((n, EXTRA), 1)
    theirs_ref[:, half:] = jnp.where(lane == 0, high, jnp.where(lane == 1, u - high, 0.0)).astype(BF)
    far = pl.ds(pl.multiple_of((1 - tp) * half, half), half)
    theirs_ref[:, 0:half] = (nt(gd, gate_ref[far, :]) + nt(ud, up_ref[far, :])).astype(BF)
    near = pl.ds(pl.multiple_of(tp * half, half), half)
    mine_ref[...] = (nt(gd, gate_ref[near, :]) + nt(ud, up_ref[near, :])).astype(BF)
    for save in saves:
        save.wait()


def summed(u_ref, came_ref):
    half = came_ref.shape[1] - EXTRA
    return u_ref[...] + came_ref[:, half : half + 1].astype(F32) + came_ref[:, half + 1 : half + 2].astype(F32)


def router_terms(tp, x_ref, y_ref, b, bs):
    cols = slice(b * 16 * bs, (b + 1) * 16 * bs)
    rc = tn(x_ref[:, cols], y_ref[...]).reshape(bs, 16, EXTRA)
    return jnp.where(tp == 0, rc[:, 0:8, :], rc[:, 8:16, :]).reshape(bs * 8, EXTRA)


def early_kernel(tp_ref, came_ref, u_ref, z_ref, x_ref, rc_ref, ul_ref, y_ref):
    tp = tp_ref[0]
    n = u_ref.shape[0]
    u = summed(u_ref, came_ref)
    y_ref[...] = (u * z_ref[...].astype(F32)).astype(BF)
    ul_ref[...] = jnp.where(iota((n, EXTRA), 1) == U_LANE, u, 0.0).astype(BF)
    bs = min(32, n // 2)
    for b in range(n // (2 * bs)):
        rc_ref[b * bs * 8 : (b + 1) * bs * 8, :] = router_terms(tp, x_ref, y_ref, b, bs)


def pack_kernel(tp_ref, *refs):
    tp = tp_ref[0]
    mine, came = refs[0:2], refs[2:4]
    u_ref, z_ref, x_ref, rc1_ref, ul1_ref, ret_out, ret_ref, y_ref, ul_ref, sems = refs[4:14]
    saves = []
    n, half = mine[0].shape
    width = half // 2
    u = summed(u_ref, came[0])
    y_ref[...] = (u * z_ref[...].astype(F32)).astype(BF)
    ul_ref[...] = jnp.where(iota((n, EXTRA), 1) == U_LANE, u, 0.0).astype(BF)
    blk = min(256, n * 4)
    bs = blk // 8
    o, i = iota((blk, blk), 0), iota((blk, blk), 1)
    perm = ones_where(i == ((o >> 2) & 1) * (4 * bs) + ((o >> 1) & 1) * (2 * bs) + (o >> 3) * 2 + (o & 1))
    wide = iota((blk, EXTRA), 1) < LOW_LANE
    for b in range(n // (2 * bs)):
        rows = slice(b * 2 * bs, (b + 1) * 2 * bs)
        out = slice(b * blk, (b + 1) * blk)
        sums = [(mine[p][rows, :].astype(F32) + came[p][rows, 0:half].astype(F32)).astype(BF) for p in range(2)]
        stack = jnp.concatenate(
            [sums[0][:, 0:width], sums[1][:, 0:width], sums[0][:, width:], sums[1][:, width:]], axis=0
        )
        ret_ref[out, 0:width] = mm(perm, stack).astype(BF)
        ulane = jnp.concatenate([ul_ref[rows, :], ul1_ref[rows, :]], axis=0)
        base = mm(perm[:, 0 : 4 * bs], ulane)
        rc = router_terms(tp, x_ref, y_ref, b, bs) + rc1_ref[out, :]
        high = rc.astype(BF).astype(F32)
        ret_ref[out, width:] = (base + jnp.where(wide, high, rc - high)).astype(BF)
        saves.append(pltpu.make_async_copy(ret_ref.at[out, :], ret_out.at[out, :], sems.at[b]))
        saves[-1].start()
    for save in saves:
        save.wait()


def grads_kernel(*refs):
    x, sc, gd, ud, hid = (refs[2 * k : 2 * k + 2] for k in range(5))
    gate_ref, up_ref, down_ref, sq_ref, down_sq_ref, acc_ref = refs[10:]
    dm, _ = gate_ref.shape
    blk = 128
    wide = 512 if dm % 512 == 0 else 128

    def as_row(col):
        return jnp.transpose(jnp.broadcast_to(col, (col.shape[0], 128)))[0:1, :]

    def step(b, carry):
        cols = pl.ds(pl.multiple_of(b * blk, blk), blk)
        for k, (delta, out_ref) in enumerate(((gd, gate_ref), (ud, up_ref))):
            full = tn(x[0][:, cols], delta[0][...]) + tn(x[1][:, cols], delta[1][...])
            out_ref[cols, :] = full.astype(BF)
            sq_ref[k : k + 1, cols] = as_row(jnp.sum(full * full, axis=1, keepdims=True))
        return carry

    lax.fori_loop(0, dm // blk, step, 0)
    acc_ref[...] = jnp.zeros_like(acc_ref)

    def down_step(b, carry):
        cols = pl.ds(pl.multiple_of(b * wide, wide), wide)
        full = tn(hid[0][...], sc[0][:, cols]) + tn(hid[1][...], sc[1][:, cols])
        down_ref[:, cols] = full.astype(BF)
        acc_ref[...] += jnp.broadcast_to(jnp.sum(full * full, axis=1, keepdims=True), acc_ref.shape)
        return carry

    lax.fori_loop(0, dm // wide, down_step, 0)
    down_sq_ref[...] = jnp.transpose(acc_ref[...])[0:1, :]


def home_kernel(tp_ref, aux_ref, rg_ref, rex_ref, sel_ref, q_ref, h_ref):
    tp = tp_ref[0]
    tok = aux_ref.shape[0]
    half = q_ref.shape[1]
    groups = rg_ref.shape[0]
    experts = rex_ref.shape[1]
    gw = experts // groups
    r0, r1 = aux_ref[:, 6:7].astype(jnp.int32), aux_ref[:, 7:8].astype(jnp.int32)
    n = experts * 8
    col = iota((tok, n), 1)
    hit0 = r0 == (col >> 3)
    hit1 = r1 == (col >> 3)
    earlier = ones_where(iota((tok, tok), 1) < iota((tok, tok), 0))
    rank = mm(earlier, ones_where(hit0 | hit1))
    match = rank == ((2 * tp + (col & 3)) & 3).astype(F32)
    lower = (col & 4) == 0
    one0 = jnp.where(hit0 & match, 1.0, 0.0)
    one1 = jnp.where(hit1 & match, 1.0, 0.0)
    sel_ref[0] = jnp.where(lower, one0, 0.0).astype(BF)
    sel_ref[1] = jnp.where(lower, one1, 0.0).astype(BF)
    sel_ref[2] = jnp.where(lower, one0 + one1, 0.0).astype(BF)
    sel_ref[3] = jnp.where(lower, 0.0, one0 + one1).astype(BF)
    ei = iota((tok, experts), 1)
    pick = (jnp.where(ei == r0, 1.0, 0.0) - jnp.where(ei == r1, 1.0, 0.0)).astype(BF)
    near = pl.ds(pl.multiple_of(tp * half, half), half)
    q_ref[...] = nt(pick, rex_ref[near, :])
    h = None
    for j in range(groups):
        side = jnp.where(r0 // gw == j, 1.0, 0.0) - aux_ref[:, 2 + j : 3 + j]
        term = side * rg_ref[pl.ds(j, 1), near].astype(F32)
        h = term if j == 0 else h + term
    h_ref[...] = h


def final_kernel(
    back_ref, sel_ref, aux_ref, q_ref, h_ref, sq_ref, sqo_ref,
    tg_ref, rex_ref, rg_ref, rows_ref, gate_sq_ref, up_sq_ref,
):
    gate_sq_ref[...] = sq_ref[0:1, :] + sqo_ref[0:1, :]
    up_sq_ref[...] = sq_ref[1:2, :] + sqo_ref[1:2, :]
    width = back_ref.shape[1] - EXTRA
    experts = rex_ref.shape[1]
    groups = rg_ref.shape[0]
    gw = experts // groups
    extra = back_ref[:, width:]
    u0 = mm(sel_ref[0], extra)[:, U_LANE : U_LANE + 1]
    u1 = mm(sel_ref[1], extra)[:, U_LANE : U_LANE + 1]
    lean = aux_ref[:, 1:2] * u0 - aux_ref[:, 0:1] * u1
    both = u0 + u1
    for c in range(2):
        cols = slice(c * width, (c + 1) * width)
        part = mm(sel_ref[2 + c], back_ref[:, 0:width])
        tg_ref[:, cols] = (part + (both * h_ref[:, cols] + lean * q_ref[:, cols])).astype(BF)
    sums = jnp.sum(extra.astype(F32).reshape(groups, gw, 8, EXTRA), axis=1)
    rg = None
    square = None
    lane = iota((8, EXTRA), 1)
    for g in range(groups):
        s = sums[g]
        s = s + jnp.concatenate([s[:, LOW_LANE:], s[:, 0:LOW_LANE]], axis=1)
        rex = s[:, 0:gw]
        rex_ref[:, g * gw : (g + 1) * gw] = rex
        rg = s if g == 0 else rg + s
        sq = jnp.sum(rex * rex, axis=1, keepdims=True)
        square = sq if g == 0 else square + sq
    grp = rg[:, GROUP_LANE : GROUP_LANE + groups]
    square = square + jnp.sum(grp * grp, axis=1, keepdims=True)
    rest = jnp.transpose(jnp.where(lane == GROUP_LANE + groups, square, rg))
    rg_ref[...] = rest[GROUP_LANE : GROUP_LANE + groups, :]
    rows_ref[...] = rest[GROUP_LANE + groups : GROUP_LANE + groups + 1, :]


def body(tokens, cotangent, routes, router_group, router_expert, gate_proj, up_proj, down_proj):
    tok, dm = tokens.shape
    experts = router_expert.shape[1]
    groups = router_group.shape[1]
    width, half = dm // 4, dm // 2
    ff = gate_proj.shape[2]
    n = experts * 2
    tp = lax.axis_index("tp").reshape(1)
    swap = [(0, 1), (1, 0)]
    rgt = router_group.T
    ep = lax.axis_index("ep")
    planes = experts // 16
    idx = [ep.reshape(1), tp]
    gate, up, down = gate_proj[0], up_proj[0], down_proj[0]

    def exchange(x):
        m = x.shape[1]
        y = lax.all_to_all(x.reshape(experts, 8, m), "ep", split_axis=0, concat_axis=0, tiled=True)
        return y.reshape(experts * 8, m)

    def partner(x):
        return lax.ppermute(x, "tp", swap)

    def shift(v, stride, d):
        size = planes if stride == 16 else 4
        pairs = []
        for e in range(experts):
            at = e // stride % size
            pairs.append((e, e + ((at + d) % size - at) * stride))
        return lax.ppermute(v, "ep", pairs)

    send, aux = call(
        pre_kernel, 1 << 30, 20,
        [((experts * 8, 2 * width), BF), ((EXTRA, tok), F32)],
        idx, [far(routes.T), far(rgt), far(tokens), far(cotangent), far(router_expert)],
        scratch=[
            pltpu.VMEM((experts * 8, 2 * width), BF), pltpu.VMEM((experts * 8, 4 * tok), BF),
            pltpu.VMEM((2, tok), jnp.int32), pltpu.VMEM((groups, dm), BF),
            pltpu.VMEM((tok, dm), BF), pltpu.VMEM((tok, dm), BF), pltpu.VMEM((dm, experts), BF),
            pltpu.VMEM((2, experts * 8, tok), BF), pltpu.SemaphoreType.DMA((13,)),
        ],
        spaces=[HB] * 5,
        out_spaces=[HB, VM],
    )
    got = exchange(send)
    sides = call(
        functools.partial(side_x_kernel, groups), 1 << 28, 6,
        [((experts // 4, EXTRA), BF)] * 4, idx[:1], [aux],
    )
    sides = [shift(v, 1, d) if d else v for d, v in enumerate(sides)]
    sides = call(side_y_kernel, 1 << 24, 6, [((experts // 4, EXTRA), BF)] * 4, idx[:1], sides)
    sides = [shift(v, 4, d) if d else v for d, v in enumerate(sides)]
    sides = call(side_z_kernel, 1 << 24, 6, [((16, EXTRA), BF)] * planes, idx[:1], sides)
    sides = [shift(v, 16, d) if d else v for d, v in enumerate(sides)]
    (aux_cols,) = call(mark_kernel, 1 << 20, 4, [((tok, EXTRA), F32)], [], [aux])
    z = call(functools.partial(side_end_kernel, groups), 1 << 24, 6, [((n, EXTRA), BF)] * 2, idx, sides)
    other = partner(got)

    def expert(g, weights, load):
        held = [((dm, ff), BF), ((ff, dm), BF)] if load else []
        return call(
            functools.partial(expert_kernel, load), 3 << 30, 18,
            [((n, EXTRA), F32), ((n, half), BF), ((n, half + EXTRA), BF), ((n, dm), BF),
             ((n, dm), BF), ((n, dm), BF), ((n, ff), BF), ((n, ff), BF), ((n, ff), BF)] + held,
            [tp], [g, *weights],
            scratch=[pltpu.VMEM((n, w), BF) for w in (dm, ff, ff, ff)] + [pltpu.SemaphoreType.DMA((8,))],
            spaces=[VM] * 2 + [HB if load else VM] * 2,
            out_spaces=[VM] * 4 + [HB] * 5 + [VM] * len(held),
        )

    first = expert(got, [gate, far(up), far(down)], True)
    second = expert(other, [gate, *first[9:]], False)
    u, mine, theirs, xv, x, sc, gd, ud, hid = [list(v) for v in zip(first[:9], second)]
    came = [partner(theirs[1]), partner(theirs[0])]
    rc1, ul1 = call(
        early_kernel, 1 << 28, 8, [((experts * 8, EXTRA), F32), ((n, EXTRA), BF)],
        [tp], [came[1], u[1], z[1], xv[1]], scratch=[pltpu.VMEM((n, EXTRA), BF)],
    )
    (ret,) = call(
        pack_kernel, 1 << 29, 16, [((experts * 8, width + EXTRA), BF)],
        [tp], [*mine, *came, u[0], z[0], xv[0], rc1, ul1],
        scratch=[
            pltpu.VMEM((experts * 8, width + EXTRA), BF), pltpu.VMEM((n, EXTRA), BF), pltpu.VMEM((n, EXTRA), BF),
            pltpu.SemaphoreType.DMA((4,)),
        ],
        out_spaces=[HB],
    )
    back = exchange(ret)
    gate_grad, up_grad, down_grad, sq, down_sq = call(
        grads_kernel, 3 << 30, 20,
        [((dm, ff), BF), ((dm, ff), BF), ((ff, dm), BF), ((2, dm), F32), ((1, ff), F32)],
        [], [*x, *sc, *gd, *ud, *hid], scratch=[pltpu.VMEM((ff, 128), F32)],
    )
    sq_other = partner(sq)
    sel, q, h = call(
        home_kernel, 1 << 29, 8,
        [((4, tok, experts * 8), BF), ((tok, half), F32), ((tok, half), F32)],
        [tp], [aux_cols, rgt, router_expert],
    )
    token_grad, rex_grad, rg_grad, rows, gate_sq, up_sq = call(
        final_kernel, 1 << 29, 10,
        [((tok, half), BF), ((8, experts), F32), ((groups, 8), F32), ((1, 8), F32),
         ((1, dm), F32), ((1, dm), F32)],
        [], [back, sel, aux_cols, q, h, sq, sq_other],
    )
    return (
        token_grad,
        gate_grad[None],
        up_grad[None],
        down_grad[None],
        gate_sq,
        up_sq,
        down_sq,
        rex_grad,
        rg_grad.T,
        rows[0],
    )


def solution(mesh):
    return jax.shard_map(
        body,
        mesh=mesh,
        in_specs=(
            P("ep", None),
            P("ep", None),
            P("ep", None),
            P(),
            P(),
            P("ep", None, "tp"),
            P("ep", None, "tp"),
            P("ep", "tp", None),
        ),
        out_specs=(
            P("ep", "tp"),
            P("ep", None, "tp"),
            P("ep", None, "tp"),
            P("ep", "tp", None),
            P("ep", None),
            P("ep", None),
            P("ep", "tp"),
            P(("ep", "tp"), None),
            P(("ep", "tp"), None),
            P(("ep", "tp")),
        ),
        check_vma=False,
    )
```

```python
import functools

import jax
import jax.numpy as jnp
from jax import lax
from jax.experimental import pallas as pl
from jax.experimental.pallas import tpu as pltpu
from jax.sharding import PartitionSpec as P


BF = jnp.bfloat16
F32 = jnp.float32
GROUP_LANE = 32
U_LANE = 40
LOW_LANE = 64
EXTRA = 128


def mm(a, b):
    return lax.dot_general(a, b, (((1,), (0,)), ((), ())), preferred_element_type=F32)


def nt(a, b):
    return lax.dot_general(a, b, (((1,), (1,)), ((), ())), preferred_element_type=F32)


def tn(a, b):
    return lax.dot_general(a, b, (((0,), (0,)), ((), ())), preferred_element_type=F32)


def iota(shape, dim):
    return lax.broadcasted_iota(jnp.int32, shape, dim)


VM = pl.BlockSpec(memory_space=pltpu.VMEM)
HB = pl.BlockSpec(memory_space=pltpu.HBM)


def far(x):
    return pltpu.with_memory_space_constraint(x, pltpu.HBM)


def call(kernel, flops, limit, outs, scalars, arrays, scratch=(), spaces=None, out_spaces=None):
    smem = pl.BlockSpec(memory_space=pltpu.SMEM)
    vmem = pl.BlockSpec(memory_space=pltpu.VMEM)
    return pl.pallas_call(
        kernel,
        out_shape=[
            pltpu.HBM(shape, dtype) if out_spaces and out_spaces[k] is HB else jax.ShapeDtypeStruct(shape, dtype)
            for k, (shape, dtype) in enumerate(outs)
        ],
        in_specs=[smem] * len(scalars) + (spaces or [vmem] * len(arrays)),
        out_specs=out_spaces or [vmem] * len(outs),
        scratch_shapes=list(scratch),
        cost_estimate=pl.CostEstimate(flops=flops, bytes_accessed=4 << 20, transcendentals=0),
        compiler_params=pltpu.CompilerParams(vmem_limit_bytes=limit << 20),
    )(*scalars, *arrays)


def ones_where(mask):
    return jnp.where(mask, 1.0, 0.0).astype(BF)


def pre_kernel(
    ep_ref, tp_ref, rt_hbm, rgt_hbm, tok_hbm, cot_hbm, rex_hbm,
    send_out, aux_ref, send_ref, rt_ref, rgt_ref, tok_ref, cot_ref, rex_ref, one_ref, sems,
):
    tp = tp_ref[0]
    tok, dm = tok_ref.shape
    experts = rex_ref.shape[1]
    groups = rgt_ref.shape[0]
    gw = experts // groups
    width = dm // 4
    loads = [
        pltpu.make_async_copy(src, dst, sems.at[k])
        for k, (src, dst) in enumerate(
            ((rt_hbm, rt_ref), (tok_hbm, tok_ref), (rgt_hbm, rgt_ref), (rex_hbm, rex_ref), (cot_hbm, cot_ref))
        )
    ]
    for load in loads:
        load.start()
    loads[0].wait()
    r0, r1 = rt_ref[0:1, :], rt_ref[1:2, :]
    before = ones_where(iota((tok, tok), 0) < iota((tok, tok), 1))
    n = experts * 2
    row = iota((n, tok), 0)
    hit0 = r0 == (row >> 1)
    hit1 = r1 == (row >> 1)
    match = mm(ones_where(hit0 | hit1), before) == (2 * tp + (row & 1)).astype(F32)
    one0 = jnp.where(hit0 & match, 1.0, 0.0)
    one1 = jnp.where(hit1 & match, 1.0, 0.0)
    one_ref[...] = (one0 + one1).astype(BF)
    saves = []

    def place(k, first, rows):
        cols = pl.ds(first + k * width, width)
        send_ref[:, :, cols] = rows.astype(BF).reshape(experts, 2, width)
        saves.append(pltpu.make_async_copy(send_ref.at[:, :, cols], send_out.at[:, :, cols], sems.at[5 + len(saves)]))
        saves[-1].start()

    loads[1].wait()
    for c in range(4):
        place(c, 0, mm(one_ref[...], tok_ref[:, c * width : (c + 1) * width]))
    loads[2].wait()
    loads[3].wait()
    group_exp = jnp.exp(nt(rgt_ref[...], tok_ref[...]))
    group_prob = group_exp / jnp.sum(group_exp, axis=0, keepdims=True)
    logits = jnp.transpose(mm(tok_ref[...], rex_ref[...]))
    ei = iota((experts, tok), 0)
    l0 = jnp.sum(jnp.where(ei == r0, logits, 0.0), axis=0, keepdims=True)
    l1 = jnp.sum(jnp.where(ei == r1, logits, 0.0), axis=0, keepdims=True)
    x0, x1 = jnp.exp(l0), jnp.exp(l1)
    p0, p1 = x0 / (x0 + x1), x1 / (x0 + x1)
    chosen = r0 // gw
    gi = iota((groups, tok), 0)
    picked = jnp.sum(jnp.where(gi == chosen, group_prob, 0.0), axis=0, keepdims=True)
    w0 = (picked * p0).astype(BF).astype(F32)
    w1 = (picked * p1).astype(BF).astype(F32)
    arow = iota((EXTRA, tok), 0)
    aux = jnp.where(arow == 0, p0, jnp.where(arow == 1, p1, 0.0))
    for j in range(groups):
        aux = jnp.where(arow == 2 + j, group_prob[j : j + 1, :], aux)
    aux = jnp.where(arow == 6, r0.astype(F32), jnp.where(arow == 7, r1.astype(F32), aux))
    aux_ref[...] = aux
    loads[4].wait()
    scale = jnp.sum(one0 * w0 + one1 * w1, axis=1, keepdims=True)
    for c in range(4):
        place(c, dm, mm(one_ref[...], cot_ref[:, c * width : (c + 1) * width]) * scale)
    for copy in saves:
        copy.wait()


def pick_rows(outs, rows_in, stride, at):
    n = rows_in.shape[0] // stride
    for d, out_ref in enumerate(outs):
        want = iota((n, n * stride), 0) * stride + ((at + d) & (stride - 1))
        out_ref[...] = mm(ones_where(iota((n, n * stride), 1) == want), rows_in).astype(BF)


def mark_kernel(aux_ref, out_ref):
    out_ref[...] = jnp.transpose(aux_ref[...])


def side_x_kernel(groups, ep_ref, aux_ref, *outs):
    tok = aux_ref.shape[1]
    experts = outs[0].shape[0] * 4
    gw = experts // groups
    r0, r1 = aux_ref[6:7, :].astype(jnp.int32), aux_ref[7:8, :].astype(jnp.int32)
    ei = iota((experts, tok), 0)
    one0 = jnp.where(ei == r0, 1.0, 0.0)
    one1 = jnp.where(ei == r1, 1.0, 0.0)
    before = ones_where(iota((tok, tok), 0) < iota((tok, tok), 1))
    rank = mm((one0 + one1).astype(BF), before)
    li = iota((EXTRA, tok), 0)
    base = (r0 // gw) * gw
    shared = jnp.zeros((EXTRA, tok), F32)
    for j in range(groups):
        shared = jnp.where((li & 7) == 2 + j, aux_ref[2 + j : 3 + j, :], shared)
    kinds = []
    for other, prob in ((r1, aux_ref[1:2, :]), (r0, aux_ref[0:1, :])):
        kinds.append(
            jnp.where((li & 7) == 0, (other - base).astype(F32), jnp.where((li & 7) == 1, prob, shared))
        )
    total = None
    for r in range(4):
        for one, kind in ((one0, kinds[0]), (one1, kinds[1])):
            left = jnp.where(rank == float(r), one, 0.0).astype(BF)
            right = jnp.where((li >> 3) == r, kind, 0.0).astype(BF)
            term = nt(left, right)
            total = term if total is None else total + term
    pick_rows(outs, total.astype(BF), 4, ep_ref[0] & 3)


def side_y_kernel(ep_ref, a_ref, b_ref, c_ref, d_ref, *outs):
    rows = jnp.concatenate([a_ref[...], b_ref[...], c_ref[...], d_ref[...]], axis=0)
    pick_rows(outs, rows, 4, (ep_ref[0] >> 2) & 3)


def side_z_kernel(ep_ref, a_ref, b_ref, c_ref, d_ref, *outs):
    rows = jnp.concatenate([a_ref[...], b_ref[...], c_ref[...], d_ref[...]], axis=0)
    pick_rows(outs, rows, len(outs), ep_ref[0] >> 4)


def side_end_kernel(groups, ep_ref, tp_ref, *refs):
    ins, outs = refs[:-2], refs[-2:]
    rows = jnp.concatenate([ref[...] for ref in ins], axis=0)
    experts = rows.shape[0]
    planes = len(ins)
    gw = experts // groups
    e, tp = ep_ref[0], tp_ref[0]
    n = experts * 2
    src = iota((n, experts), 0) >> 1
    dz = ((e >> 4) - (src >> 4)) & (planes - 1)
    dy = ((e >> 2) - (src >> 2)) & 3
    dx = (e - src) & 3
    spread = mm(ones_where(iota((n, experts), 1) == dz * 16 + dy * 4 + dx), rows)
    lane = iota((n, EXTRA), 1)
    li = lane & (LOW_LANE - 1)
    chosen = e // gw
    own = jnp.where(li == e - chosen * gw, 1.0, 0.0)
    mark = jnp.where(li == GROUP_LANE + chosen, 1.0, 0.0)
    for p, out_ref in enumerate(outs):
        slot = 2 * ((tp + p) & 1) + (iota((n, EXTRA), 0) & 1)

        def value(v):
            return jnp.sum(jnp.where(lane == slot * 8 + v, spread, 0.0), axis=1, keepdims=True)

        z = value(1) * (own - jnp.where(li.astype(F32) == value(0), 1.0, 0.0)) + mark
        for j in range(groups):
            z = z - jnp.where(li == GROUP_LANE + j, value(2 + j), 0.0)
        out_ref[...] = z.astype(BF)


def expert_kernel(load, tp_ref, got_ref, *refs):
    tp = tp_ref[0]
    weights, refs = refs[:3], refs[3:]
    u_ref, mine_ref, theirs_ref, x_ref, x_out, sc_out, gd_out, ud_out, hid_out = refs[:9]
    sc_ref, gd_ref, ud_ref, hid_ref, sems = refs[-5:]
    gate_ref = weights[0]
    up_ref, down_ref = refs[9:11] if load else weights[1:]
    loads = []
    if load:
        loads = [
            pltpu.make_async_copy(src, dst, sems.at[5 + k])
            for k, (src, dst) in enumerate(zip(weights[1:], (up_ref, down_ref)))
        ]
        loads[0].start()
    dm = gate_ref.shape[0]
    half = dm // 2
    x_ref[...] = got_ref[:, :, 0:dm].reshape(x_ref.shape)
    sc_ref[...] = got_ref[:, :, dm:].reshape(sc_ref.shape)
    saves = [
        pltpu.make_async_copy(src, dst, sems.at[k])
        for k, (src, dst) in enumerate(
            ((x_ref, x_out), (sc_ref, sc_out), (gd_ref, gd_out), (ud_ref, ud_out), (hid_ref, hid_out))
        )
    ]
    if load:
        loads[1].start()
    else:
        saves[0].start()
        saves[1].start()
    gp = mm(x_ref[...], gate_ref[...])
    if load:
        loads[0].wait()
    upre = mm(x_ref[...], up_ref[...])
    if load:
        loads[1].wait()
        saves[0].start()
        saves[1].start()
    pulled = nt(sc_ref[...], down_ref[...])
    sig = 1.0 / (1.0 + jnp.exp(-gp))
    act = gp * sig
    hid = (act * upre).astype(BF)
    hid_ref[...] = hid
    u = jnp.sum(pulled * hid.astype(F32), axis=1, keepdims=True)
    gd = (pulled * (upre * sig * (1.0 + gp * (1.0 - sig)))).astype(BF)
    ud = (pulled * act).astype(BF)
    gd_ref[...] = gd
    ud_ref[...] = ud
    for save in saves[2:]:
        save.start()
    n = x_ref.shape[0]
    u_ref[...] = jnp.broadcast_to(u, (n, EXTRA))
    high = u.astype(BF).astype(F32)
    lane = iota((n, EXTRA), 1)
    theirs_ref[:, half:] = jnp.where(lane == 0, high, jnp.where(lane == 1, u - high, 0.0)).astype(BF)
    far = pl.ds(pl.multiple_of((1 - tp) * half, half), half)
    theirs_ref[:, 0:half] = (nt(gd, gate_ref[far, :]) + nt(ud, up_ref[far, :])).astype(BF)
    near = pl.ds(pl.multiple_of(tp * half, half), half)
    mine_ref[...] = (nt(gd, gate_ref[near, :]) + nt(ud, up_ref[near, :])).astype(BF)
    for save in saves:
        save.wait()


def summed(u_ref, came_ref):
    half = came_ref.shape[1] - EXTRA
    return u_ref[...] + came_ref[:, half : half + 1].astype(F32) + came_ref[:, half + 1 : half + 2].astype(F32)


def router_terms(tp, x_ref, y_ref, b, bs):
    cols = slice(b * 16 * bs, (b + 1) * 16 * bs)
    rc = tn(x_ref[:, cols], y_ref[...]).reshape(bs, 16, EXTRA)
    rc = jnp.where(tp == 0, rc[:, 0:8, :], rc[:, 8:16, :])
    return jnp.where(iota((bs, 4, EXTRA), 2) < LOW_LANE, rc[:, 0:4, :], rc[:, 4:8, :])


def early_kernel(tp_ref, came_ref, u_ref, z_ref, x_ref, rc_ref, ul_ref, y_ref):
    tp = tp_ref[0]
    n = u_ref.shape[0]
    u = summed(u_ref, came_ref)
    y_ref[...] = (u * z_ref[...].astype(F32)).astype(BF)
    ul_ref[...] = jnp.where(iota((n, EXTRA), 1) == U_LANE, u, 0.0)
    bs = min(32, n // 2)
    for b in range(n // (2 * bs)):
        rc_ref[b * bs : (b + 1) * bs] = router_terms(tp, x_ref, y_ref, b, bs)


def pack_kernel(tp_ref, *refs):
    tp = tp_ref[0]
    mine, came = refs[0:2], refs[2:4]
    u_ref, z_ref, x_ref, rc1_ref, ul1_ref, ret_out, ret_ref, y_ref, ul_ref, sems = refs[4:14]
    saves = []
    n, half = mine[0].shape
    u = summed(u_ref, came[0])
    y_ref[...] = (u * z_ref[...].astype(F32)).astype(BF)
    ul_ref[...] = jnp.where(iota((n, EXTRA), 1) == U_LANE, u, 0.0)
    bs = min(32, n // 2)
    for b in range(n // (2 * bs)):
        rows = slice(b * 2 * bs, (b + 1) * 2 * bs)
        out = slice(b * bs, (b + 1) * bs)
        rc = router_terms(tp, x_ref, y_ref, b, bs) + rc1_ref[out]
        for p, lanes in ((0, ul_ref), (1, ul1_ref)):
            total = (mine[p][rows, :].astype(F32) + came[p][rows, 0:half].astype(F32)).astype(BF)
            at = slice(2 * p, 2 * p + 2)
            ret_ref[out, at, 0:half] = total.reshape(bs, 2, half)
            ret_ref[out, at, half:] = (rc[:, at, :] + lanes[rows, :].reshape(bs, 2, EXTRA)).astype(BF)
        saves.append(pltpu.make_async_copy(ret_ref.at[out], ret_out.at[out], sems.at[b]))
        saves[-1].start()
    for save in saves:
        save.wait()


def grads_kernel(*refs):
    x, sc, gd, ud, hid = (refs[2 * k : 2 * k + 2] for k in range(5))
    gate_ref, up_ref, down_ref, sq_ref, down_sq_ref, acc_ref = refs[10:]
    dm, _ = gate_ref.shape
    blk = 128
    wide = 512 if dm % 512 == 0 else 128

    def as_row(col):
        return jnp.transpose(jnp.broadcast_to(col, (col.shape[0], 128)))[0:1, :]

    def step(b, carry):
        cols = pl.ds(pl.multiple_of(b * blk, blk), blk)
        for k, (delta, out_ref) in enumerate(((gd, gate_ref), (ud, up_ref))):
            full = tn(x[0][:, cols], delta[0][...]) + tn(x[1][:, cols], delta[1][...])
            out_ref[cols, :] = full.astype(BF)
            sq_ref[k : k + 1, cols] = as_row(jnp.sum(full * full, axis=1, keepdims=True))
        return carry

    lax.fori_loop(0, dm // blk, step, 0)
    acc_ref[...] = jnp.zeros_like(acc_ref)

    def down_step(b, carry):
        cols = pl.ds(pl.multiple_of(b * wide, wide), wide)
        full = tn(hid[0][...], sc[0][:, cols]) + tn(hid[1][...], sc[1][:, cols])
        down_ref[:, cols] = full.astype(BF)
        acc_ref[...] += jnp.broadcast_to(jnp.sum(full * full, axis=1, keepdims=True), acc_ref.shape)
        return carry

    lax.fori_loop(0, dm // wide, down_step, 0)
    down_sq_ref[...] = jnp.transpose(acc_ref[...])[0:1, :]


def home_kernel(tp_ref, aux_ref, rg_ref, rex_ref, sel_ref, q_ref, h_ref):
    tp = tp_ref[0]
    tok = aux_ref.shape[0]
    half = q_ref.shape[1]
    groups = rg_ref.shape[0]
    experts = rex_ref.shape[1]
    gw = experts // groups
    r0, r1 = aux_ref[:, 6:7].astype(jnp.int32), aux_ref[:, 7:8].astype(jnp.int32)
    n = experts * 4
    col = iota((tok, n), 1)
    hit0 = r0 == (col >> 2)
    hit1 = r1 == (col >> 2)
    earlier = ones_where(iota((tok, tok), 1) < iota((tok, tok), 0))
    rank = mm(earlier, ones_where(hit0 | hit1))
    match = rank == ((2 * tp + (col & 3)) & 3).astype(F32)
    sel_ref[0] = ones_where(hit0 & match)
    sel_ref[1] = ones_where(hit1 & match)
    ei = iota((tok, experts), 1)
    pick = (jnp.where(ei == r0, 1.0, 0.0) - jnp.where(ei == r1, 1.0, 0.0)).astype(BF)
    near = pl.ds(pl.multiple_of(tp * half, half), half)
    q_ref[...] = nt(pick, rex_ref[near, :])
    h = None
    for j in range(groups):
        side = jnp.where(r0 // gw == j, 1.0, 0.0) - aux_ref[:, 2 + j : 3 + j]
        term = side * rg_ref[pl.ds(j, 1), near].astype(F32)
        h = term if j == 0 else h + term
    h_ref[...] = h


def final_kernel(
    back_ref, sel_ref, aux_ref, q_ref, h_ref, sq_ref, sqo_ref,
    tg_ref, rex_ref, rg_ref, rows_ref, gate_sq_ref, up_sq_ref,
):
    gate_sq_ref[...] = sq_ref[0:1, :] + sqo_ref[0:1, :]
    up_sq_ref[...] = sq_ref[1:2, :] + sqo_ref[1:2, :]
    half = tg_ref.shape[1]
    width = half // 2
    experts = rex_ref.shape[1]
    groups = rg_ref.shape[0]
    gw = experts // groups
    slots = experts * 4
    extra3 = back_ref[:, :, half:]
    extra = extra3.reshape(slots, EXTRA)
    u0 = mm(sel_ref[0], extra)[:, U_LANE : U_LANE + 1]
    u1 = mm(sel_ref[1], extra)[:, U_LANE : U_LANE + 1]
    lean = aux_ref[:, 1:2] * u0 - aux_ref[:, 0:1] * u1
    both = u0 + u1
    sel = (sel_ref[0].astype(F32) + sel_ref[1].astype(F32)).astype(BF)
    for c in range(2):
        cols = slice(c * width, (c + 1) * width)
        part = mm(sel, back_ref[:, :, cols].reshape(slots, width))
        tg_ref[:, cols] = (part + (both * h_ref[:, cols] + lean * q_ref[:, cols])).astype(BF)
    sums = jnp.sum(extra3.astype(F32).reshape(groups, gw, 4, EXTRA), axis=1)
    rg = None
    square = None
    lane = iota((8, EXTRA), 1)
    for g in range(groups):
        s = sums[g]
        s = jnp.concatenate([s, jnp.concatenate([s[:, LOW_LANE:], s[:, 0:LOW_LANE]], axis=1)], axis=0)
        rex = s[:, 0:gw]
        rex_ref[:, g * gw : (g + 1) * gw] = rex
        rg = s if g == 0 else rg + s
        sq = jnp.sum(rex * rex, axis=1, keepdims=True)
        square = sq if g == 0 else square + sq
    grp = rg[:, GROUP_LANE : GROUP_LANE + groups]
    square = square + jnp.sum(grp * grp, axis=1, keepdims=True)
    rest = jnp.transpose(jnp.where(lane == GROUP_LANE + groups, square, rg))
    rg_ref[...] = rest[GROUP_LANE : GROUP_LANE + groups, :]
    rows_ref[...] = rest[GROUP_LANE + groups : GROUP_LANE + groups + 1, :]


def body(tokens, cotangent, routes, router_group, router_expert, gate_proj, up_proj, down_proj):
    tok, dm = tokens.shape
    experts = router_expert.shape[1]
    groups = router_group.shape[1]
    half = dm // 2
    ff = gate_proj.shape[2]
    n = experts * 2
    tp = lax.axis_index("tp").reshape(1)
    swap = [(0, 1), (1, 0)]
    rgt = router_group.T
    ep = lax.axis_index("ep")
    planes = experts // 16
    idx = [ep.reshape(1), tp]
    gate, up, down = gate_proj[0], up_proj[0], down_proj[0]

    def exchange(x):
        return lax.all_to_all(x, "ep", split_axis=0, concat_axis=0, tiled=True)

    def partner(x):
        return lax.ppermute(x, "tp", swap)

    def shift(v, stride, d):
        size = planes if stride == 16 else 4
        pairs = []
        for e in range(experts):
            at = e // stride % size
            pairs.append((e, e + ((at + d) % size - at) * stride))
        return lax.ppermute(v, "ep", pairs)

    send, aux = call(
        pre_kernel, 1 << 30, 20,
        [((experts, 2, 2 * dm), BF), ((EXTRA, tok), F32)],
        idx, [far(routes.T), far(rgt), far(tokens), far(cotangent), far(router_expert)],
        scratch=[
            pltpu.VMEM((experts, 2, 2 * dm), BF),
            pltpu.VMEM((2, tok), jnp.int32), pltpu.VMEM((groups, dm), BF),
            pltpu.VMEM((tok, dm), BF), pltpu.VMEM((tok, dm), BF), pltpu.VMEM((dm, experts), BF),
            pltpu.VMEM((n, tok), BF), pltpu.SemaphoreType.DMA((13,)),
        ],
        spaces=[HB] * 5,
        out_spaces=[HB, VM],
    )
    got = exchange(send)
    sides = call(
        functools.partial(side_x_kernel, groups), 1 << 28, 6,
        [((experts // 4, EXTRA), BF)] * 4, idx[:1], [aux],
    )
    sides = [shift(v, 1, d) if d else v for d, v in enumerate(sides)]
    sides = call(side_y_kernel, 1 << 24, 6, [((experts // 4, EXTRA), BF)] * 4, idx[:1], sides)
    sides = [shift(v, 4, d) if d else v for d, v in enumerate(sides)]
    sides = call(side_z_kernel, 1 << 24, 6, [((16, EXTRA), BF)] * planes, idx[:1], sides)
    sides = [shift(v, 16, d) if d else v for d, v in enumerate(sides)]
    (aux_cols,) = call(mark_kernel, 1 << 20, 4, [((tok, EXTRA), F32)], [], [aux])
    z = call(functools.partial(side_end_kernel, groups), 1 << 24, 6, [((n, EXTRA), BF)] * 2, idx, sides)
    other = partner(got)

    def expert(g, weights, load):
        held = [((dm, ff), BF), ((ff, dm), BF)] if load else []
        return call(
            functools.partial(expert_kernel, load), 3 << 30, 18,
            [((n, EXTRA), F32), ((n, half), BF), ((n, half + EXTRA), BF), ((n, dm), BF),
             ((n, dm), BF), ((n, dm), BF), ((n, ff), BF), ((n, ff), BF), ((n, ff), BF)] + held,
            [tp], [g, *weights],
            scratch=[pltpu.VMEM((n, w), BF) for w in (dm, ff, ff, ff)] + [pltpu.SemaphoreType.DMA((8,))],
            spaces=[VM] * 2 + [HB if load else VM] * 2,
            out_spaces=[VM] * 4 + [HB] * 5 + [VM] * len(held),
        )

    first = expert(got, [gate, far(up), far(down)], True)
    second = expert(other, [gate, *first[9:]], False)
    u, mine, theirs, xv, x, sc, gd, ud, hid = [list(v) for v in zip(first[:9], second)]
    came = [partner(theirs[1]), partner(theirs[0])]
    rc1, ul1 = call(
        early_kernel, 1 << 28, 8, [((experts, 4, EXTRA), F32), ((n, EXTRA), F32)],
        [tp], [came[1], u[1], z[1], xv[1]], scratch=[pltpu.VMEM((n, EXTRA), BF)],
    )
    (ret,) = call(
        pack_kernel, 1 << 29, 16, [((experts, 4, half + EXTRA), BF)],
        [tp], [*mine, *came, u[0], z[0], xv[0], rc1, ul1],
        scratch=[
            pltpu.VMEM((experts, 4, half + EXTRA), BF), pltpu.VMEM((n, EXTRA), BF), pltpu.VMEM((n, EXTRA), F32),
            pltpu.SemaphoreType.DMA((4,)),
        ],
        out_spaces=[HB],
    )
    back = exchange(ret)
    gate_grad, up_grad, down_grad, sq, down_sq = call(
        grads_kernel, 3 << 30, 20,
        [((dm, ff), BF), ((dm, ff), BF), ((ff, dm), BF), ((2, dm), F32), ((1, ff), F32)],
        [], [*x, *sc, *gd, *ud, *hid], scratch=[pltpu.VMEM((ff, 128), F32)],
    )
    sq_other = partner(sq)
    sel, q, h = call(
        home_kernel, 1 << 29, 8,
        [((2, tok, experts * 4), BF), ((tok, half), F32), ((tok, half), F32)],
        [tp], [aux_cols, rgt, router_expert],
    )
    token_grad, rex_grad, rg_grad, rows, gate_sq, up_sq = call(
        final_kernel, 1 << 29, 10,
        [((tok, half), BF), ((8, experts), F32), ((groups, 8), F32), ((1, 8), F32),
         ((1, dm), F32), ((1, dm), F32)],
        [], [back, sel, aux_cols, q, h, sq, sq_other],
    )
    return (
        token_grad,
        gate_grad[None],
        up_grad[None],
        down_grad[None],
        gate_sq,
        up_sq,
        down_sq,
        rex_grad,
        rg_grad.T,
        rows[0],
    )


def solution(mesh):
    return jax.shard_map(
        body,
        mesh=mesh,
        in_specs=(
            P("ep", None),
            P("ep", None),
            P("ep", None),
            P(),
            P(),
            P("ep", None, "tp"),
            P("ep", None, "tp"),
            P("ep", "tp", None),
        ),
        out_specs=(
            P("ep", "tp"),
            P("ep", None, "tp"),
            P("ep", None, "tp"),
            P("ep", "tp", None),
            P("ep", None),
            P("ep", None),
            P("ep", "tp"),
            P(("ep", "tp"), None),
            P(("ep", "tp"), None),
            P(("ep", "tp")),
        ),
        check_vma=False,
    )
```

```python
import functools

import jax
import jax.numpy as jnp
from jax import lax
from jax.experimental import pallas as pl
from jax.experimental.pallas import tpu as pltpu
from jax.sharding import PartitionSpec as P


BF = jnp.bfloat16
F32 = jnp.float32
GROUP_LANE = 32
U_LANE = 40
LOW_LANE = 64
EXTRA = 128


def mm(a, b):
    return lax.dot_general(a, b, (((1,), (0,)), ((), ())), preferred_element_type=F32)


def nt(a, b):
    return lax.dot_general(a, b, (((1,), (1,)), ((), ())), preferred_element_type=F32)


def tn(a, b):
    return lax.dot_general(a, b, (((0,), (0,)), ((), ())), preferred_element_type=F32)


def iota(shape, dim):
    return lax.broadcasted_iota(jnp.int32, shape, dim)


VM = pl.BlockSpec(memory_space=pltpu.VMEM)
HB = pl.BlockSpec(memory_space=pltpu.HBM)


def far(x):
    return pltpu.with_memory_space_constraint(x, pltpu.HBM)


def call(kernel, flops, limit, outs, scalars, arrays, scratch=(), spaces=None, out_spaces=None):
    smem = pl.BlockSpec(memory_space=pltpu.SMEM)
    vmem = pl.BlockSpec(memory_space=pltpu.VMEM)
    return pl.pallas_call(
        kernel,
        out_shape=[
            pltpu.HBM(shape, dtype) if out_spaces and out_spaces[k] is HB else jax.ShapeDtypeStruct(shape, dtype)
            for k, (shape, dtype) in enumerate(outs)
        ],
        in_specs=[smem] * len(scalars) + (spaces or [vmem] * len(arrays)),
        out_specs=out_spaces or [vmem] * len(outs),
        scratch_shapes=list(scratch),
        cost_estimate=pl.CostEstimate(flops=flops, bytes_accessed=4 << 20, transcendentals=0),
        compiler_params=pltpu.CompilerParams(vmem_limit_bytes=limit << 20),
    )(*scalars, *arrays)


def ones_where(mask):
    return jnp.where(mask, 1.0, 0.0).astype(BF)


def pre_kernel(
    ep_ref, tp_ref, rt_hbm, rgt_hbm, tok_hbm, cot_hbm, rex_hbm,
    send_out, aux_ref, send_ref, rt_ref, rgt_ref, tok_ref, cot_ref, rex_ref, one_ref, sems,
):
    tp = tp_ref[0]
    tok, dm = tok_ref.shape
    experts = rex_ref.shape[1]
    groups = rgt_ref.shape[0]
    gw = experts // groups
    width = dm // 4
    loads = [
        pltpu.make_async_copy(src, dst, sems.at[k])
        for k, (src, dst) in enumerate(
            ((rt_hbm, rt_ref), (tok_hbm, tok_ref), (rgt_hbm, rgt_ref), (rex_hbm, rex_ref), (cot_hbm, cot_ref))
        )
    ]
    for load in loads:
        load.start()
    loads[0].wait()
    r0, r1 = rt_ref[0:1, :], rt_ref[1:2, :]
    before = ones_where(iota((tok, tok), 0) < iota((tok, tok), 1))
    n = experts * 2
    row = iota((n, tok), 0)
    hit0 = r0 == (row >> 1)
    hit1 = r1 == (row >> 1)
    match = mm(ones_where(hit0 | hit1), before) == (2 * tp + (row & 1)).astype(F32)
    one0 = jnp.where(hit0 & match, 1.0, 0.0)
    one1 = jnp.where(hit1 & match, 1.0, 0.0)
    one_ref[...] = (one0 + one1).astype(BF)
    saves = []

    def place(k, first, rows):
        cols = pl.ds(first + k * width, width)
        send_ref[:, :, cols] = rows.astype(BF).reshape(experts, 2, width)
        saves.append(pltpu.make_async_copy(send_ref.at[:, :, cols], send_out.at[:, :, cols], sems.at[5 + len(saves)]))
        saves[-1].start()

    loads[1].wait()
    for c in range(4):
        place(c, 0, mm(one_ref[...], tok_ref[:, c * width : (c + 1) * width]))
    loads[2].wait()
    loads[3].wait()
    group_exp = jnp.exp(nt(rgt_ref[...], tok_ref[...]))
    group_prob = group_exp / jnp.sum(group_exp, axis=0, keepdims=True)
    logits = jnp.transpose(mm(tok_ref[...], rex_ref[...]))
    ei = iota((experts, tok), 0)
    l0 = jnp.sum(jnp.where(ei == r0, logits, 0.0), axis=0, keepdims=True)
    l1 = jnp.sum(jnp.where(ei == r1, logits, 0.0), axis=0, keepdims=True)
    x0, x1 = jnp.exp(l0), jnp.exp(l1)
    p0, p1 = x0 / (x0 + x1), x1 / (x0 + x1)
    chosen = r0 // gw
    gi = iota((groups, tok), 0)
    picked = jnp.sum(jnp.where(gi == chosen, group_prob, 0.0), axis=0, keepdims=True)
    w0 = (picked * p0).astype(BF).astype(F32)
    w1 = (picked * p1).astype(BF).astype(F32)
    arow = iota((EXTRA, tok), 0)
    aux = jnp.where(arow == 0, p0, jnp.where(arow == 1, p1, 0.0))
    for j in range(groups):
        aux = jnp.where(arow == 2 + j, group_prob[j : j + 1, :], aux)
    aux = jnp.where(arow == 6, r0.astype(F32), jnp.where(arow == 7, r1.astype(F32), aux))
    aux_ref[...] = aux
    loads[4].wait()
    scale = jnp.sum(one0 * w0 + one1 * w1, axis=1, keepdims=True)
    for c in range(4):
        place(c, dm, mm(one_ref[...], cot_ref[:, c * width : (c + 1) * width]) * scale)
    for copy in saves:
        copy.wait()


def pick_rows(outs, rows_in, stride, at):
    n = rows_in.shape[0] // stride
    for d, out_ref in enumerate(outs):
        want = iota((n, n * stride), 0) * stride + ((at + d) & (stride - 1))
        out_ref[...] = mm(ones_where(iota((n, n * stride), 1) == want), rows_in).astype(BF)


def mark_kernel(aux_ref, out_ref):
    out_ref[...] = jnp.transpose(aux_ref[...])


def side_x_kernel(groups, ep_ref, aux_ref, *outs):
    tok = aux_ref.shape[1]
    experts = outs[0].shape[0] * 4
    gw = experts // groups
    r0, r1 = aux_ref[6:7, :].astype(jnp.int32), aux_ref[7:8, :].astype(jnp.int32)
    ei = iota((experts, tok), 0)
    one0 = jnp.where(ei == r0, 1.0, 0.0)
    one1 = jnp.where(ei == r1, 1.0, 0.0)
    before = ones_where(iota((tok, tok), 0) < iota((tok, tok), 1))
    rank = mm((one0 + one1).astype(BF), before)
    li = iota((EXTRA, tok), 0)
    base = (r0 // gw) * gw
    shared = jnp.zeros((EXTRA, tok), F32)
    for j in range(groups):
        shared = jnp.where((li & 7) == 2 + j, aux_ref[2 + j : 3 + j, :], shared)
    kinds = []
    for other, prob in ((r1, aux_ref[1:2, :]), (r0, aux_ref[0:1, :])):
        kinds.append(
            jnp.where((li & 7) == 0, (other - base).astype(F32), jnp.where((li & 7) == 1, prob, shared))
        )
    total = None
    for r in range(4):
        for one, kind in ((one0, kinds[0]), (one1, kinds[1])):
            left = jnp.where(rank == float(r), one, 0.0).astype(BF)
            right = jnp.where((li >> 3) == r, kind, 0.0).astype(BF)
            term = nt(left, right)
            total = term if total is None else total + term
    pick_rows(outs, total.astype(BF), 4, ep_ref[0] & 3)


def side_y_kernel(ep_ref, a_ref, b_ref, c_ref, d_ref, *outs):
    rows = jnp.concatenate([a_ref[...], b_ref[...], c_ref[...], d_ref[...]], axis=0)
    pick_rows(outs, rows, 4, (ep_ref[0] >> 2) & 3)


def side_z_kernel(ep_ref, a_ref, b_ref, c_ref, d_ref, *outs):
    rows = jnp.concatenate([a_ref[...], b_ref[...], c_ref[...], d_ref[...]], axis=0)
    pick_rows(outs, rows, len(outs), ep_ref[0] >> 4)


def side_end_kernel(groups, ep_ref, tp_ref, *refs):
    ins, outs = refs[:-2], refs[-2:]
    rows = jnp.concatenate([ref[...] for ref in ins], axis=0)
    experts = rows.shape[0]
    planes = len(ins)
    gw = experts // groups
    e, tp = ep_ref[0], tp_ref[0]
    n = experts * 2
    src = iota((n, experts), 0) >> 1
    dz = ((e >> 4) - (src >> 4)) & (planes - 1)
    dy = ((e >> 2) - (src >> 2)) & 3
    dx = (e - src) & 3
    spread = mm(ones_where(iota((n, experts), 1) == dz * 16 + dy * 4 + dx), rows)
    lane = iota((n, EXTRA), 1)
    li = lane & (LOW_LANE - 1)
    chosen = e // gw
    own = jnp.where(li == e - chosen * gw, 1.0, 0.0)
    mark = jnp.where(li == GROUP_LANE + chosen, 1.0, 0.0)
    for p, out_ref in enumerate(outs):
        slot = 2 * ((tp + p) & 1) + (iota((n, EXTRA), 0) & 1)

        def value(v):
            return jnp.sum(jnp.where(lane == slot * 8 + v, spread, 0.0), axis=1, keepdims=True)

        z = value(1) * (own - jnp.where(li.astype(F32) == value(0), 1.0, 0.0)) + mark
        for j in range(groups):
            z = z - jnp.where(li == GROUP_LANE + j, value(2 + j), 0.0)
        out_ref[...] = z.astype(BF)


def expert_kernel(load, tp_ref, got_ref, *refs):
    tp = tp_ref[0]
    weights, refs = refs[:3], refs[3:]
    if load:
        gate_ref, up_ref, down_ref = refs[8:11]
        u_ref, mine_ref, theirs_ref, x_ref, sc_ref, gd_out, ud_out, hid_out = refs[:8]
        gd_ref, ud_ref, hid_ref, sems = refs[11:]
        loads = [
            pltpu.make_async_copy(src, dst, sems.at[3 + k])
            for k, (src, dst) in enumerate(zip(weights, (gate_ref, up_ref, down_ref)))
        ]
        loads[0].start()
        pairs = []
    else:
        gate_ref, up_ref, down_ref = weights
        x0_ref, sc0_ref = refs[:2]
        u_ref, mine_ref, theirs_ref, x_ref, gd_out, ud_out, hid_out, x0_out, sc0_out, x_out, sc_out = refs[2:13]
        sc_ref, gd_ref, ud_ref, hid_ref, sems = refs[13:]
        pairs = [(x0_ref, x0_out), (sc0_ref, sc0_out), (x_ref, x_out), (sc_ref, sc_out)]
    pairs = [(gd_ref, gd_out), (ud_ref, ud_out), (hid_ref, hid_out)] + pairs
    base = 6 if load else 0
    saves = [pltpu.make_async_copy(src, dst, sems.at[base + k]) for k, (src, dst) in enumerate(pairs)]
    dm = gate_ref.shape[0]
    half = dm // 2
    if not load:
        saves[3].start()
        saves[4].start()
    x_ref[...] = got_ref[:, :, 0:dm].reshape(x_ref.shape)
    if load:
        loads[1].start()
    sc_ref[...] = got_ref[:, :, dm:].reshape(sc_ref.shape)
    if load:
        loads[2].start()
        loads[0].wait()
    else:
        saves[5].start()
        saves[6].start()
    gp = mm(x_ref[...], gate_ref[...])
    if load:
        loads[1].wait()
    upre = mm(x_ref[...], up_ref[...])
    if load:
        loads[2].wait()
    pulled = nt(sc_ref[...], down_ref[...])
    sig = 1.0 / (1.0 + jnp.exp(-gp))
    act = gp * sig
    hid = (act * upre).astype(BF)
    hid_ref[...] = hid
    u = jnp.sum(pulled * hid.astype(F32), axis=1, keepdims=True)
    gd = (pulled * (upre * sig * (1.0 + gp * (1.0 - sig)))).astype(BF)
    ud = (pulled * act).astype(BF)
    gd_ref[...] = gd
    ud_ref[...] = ud
    for save in saves[:3]:
        save.start()
    n = x_ref.shape[0]
    u_ref[...] = jnp.broadcast_to(u, (n, EXTRA))
    high = u.astype(BF).astype(F32)
    lane = iota((n, EXTRA), 1)
    theirs_ref[:, half:] = jnp.where(lane == 0, high, jnp.where(lane == 1, u - high, 0.0)).astype(BF)
    far = pl.ds(pl.multiple_of((1 - tp) * half, half), half)
    theirs_ref[:, 0:half] = (nt(gd, gate_ref[far, :]) + nt(ud, up_ref[far, :])).astype(BF)
    near = pl.ds(pl.multiple_of(tp * half, half), half)
    mine_ref[...] = (nt(gd, gate_ref[near, :]) + nt(ud, up_ref[near, :])).astype(BF)
    for save in saves:
        save.wait()


def summed(u_ref, came_ref):
    half = came_ref.shape[1] - EXTRA
    return u_ref[...] + came_ref[:, half : half + 1].astype(F32) + came_ref[:, half + 1 : half + 2].astype(F32)


def router_terms(tp, x_ref, y_ref, b, bs):
    cols = slice(b * 16 * bs, (b + 1) * 16 * bs)
    rc = tn(x_ref[:, cols], y_ref[...]).reshape(bs, 16, EXTRA)
    rc = jnp.where(tp == 0, rc[:, 0:8, :], rc[:, 8:16, :])
    return jnp.where(iota((bs, 4, EXTRA), 2) < LOW_LANE, rc[:, 0:4, :], rc[:, 4:8, :])


def early_kernel(tp_ref, came_ref, u_ref, z_ref, x_ref, rc_ref, ul_ref, y_ref):
    tp = tp_ref[0]
    n = u_ref.shape[0]
    u = summed(u_ref, came_ref)
    y_ref[...] = (u * z_ref[...].astype(F32)).astype(BF)
    ul_ref[...] = jnp.where(iota((n, EXTRA), 1) == U_LANE, u, 0.0)
    bs = min(32, n // 2)
    for b in range(n // (2 * bs)):
        rc_ref[b * bs : (b + 1) * bs] = router_terms(tp, x_ref, y_ref, b, bs)


def pack_kernel(tp_ref, *refs):
    tp = tp_ref[0]
    mine, came = refs[0:2], refs[2:4]
    u_ref, z_ref, x_ref, rc1_ref, ul1_ref, ret_out, ret_ref, y_ref, ul_ref, sems = refs[4:14]
    saves = []
    n, half = mine[0].shape
    u = summed(u_ref, came[0])
    y_ref[...] = (u * z_ref[...].astype(F32)).astype(BF)
    ul_ref[...] = jnp.where(iota((n, EXTRA), 1) == U_LANE, u, 0.0)
    bs = min(32, n // 2)
    for b in range(n // (2 * bs)):
        rows = slice(b * 2 * bs, (b + 1) * 2 * bs)
        out = slice(b * bs, (b + 1) * bs)
        rc = router_terms(tp, x_ref, y_ref, b, bs) + rc1_ref[out]
        for p, lanes in ((0, ul_ref), (1, ul1_ref)):
            total = (mine[p][rows, :].astype(F32) + came[p][rows, 0:half].astype(F32)).astype(BF)
            at = slice(2 * p, 2 * p + 2)
            ret_ref[out, at, 0:half] = total.reshape(bs, 2, half)
            ret_ref[out, at, half:] = (rc[:, at, :] + lanes[rows, :].reshape(bs, 2, EXTRA)).astype(BF)
        saves.append(pltpu.make_async_copy(ret_ref.at[out], ret_out.at[out], sems.at[b]))
        saves[-1].start()
    for save in saves:
        save.wait()


def grads_kernel(*refs):
    x, sc, gd, ud, hid = (refs[2 * k : 2 * k + 2] for k in range(5))
    gate_ref, up_ref, down_ref, sq_ref, down_sq_ref, acc_ref = refs[10:]
    dm, _ = gate_ref.shape
    blk = 128
    wide = 512 if dm % 512 == 0 else 128

    def as_row(col):
        return jnp.transpose(jnp.broadcast_to(col, (col.shape[0], 128)))[0:1, :]

    def step(b, carry):
        cols = pl.ds(pl.multiple_of(b * blk, blk), blk)
        for k, (delta, out_ref) in enumerate(((gd, gate_ref), (ud, up_ref))):
            full = tn(x[0][:, cols], delta[0][...]) + tn(x[1][:, cols], delta[1][...])
            out_ref[cols, :] = full.astype(BF)
            sq_ref[k : k + 1, cols] = as_row(jnp.sum(full * full, axis=1, keepdims=True))
        return carry

    lax.fori_loop(0, dm // blk, step, 0)
    acc_ref[...] = jnp.zeros_like(acc_ref)

    def down_step(b, carry):
        cols = pl.ds(pl.multiple_of(b * wide, wide), wide)
        full = tn(hid[0][...], sc[0][:, cols]) + tn(hid[1][...], sc[1][:, cols])
        down_ref[:, cols] = full.astype(BF)
        acc_ref[...] += jnp.broadcast_to(jnp.sum(full * full, axis=1, keepdims=True), acc_ref.shape)
        return carry

    lax.fori_loop(0, dm // wide, down_step, 0)
    down_sq_ref[...] = jnp.transpose(acc_ref[...])[0:1, :]


def home_kernel(tp_ref, aux_ref, rg_ref, rex_ref, sel_ref, q_ref, h_ref):
    tp = tp_ref[0]
    tok = aux_ref.shape[0]
    half = q_ref.shape[1]
    groups = rg_ref.shape[0]
    experts = rex_ref.shape[1]
    gw = experts // groups
    r0, r1 = aux_ref[:, 6:7].astype(jnp.int32), aux_ref[:, 7:8].astype(jnp.int32)
    n = experts * 4
    col = iota((tok, n), 1)
    hit0 = r0 == (col >> 2)
    hit1 = r1 == (col >> 2)
    earlier = ones_where(iota((tok, tok), 1) < iota((tok, tok), 0))
    rank = mm(earlier, ones_where(hit0 | hit1))
    match = rank == ((2 * tp + (col & 3)) & 3).astype(F32)
    sel_ref[0] = ones_where(hit0 & match)
    sel_ref[1] = ones_where(hit1 & match)
    ei = iota((tok, experts), 1)
    pick = (jnp.where(ei == r0, 1.0, 0.0) - jnp.where(ei == r1, 1.0, 0.0)).astype(BF)
    near = pl.ds(pl.multiple_of(tp * half, half), half)
    q_ref[...] = nt(pick, rex_ref[near, :])
    h = None
    for j in range(groups):
        side = jnp.where(r0 // gw == j, 1.0, 0.0) - aux_ref[:, 2 + j : 3 + j]
        term = side * rg_ref[pl.ds(j, 1), near].astype(F32)
        h = term if j == 0 else h + term
    h_ref[...] = h


def final_kernel(
    back_ref, sel_ref, aux_ref, q_ref, h_ref, sq_ref, sqo_ref,
    tg_ref, rex_ref, rg_ref, rows_ref, gate_sq_ref, up_sq_ref,
):
    gate_sq_ref[...] = sq_ref[0:1, :] + sqo_ref[0:1, :]
    up_sq_ref[...] = sq_ref[1:2, :] + sqo_ref[1:2, :]
    half = tg_ref.shape[1]
    width = half // 2
    experts = rex_ref.shape[1]
    groups = rg_ref.shape[0]
    gw = experts // groups
    slots = experts * 4
    extra3 = back_ref[:, :, half:]
    extra = extra3.reshape(slots, EXTRA)
    u0 = mm(sel_ref[0], extra)[:, U_LANE : U_LANE + 1]
    u1 = mm(sel_ref[1], extra)[:, U_LANE : U_LANE + 1]
    lean = aux_ref[:, 1:2] * u0 - aux_ref[:, 0:1] * u1
    both = u0 + u1
    sel = (sel_ref[0].astype(F32) + sel_ref[1].astype(F32)).astype(BF)
    for c in range(2):
        cols = slice(c * width, (c + 1) * width)
        part = mm(sel, back_ref[:, :, cols].reshape(slots, width))
        tg_ref[:, cols] = (part + (both * h_ref[:, cols] + lean * q_ref[:, cols])).astype(BF)
    sums = jnp.sum(extra3.astype(F32).reshape(groups, gw, 4, EXTRA), axis=1)
    rg = None
    square = None
    lane = iota((8, EXTRA), 1)
    for g in range(groups):
        s = sums[g]
        s = jnp.concatenate([s, jnp.concatenate([s[:, LOW_LANE:], s[:, 0:LOW_LANE]], axis=1)], axis=0)
        rex = s[:, 0:gw]
        rex_ref[:, g * gw : (g + 1) * gw] = rex
        rg = s if g == 0 else rg + s
        sq = jnp.sum(rex * rex, axis=1, keepdims=True)
        square = sq if g == 0 else square + sq
    grp = rg[:, GROUP_LANE : GROUP_LANE + groups]
    square = square + jnp.sum(grp * grp, axis=1, keepdims=True)
    rest = jnp.transpose(jnp.where(lane == GROUP_LANE + groups, square, rg))
    rg_ref[...] = rest[GROUP_LANE : GROUP_LANE + groups, :]
    rows_ref[...] = rest[GROUP_LANE + groups : GROUP_LANE + groups + 1, :]


def body(tokens, cotangent, routes, router_group, router_expert, gate_proj, up_proj, down_proj):
    tok, dm = tokens.shape
    experts = router_expert.shape[1]
    groups = router_group.shape[1]
    half = dm // 2
    ff = gate_proj.shape[2]
    n = experts * 2
    tp = lax.axis_index("tp").reshape(1)
    swap = [(0, 1), (1, 0)]
    rgt = router_group.T
    ep = lax.axis_index("ep")
    planes = experts // 16
    idx = [ep.reshape(1), tp]
    gate, up, down = gate_proj[0], up_proj[0], down_proj[0]

    def exchange(x):
        return lax.all_to_all(x, "ep", split_axis=0, concat_axis=0, tiled=True)

    def partner(x):
        return lax.ppermute(x, "tp", swap)

    def shift(v, stride, d):
        size = planes if stride == 16 else 4
        pairs = []
        for e in range(experts):
            at = e // stride % size
            pairs.append((e, e + ((at + d) % size - at) * stride))
        return lax.ppermute(v, "ep", pairs)

    send, aux = call(
        pre_kernel, 1 << 30, 20,
        [((experts, 2, 2 * dm), BF), ((EXTRA, tok), F32)],
        idx, [far(routes.T), far(rgt), far(tokens), far(cotangent), far(router_expert)],
        scratch=[
            pltpu.VMEM((experts, 2, 2 * dm), BF),
            pltpu.VMEM((2, tok), jnp.int32), pltpu.VMEM((groups, dm), BF),
            pltpu.VMEM((tok, dm), BF), pltpu.VMEM((tok, dm), BF), pltpu.VMEM((dm, experts), BF),
            pltpu.VMEM((n, tok), BF), pltpu.SemaphoreType.DMA((13,)),
        ],
        spaces=[HB] * 5,
        out_spaces=[HB, VM],
    )
    got = exchange(send)
    sides = call(
        functools.partial(side_x_kernel, groups), 1 << 28, 6,
        [((experts // 4, EXTRA), BF)] * 4, idx[:1], [aux],
    )
    sides = [shift(v, 1, d) if d else v for d, v in enumerate(sides)]
    sides = call(side_y_kernel, 1 << 24, 6, [((experts // 4, EXTRA), BF)] * 4, idx[:1], sides)
    sides = [shift(v, 4, d) if d else v for d, v in enumerate(sides)]
    sides = call(side_z_kernel, 1 << 24, 6, [((16, EXTRA), BF)] * planes, idx[:1], sides)
    sides = [shift(v, 16, d) if d else v for d, v in enumerate(sides)]
    (aux_cols,) = call(mark_kernel, 1 << 20, 4, [((tok, EXTRA), F32)], [], [aux])
    z = call(functools.partial(side_end_kernel, groups), 1 << 24, 6, [((n, EXTRA), BF)] * 2, idx, sides)
    other = partner(got)

    def expert(g, weights, load, saved):
        shared = [((n, EXTRA), F32), ((n, half), BF), ((n, half + EXTRA), BF), ((n, dm), BF)]
        deltas = [((n, ff), BF)] * 3
        if load:
            outs = shared + [((n, dm), BF)] + deltas + [((dm, ff), BF), ((dm, ff), BF), ((ff, dm), BF)]
            places = [VM] * 5 + [HB] * 3 + [VM] * 3
        else:
            outs = shared + deltas + [((n, dm), BF)] * 4
            places = [VM] * 4 + [HB] * 7
        return call(
            functools.partial(expert_kernel, load), 3 << 30, 18, outs, [tp], [g, *weights, *saved],
            scratch=[pltpu.VMEM((n, w), BF) for w in ((ff, ff, ff) if load else (dm, ff, ff, ff))]
            + [pltpu.SemaphoreType.DMA((9,))],
            spaces=[VM] + [HB if load else VM] * 3 + [VM] * len(saved),
            out_spaces=places,
        )

    u0, mine0, theirs0, x0, sc0, gd0, ud0, hid0, *held = expert(got, [far(gate), far(up), far(down)], True, [])
    u1, mine1, theirs1, x1, gd1, ud1, hid1, *stored = expert(other, held, False, [x0, sc0])
    u, mine, theirs, xv = [u0, u1], [mine0, mine1], [theirs0, theirs1], [x0, x1]
    gd, ud, hid = [gd0, gd1], [ud0, ud1], [hid0, hid1]
    x, sc = [stored[0], stored[2]], [stored[1], stored[3]]
    came = [partner(theirs[1]), partner(theirs[0])]
    rc1, ul1 = call(
        early_kernel, 1 << 28, 8, [((experts, 4, EXTRA), F32), ((n, EXTRA), F32)],
        [tp], [came[1], u[1], z[1], xv[1]], scratch=[pltpu.VMEM((n, EXTRA), BF)],
    )
    (ret,) = call(
        pack_kernel, 1 << 29, 16, [((experts, 4, half + EXTRA), BF)],
        [tp], [*mine, *came, u[0], z[0], xv[0], rc1, ul1],
        scratch=[
            pltpu.VMEM((experts, 4, half + EXTRA), BF), pltpu.VMEM((n, EXTRA), BF), pltpu.VMEM((n, EXTRA), F32),
            pltpu.SemaphoreType.DMA((4,)),
        ],
        out_spaces=[HB],
    )
    back = exchange(ret)
    gate_grad, up_grad, down_grad, sq, down_sq = call(
        grads_kernel, 3 << 30, 20,
        [((dm, ff), BF), ((dm, ff), BF), ((ff, dm), BF), ((2, dm), F32), ((1, ff), F32)],
        [], [*x, *sc, *gd, *ud, *hid], scratch=[pltpu.VMEM((ff, 128), F32)],
    )
    sq_other = partner(sq)
    sel, q, h = call(
        home_kernel, 1 << 29, 8,
        [((2, tok, experts * 4), BF), ((tok, half), F32), ((tok, half), F32)],
        [tp], [aux_cols, rgt, router_expert],
    )
    token_grad, rex_grad, rg_grad, rows, gate_sq, up_sq = call(
        final_kernel, 1 << 29, 10,
        [((tok, half), BF), ((8, experts), F32), ((groups, 8), F32), ((1, 8), F32),
         ((1, dm), F32), ((1, dm), F32)],
        [], [back, sel, aux_cols, q, h, sq, sq_other],
    )
    return (
        token_grad,
        gate_grad[None],
        up_grad[None],
        down_grad[None],
        gate_sq,
        up_sq,
        down_sq,
        rex_grad,
        rg_grad.T,
        rows[0],
    )


def solution(mesh):
    return jax.shard_map(
        body,
        mesh=mesh,
        in_specs=(
            P("ep", None),
            P("ep", None),
            P("ep", None),
            P(),
            P(),
            P("ep", None, "tp"),
            P("ep", None, "tp"),
            P("ep", "tp", None),
        ),
        out_specs=(
            P("ep", "tp"),
            P("ep", None, "tp"),
            P("ep", None, "tp"),
            P("ep", "tp", None),
            P("ep", None),
            P("ep", None),
            P("ep", "tp"),
            P(("ep", "tp"), None),
            P(("ep", "tp"), None),
            P(("ep", "tp")),
        ),
        check_vma=False,
    )
```

```python
import functools

import jax
import jax.numpy as jnp
from jax import lax
from jax.experimental import pallas as pl
from jax.experimental.pallas import tpu as pltpu
from jax.sharding import PartitionSpec as P


BF = jnp.bfloat16
F32 = jnp.float32
GROUP_LANE = 32
U_LANE = 40
LOW_LANE = 64
EXTRA = 128


def mm(a, b):
    return lax.dot_general(a, b, (((1,), (0,)), ((), ())), preferred_element_type=F32)


def nt(a, b):
    return lax.dot_general(a, b, (((1,), (1,)), ((), ())), preferred_element_type=F32)


def tn(a, b):
    return lax.dot_general(a, b, (((0,), (0,)), ((), ())), preferred_element_type=F32)


def iota(shape, dim):
    return lax.broadcasted_iota(jnp.int32, shape, dim)


VM = pl.BlockSpec(memory_space=pltpu.VMEM)
HB = pl.BlockSpec(memory_space=pltpu.HBM)


def far(x):
    return pltpu.with_memory_space_constraint(x, pltpu.HBM)


def call(kernel, flops, limit, outs, scalars, arrays, scratch=(), spaces=None, out_spaces=None):
    smem = pl.BlockSpec(memory_space=pltpu.SMEM)
    vmem = pl.BlockSpec(memory_space=pltpu.VMEM)
    return pl.pallas_call(
        kernel,
        out_shape=[
            pltpu.HBM(shape, dtype) if out_spaces and out_spaces[k] is HB else jax.ShapeDtypeStruct(shape, dtype)
            for k, (shape, dtype) in enumerate(outs)
        ],
        in_specs=[smem] * len(scalars) + (spaces or [vmem] * len(arrays)),
        out_specs=out_spaces or [vmem] * len(outs),
        scratch_shapes=list(scratch),
        cost_estimate=pl.CostEstimate(flops=flops, bytes_accessed=4 << 20, transcendentals=0),
        compiler_params=pltpu.CompilerParams(vmem_limit_bytes=limit << 20),
    )(*scalars, *arrays)


def ones_where(mask):
    return jnp.where(mask, 1.0, 0.0).astype(BF)


def pre_kernel(
    ep_ref, tp_ref, rt_hbm, rgt_hbm, tok_hbm, cot_hbm, rex_hbm,
    send_out, aux_ref, send_ref, rt_ref, rgt_ref, tok_ref, cot_ref, rex_ref, one_ref, sems,
):
    tp = tp_ref[0]
    tok, dm = tok_ref.shape
    experts = rex_ref.shape[1]
    groups = rgt_ref.shape[0]
    gw = experts // groups
    width = dm // 4
    loads = [
        pltpu.make_async_copy(src, dst, sems.at[k])
        for k, (src, dst) in enumerate(
            ((rt_hbm, rt_ref), (tok_hbm, tok_ref), (rgt_hbm, rgt_ref), (rex_hbm, rex_ref), (cot_hbm, cot_ref))
        )
    ]
    for load in loads:
        load.start()
    loads[0].wait()
    r0, r1 = rt_ref[0:1, :], rt_ref[1:2, :]
    before = ones_where(iota((tok, tok), 0) < iota((tok, tok), 1))
    n = experts * 2
    row = iota((n, tok), 0)
    hit0 = r0 == (row >> 1)
    hit1 = r1 == (row >> 1)
    match = mm(ones_where(hit0 | hit1), before) == (2 * tp + (row & 1)).astype(F32)
    one0 = jnp.where(hit0 & match, 1.0, 0.0)
    one1 = jnp.where(hit1 & match, 1.0, 0.0)
    one_ref[...] = (one0 + one1).astype(BF)
    saves = []

    def place(k, first, rows):
        cols = pl.ds(first + k * width, width)
        send_ref[:, :, cols] = rows.astype(BF).reshape(experts, 2, width)
        saves.append(pltpu.make_async_copy(send_ref.at[:, :, cols], send_out.at[:, :, cols], sems.at[5 + len(saves)]))
        saves[-1].start()

    loads[1].wait()
    for c in range(4):
        place(c, 0, mm(one_ref[...], tok_ref[:, c * width : (c + 1) * width]))
    loads[2].wait()
    loads[3].wait()
    group_exp = jnp.exp(nt(rgt_ref[...], tok_ref[...]))
    group_prob = group_exp / jnp.sum(group_exp, axis=0, keepdims=True)
    logits = jnp.transpose(mm(tok_ref[...], rex_ref[...]))
    ei = iota((experts, tok), 0)
    l0 = jnp.sum(jnp.where(ei == r0, logits, 0.0), axis=0, keepdims=True)
    l1 = jnp.sum(jnp.where(ei == r1, logits, 0.0), axis=0, keepdims=True)
    x0, x1 = jnp.exp(l0), jnp.exp(l1)
    p0, p1 = x0 / (x0 + x1), x1 / (x0 + x1)
    chosen = r0 // gw
    gi = iota((groups, tok), 0)
    picked = jnp.sum(jnp.where(gi == chosen, group_prob, 0.0), axis=0, keepdims=True)
    w0 = (picked * p0).astype(BF).astype(F32)
    w1 = (picked * p1).astype(BF).astype(F32)
    arow = iota((EXTRA, tok), 0)
    aux = jnp.where(arow == 0, p0, jnp.where(arow == 1, p1, 0.0))
    for j in range(groups):
        aux = jnp.where(arow == 2 + j, group_prob[j : j + 1, :], aux)
    aux = jnp.where(arow == 6, r0.astype(F32), jnp.where(arow == 7, r1.astype(F32), aux))
    aux_ref[...] = aux
    loads[4].wait()
    scale = jnp.sum(one0 * w0 + one1 * w1, axis=1, keepdims=True)
    for c in range(4):
        place(c, dm, mm(one_ref[...], cot_ref[:, c * width : (c + 1) * width]) * scale)
    for copy in saves:
        copy.wait()


def pick_rows(outs, rows_in, stride, at):
    n = rows_in.shape[0] // stride
    for d, out_ref in enumerate(outs):
        want = iota((n, n * stride), 0) * stride + ((at + d) & (stride - 1))
        out_ref[...] = mm(ones_where(iota((n, n * stride), 1) == want), rows_in).astype(BF)


def mark_kernel(aux_ref, out_ref):
    out_ref[...] = jnp.transpose(aux_ref[...])


def side_x_kernel(groups, ep_ref, aux_ref, *outs):
    tok = aux_ref.shape[1]
    experts = outs[0].shape[0] * 4
    gw = experts // groups
    r0, r1 = aux_ref[6:7, :].astype(jnp.int32), aux_ref[7:8, :].astype(jnp.int32)
    ei = iota((experts, tok), 0)
    one0 = jnp.where(ei == r0, 1.0, 0.0)
    one1 = jnp.where(ei == r1, 1.0, 0.0)
    before = ones_where(iota((tok, tok), 0) < iota((tok, tok), 1))
    rank = mm((one0 + one1).astype(BF), before)
    li = iota((EXTRA, tok), 0)
    base = (r0 // gw) * gw
    shared = jnp.zeros((EXTRA, tok), F32)
    for j in range(groups):
        shared = jnp.where((li & 7) == 2 + j, aux_ref[2 + j : 3 + j, :], shared)
    kinds = []
    for other, prob in ((r1, aux_ref[1:2, :]), (r0, aux_ref[0:1, :])):
        kinds.append(
            jnp.where((li & 7) == 0, (other - base).astype(F32), jnp.where((li & 7) == 1, prob, shared))
        )
    total = None
    for r in range(4):
        for one, kind in ((one0, kinds[0]), (one1, kinds[1])):
            left = jnp.where(rank == float(r), one, 0.0).astype(BF)
            right = jnp.where((li >> 3) == r, kind, 0.0).astype(BF)
            term = nt(left, right)
            total = term if total is None else total + term
    pick_rows(outs, total.astype(BF), 4, ep_ref[0] & 3)


def side_y_kernel(ep_ref, a_ref, b_ref, c_ref, d_ref, *outs):
    rows = jnp.concatenate([a_ref[...], b_ref[...], c_ref[...], d_ref[...]], axis=0)
    pick_rows(outs, rows, 4, (ep_ref[0] >> 2) & 3)


def side_z_kernel(ep_ref, a_ref, b_ref, c_ref, d_ref, *outs):
    rows = jnp.concatenate([a_ref[...], b_ref[...], c_ref[...], d_ref[...]], axis=0)
    pick_rows(outs, rows, len(outs), ep_ref[0] >> 4)


def side_end_kernel(groups, ep_ref, tp_ref, *refs):
    ins, outs = refs[:-2], refs[-2:]
    rows = jnp.concatenate([ref[...] for ref in ins], axis=0)
    experts = rows.shape[0]
    planes = len(ins)
    gw = experts // groups
    e, tp = ep_ref[0], tp_ref[0]
    n = experts * 2
    src = iota((n, experts), 0) >> 1
    dz = ((e >> 4) - (src >> 4)) & (planes - 1)
    dy = ((e >> 2) - (src >> 2)) & 3
    dx = (e - src) & 3
    spread = mm(ones_where(iota((n, experts), 1) == dz * 16 + dy * 4 + dx), rows)
    lane = iota((n, EXTRA), 1)
    li = lane & (LOW_LANE - 1)
    chosen = e // gw
    own = jnp.where(li == e - chosen * gw, 1.0, 0.0)
    mark = jnp.where(li == GROUP_LANE + chosen, 1.0, 0.0)
    for p, out_ref in enumerate(outs):
        slot = 2 * ((tp + p) & 1) + (iota((n, EXTRA), 0) & 1)

        def value(v):
            return jnp.sum(jnp.where(lane == slot * 8 + v, spread, 0.0), axis=1, keepdims=True)

        z = value(1) * (own - jnp.where(li.astype(F32) == value(0), 1.0, 0.0)) + mark
        for j in range(groups):
            z = z - jnp.where(li == GROUP_LANE + j, value(2 + j), 0.0)
        out_ref[...] = z.astype(BF)


def expert_kernel(load, tp_ref, got_ref, *refs):
    tp = tp_ref[0]
    weights, refs = refs[:3], refs[3:]
    if load:
        gate_ref, up_ref, down_ref = refs[8:11]
        u_ref, mine_ref, theirs_ref, x_ref, sc_ref, gd_out, ud_out, hid_out = refs[:8]
        gd_ref, ud_ref, hid_ref, sems = refs[11:]
        loads = [
            pltpu.make_async_copy(src, dst, sems.at[3 + k])
            for k, (src, dst) in enumerate(zip(weights, (gate_ref, up_ref, down_ref)))
        ]
        for copy in loads:
            copy.start()
        pairs = []
    else:
        gate_ref, up_ref, down_ref = weights
        x0_ref, sc0_ref = refs[:2]
        u_ref, mine_ref, theirs_ref, x_ref, gd_out, ud_out, hid_out, x0_out, sc0_out, x_out, sc_out = refs[2:13]
        sc_ref, gd_ref, ud_ref, hid_ref, sems = refs[13:]
        pairs = [(x0_ref, x0_out), (sc0_ref, sc0_out), (x_ref, x_out), (sc_ref, sc_out)]
    pairs = [(gd_ref, gd_out), (ud_ref, ud_out), (hid_ref, hid_out)] + pairs
    base = 6 if load else 0
    saves = [pltpu.make_async_copy(src, dst, sems.at[base + k]) for k, (src, dst) in enumerate(pairs)]
    dm = gate_ref.shape[0]
    half = dm // 2
    if not load:
        saves[3].start()
        saves[4].start()
    x_ref[...] = got_ref[:, :, 0:dm].reshape(x_ref.shape)
    sc_ref[...] = got_ref[:, :, dm:].reshape(sc_ref.shape)
    if load:
        loads[0].wait()
    else:
        saves[5].start()
        saves[6].start()
    gp = mm(x_ref[...], gate_ref[...])
    if load:
        loads[1].wait()
    upre = mm(x_ref[...], up_ref[...])
    if load:
        loads[2].wait()
    pulled = nt(sc_ref[...], down_ref[...])
    sig = 1.0 / (1.0 + jnp.exp(-gp))
    act = gp * sig
    hid = (act * upre).astype(BF)
    hid_ref[...] = hid
    u = jnp.sum(pulled * hid.astype(F32), axis=1, keepdims=True)
    gd = (pulled * (upre * sig * (1.0 + gp * (1.0 - sig)))).astype(BF)
    ud = (pulled * act).astype(BF)
    gd_ref[...] = gd
    ud_ref[...] = ud
    for save in saves[:3]:
        save.start()
    n = x_ref.shape[0]
    u_ref[...] = jnp.broadcast_to(u, (n, EXTRA))
    high = u.astype(BF).astype(F32)
    lane = iota((n, EXTRA), 1)
    theirs_ref[:, half:] = jnp.where(lane == 0, high, jnp.where(lane == 1, u - high, 0.0)).astype(BF)
    far = pl.ds(pl.multiple_of((1 - tp) * half, half), half)
    theirs_ref[:, 0:half] = (nt(gd, gate_ref[far, :]) + nt(ud, up_ref[far, :])).astype(BF)
    near = pl.ds(pl.multiple_of(tp * half, half), half)
    mine_ref[...] = (nt(gd, gate_ref[near, :]) + nt(ud, up_ref[near, :])).astype(BF)
    for save in saves:
        save.wait()


def summed(u_ref, came_ref):
    half = came_ref.shape[1] - EXTRA
    return u_ref[...] + came_ref[:, half : half + 1].astype(F32) + came_ref[:, half + 1 : half + 2].astype(F32)


def router_terms(tp, x_ref, y_ref, b, bs):
    cols = slice(b * 16 * bs, (b + 1) * 16 * bs)
    rc = tn(x_ref[:, cols], y_ref[...]).reshape(bs, 16, EXTRA)
    rc = jnp.where(tp == 0, rc[:, 0:8, :], rc[:, 8:16, :])
    return jnp.where(iota((bs, 4, EXTRA), 2) < LOW_LANE, rc[:, 0:4, :], rc[:, 4:8, :])


def early_kernel(tp_ref, came_ref, u_ref, z_ref, x_ref, rc_ref, ul_ref, y_ref):
    tp = tp_ref[0]
    n = u_ref.shape[0]
    u = summed(u_ref, came_ref)
    y_ref[...] = (u * z_ref[...].astype(F32)).astype(BF)
    ul_ref[...] = jnp.where(iota((n, EXTRA), 1) == U_LANE, u, 0.0)
    bs = min(32, n // 2)
    for b in range(n // (2 * bs)):
        rc_ref[b * bs : (b + 1) * bs] = router_terms(tp, x_ref, y_ref, b, bs)


def pack_kernel(tp_ref, *refs):
    tp = tp_ref[0]
    mine, came = refs[0:2], refs[2:4]
    u_ref, z_ref, x_ref, rc1_ref, ul1_ref, ret_out, ret_ref, y_ref, ul_ref, sems = refs[4:14]
    saves = []
    n, half = mine[0].shape
    u = summed(u_ref, came[0])
    y_ref[...] = (u * z_ref[...].astype(F32)).astype(BF)
    ul_ref[...] = jnp.where(iota((n, EXTRA), 1) == U_LANE, u, 0.0)
    bs = min(32, n // 2)
    for b in range(n // (2 * bs)):
        rows = slice(b * 2 * bs, (b + 1) * 2 * bs)
        out = slice(b * bs, (b + 1) * bs)
        rc = router_terms(tp, x_ref, y_ref, b, bs) + rc1_ref[out]
        for p, lanes in ((0, ul_ref), (1, ul1_ref)):
            total = (mine[p][rows, :].astype(F32) + came[p][rows, 0:half].astype(F32)).astype(BF)
            at = slice(2 * p, 2 * p + 2)
            ret_ref[out, at, 0:half] = total.reshape(bs, 2, half)
            ret_ref[out, at, half:] = (rc[:, at, :] + lanes[rows, :].reshape(bs, 2, EXTRA)).astype(BF)
        saves.append(pltpu.make_async_copy(ret_ref.at[out], ret_out.at[out], sems.at[b]))
        saves[-1].start()
    for save in saves:
        save.wait()


def grads_kernel(*refs):
    x, sc, gd, ud, hid = (refs[2 * k : 2 * k + 2] for k in range(5))
    gate_ref, up_ref, down_ref, sq_ref, down_sq_ref, acc_ref = refs[10:]
    dm, _ = gate_ref.shape
    blk = 128
    wide = 512 if dm % 512 == 0 else 128

    def as_row(col):
        return jnp.transpose(jnp.broadcast_to(col, (col.shape[0], 128)))[0:1, :]

    def step(b, carry):
        cols = pl.ds(pl.multiple_of(b * blk, blk), blk)
        for k, (delta, out_ref) in enumerate(((gd, gate_ref), (ud, up_ref))):
            full = tn(x[0][:, cols], delta[0][...]) + tn(x[1][:, cols], delta[1][...])
            out_ref[cols, :] = full.astype(BF)
            sq_ref[k : k + 1, cols] = as_row(jnp.sum(full * full, axis=1, keepdims=True))
        return carry

    lax.fori_loop(0, dm // blk, step, 0)
    acc_ref[...] = jnp.zeros_like(acc_ref)

    def down_step(b, carry):
        cols = pl.ds(pl.multiple_of(b * wide, wide), wide)
        full = tn(hid[0][...], sc[0][:, cols]) + tn(hid[1][...], sc[1][:, cols])
        down_ref[:, cols] = full.astype(BF)
        acc_ref[...] += jnp.broadcast_to(jnp.sum(full * full, axis=1, keepdims=True), acc_ref.shape)
        return carry

    lax.fori_loop(0, dm // wide, down_step, 0)
    down_sq_ref[...] = jnp.transpose(acc_ref[...])[0:1, :]


def home_kernel(tp_ref, aux_ref, rg_ref, rex_ref, sel_ref, q_ref, h_ref):
    tp = tp_ref[0]
    tok = aux_ref.shape[0]
    half = q_ref.shape[1]
    groups = rg_ref.shape[0]
    experts = rex_ref.shape[1]
    gw = experts // groups
    r0, r1 = aux_ref[:, 6:7].astype(jnp.int32), aux_ref[:, 7:8].astype(jnp.int32)
    n = experts * 4
    col = iota((tok, n), 1)
    hit0 = r0 == (col >> 2)
    hit1 = r1 == (col >> 2)
    earlier = ones_where(iota((tok, tok), 1) < iota((tok, tok), 0))
    rank = mm(earlier, ones_where(hit0 | hit1))
    match = rank == ((2 * tp + (col & 3)) & 3).astype(F32)
    sel_ref[0] = ones_where(hit0 & match)
    sel_ref[1] = ones_where(hit1 & match)
    ei = iota((tok, experts), 1)
    pick = (jnp.where(ei == r0, 1.0, 0.0) - jnp.where(ei == r1, 1.0, 0.0)).astype(BF)
    near = pl.ds(pl.multiple_of(tp * half, half), half)
    q_ref[...] = nt(pick, rex_ref[near, :])
    h = None
    for j in range(groups):
        side = jnp.where(r0 // gw == j, 1.0, 0.0) - aux_ref[:, 2 + j : 3 + j]
        term = side * rg_ref[pl.ds(j, 1), near].astype(F32)
        h = term if j == 0 else h + term
    h_ref[...] = h


def final_kernel(
    back_ref, sel_ref, aux_ref, q_ref, h_ref, sq_ref, sqo_ref,
    tg_ref, rex_ref, rg_ref, rows_ref, gate_sq_ref, up_sq_ref,
):
    gate_sq_ref[...] = sq_ref[0:1, :] + sqo_ref[0:1, :]
    up_sq_ref[...] = sq_ref[1:2, :] + sqo_ref[1:2, :]
    half = tg_ref.shape[1]
    width = half // 2
    experts = rex_ref.shape[1]
    groups = rg_ref.shape[0]
    gw = experts // groups
    slots = experts * 4
    extra3 = back_ref[:, :, half:]
    extra = extra3.reshape(slots, EXTRA)
    u0 = mm(sel_ref[0], extra)[:, U_LANE : U_LANE + 1]
    u1 = mm(sel_ref[1], extra)[:, U_LANE : U_LANE + 1]
    lean = aux_ref[:, 1:2] * u0 - aux_ref[:, 0:1] * u1
    both = u0 + u1
    sel = (sel_ref[0].astype(F32) + sel_ref[1].astype(F32)).astype(BF)
    for c in range(2):
        cols = slice(c * width, (c + 1) * width)
        part = mm(sel, back_ref[:, :, cols].reshape(slots, width))
        tg_ref[:, cols] = (part + (both * h_ref[:, cols] + lean * q_ref[:, cols])).astype(BF)
    sums = jnp.sum(extra3.astype(F32).reshape(groups, gw, 4, EXTRA), axis=1)
    rg = None
    square = None
    lane = iota((8, EXTRA), 1)
    for g in range(groups):
        s = sums[g]
        s = jnp.concatenate([s, jnp.concatenate([s[:, LOW_LANE:], s[:, 0:LOW_LANE]], axis=1)], axis=0)
        rex = s[:, 0:gw]
        rex_ref[:, g * gw : (g + 1) * gw] = rex
        rg = s if g == 0 else rg + s
        sq = jnp.sum(rex * rex, axis=1, keepdims=True)
        square = sq if g == 0 else square + sq
    grp = rg[:, GROUP_LANE : GROUP_LANE + groups]
    square = square + jnp.sum(grp * grp, axis=1, keepdims=True)
    rest = jnp.transpose(jnp.where(lane == GROUP_LANE + groups, square, rg))
    rg_ref[...] = rest[GROUP_LANE : GROUP_LANE + groups, :]
    rows_ref[...] = rest[GROUP_LANE + groups : GROUP_LANE + groups + 1, :]


def body(tokens, cotangent, routes, router_group, router_expert, gate_proj, up_proj, down_proj):
    tok, dm = tokens.shape
    experts = router_expert.shape[1]
    groups = router_group.shape[1]
    half = dm // 2
    ff = gate_proj.shape[2]
    n = experts * 2
    tp = lax.axis_index("tp").reshape(1)
    swap = [(0, 1), (1, 0)]
    rgt = router_group.T
    ep = lax.axis_index("ep")
    planes = experts // 16
    idx = [ep.reshape(1), tp]
    gate, up, down = gate_proj[0], up_proj[0], down_proj[0]

    def exchange(x):
        return lax.all_to_all(x, "ep", split_axis=0, concat_axis=0, tiled=True)

    def partner(x):
        return lax.ppermute(x, "tp", swap)

    def shift(v, stride, d):
        size = planes if stride == 16 else 4
        pairs = []
        for e in range(experts):
            at = e // stride % size
            pairs.append((e, e + ((at + d) % size - at) * stride))
        return lax.ppermute(v, "ep", pairs)

    send, aux = call(
        pre_kernel, 1 << 30, 20,
        [((experts, 2, 2 * dm), BF), ((EXTRA, tok), F32)],
        idx, [far(routes.T), far(rgt), far(tokens), far(cotangent), far(router_expert)],
        scratch=[
            pltpu.VMEM((experts, 2, 2 * dm), BF),
            pltpu.VMEM((2, tok), jnp.int32), pltpu.VMEM((groups, dm), BF),
            pltpu.VMEM((tok, dm), BF), pltpu.VMEM((tok, dm), BF), pltpu.VMEM((dm, experts), BF),
            pltpu.VMEM((n, tok), BF), pltpu.SemaphoreType.DMA((13,)),
        ],
        spaces=[HB] * 5,
        out_spaces=[HB, VM],
    )
    got = exchange(send)
    sides = call(
        functools.partial(side_x_kernel, groups), 1 << 28, 6,
        [((experts // 4, EXTRA), BF)] * 4, idx[:1], [aux],
    )
    sides = [shift(v, 1, d) if d else v for d, v in enumerate(sides)]
    sides = call(side_y_kernel, 1 << 24, 6, [((experts // 4, EXTRA), BF)] * 4, idx[:1], sides)
    sides = [shift(v, 4, d) if d else v for d, v in enumerate(sides)]
    sides = call(side_z_kernel, 1 << 24, 6, [((16, EXTRA), BF)] * planes, idx[:1], sides)
    sides = [shift(v, 16, d) if d else v for d, v in enumerate(sides)]
    (aux_cols,) = call(mark_kernel, 1 << 20, 4, [((tok, EXTRA), F32)], [], [aux])
    z = call(functools.partial(side_end_kernel, groups), 1 << 24, 6, [((n, EXTRA), BF)] * 2, idx, sides)
    other = partner(got)

    def expert(g, weights, load, saved):
        shared = [((n, EXTRA), F32), ((n, half), BF), ((n, half + EXTRA), BF), ((n, dm), BF)]
        deltas = [((n, ff), BF)] * 3
        if load:
            outs = shared + [((n, dm), BF)] + deltas + [((dm, ff), BF), ((dm, ff), BF), ((ff, dm), BF)]
            places = [VM] * 5 + [HB] * 3 + [VM] * 3
        else:
            outs = shared + deltas + [((n, dm), BF)] * 4
            places = [VM] * 4 + [HB] * 7
        return call(
            functools.partial(expert_kernel, load), 3 << 30, 18, outs, [tp], [g, *weights, *saved],
            scratch=[pltpu.VMEM((n, w), BF) for w in ((ff, ff, ff) if load else (dm, ff, ff, ff))]
            + [pltpu.SemaphoreType.DMA((9,))],
            spaces=[VM] + [HB if load else VM] * 3 + [VM] * len(saved),
            out_spaces=places,
        )

    u0, mine0, theirs0, x0, sc0, gd0, ud0, hid0, *held = expert(got, [far(gate), far(up), far(down)], True, [])
    u1, mine1, theirs1, x1, gd1, ud1, hid1, *stored = expert(other, held, False, [x0, sc0])
    u, mine, theirs, xv = [u0, u1], [mine0, mine1], [theirs0, theirs1], [x0, x1]
    gd, ud, hid = [gd0, gd1], [ud0, ud1], [hid0, hid1]
    x, sc = [stored[0], stored[2]], [stored[1], stored[3]]
    came = [partner(theirs[1]), partner(theirs[0])]
    rc1, ul1 = call(
        early_kernel, 1 << 28, 8, [((experts, 4, EXTRA), F32), ((n, EXTRA), F32)],
        [tp], [came[1], u[1], z[1], xv[1]], scratch=[pltpu.VMEM((n, EXTRA), BF)],
    )
    (ret,) = call(
        pack_kernel, 1 << 29, 16, [((experts, 4, half + EXTRA), BF)],
        [tp], [*mine, *came, u[0], z[0], xv[0], rc1, ul1],
        scratch=[
            pltpu.VMEM((experts, 4, half + EXTRA), BF), pltpu.VMEM((n, EXTRA), BF), pltpu.VMEM((n, EXTRA), F32),
            pltpu.SemaphoreType.DMA((4,)),
        ],
        out_spaces=[HB],
    )
    back = exchange(ret)
    gate_grad, up_grad, down_grad, sq, down_sq = call(
        grads_kernel, 3 << 30, 20,
        [((dm, ff), BF), ((dm, ff), BF), ((ff, dm), BF), ((2, dm), F32), ((1, ff), F32)],
        [], [*x, *sc, *gd, *ud, *hid], scratch=[pltpu.VMEM((ff, 128), F32)],
    )
    sq_other = partner(sq)
    sel, q, h = call(
        home_kernel, 1 << 29, 8,
        [((2, tok, experts * 4), BF), ((tok, half), F32), ((tok, half), F32)],
        [tp], [aux_cols, rgt, router_expert],
    )
    token_grad, rex_grad, rg_grad, rows, gate_sq, up_sq = call(
        final_kernel, 1 << 29, 10,
        [((tok, half), BF), ((8, experts), F32), ((groups, 8), F32), ((1, 8), F32),
         ((1, dm), F32), ((1, dm), F32)],
        [], [back, sel, aux_cols, q, h, sq, sq_other],
    )
    return (
        token_grad,
        gate_grad[None],
        up_grad[None],
        down_grad[None],
        gate_sq,
        up_sq,
        down_sq,
        rex_grad,
        rg_grad.T,
        rows[0],
    )


def solution(mesh):
    return jax.shard_map(
        body,
        mesh=mesh,
        in_specs=(
            P("ep", None),
            P("ep", None),
            P("ep", None),
            P(),
            P(),
            P("ep", None, "tp"),
            P("ep", None, "tp"),
            P("ep", "tp", None),
        ),
        out_specs=(
            P("ep", "tp"),
            P("ep", None, "tp"),
            P("ep", None, "tp"),
            P("ep", "tp", None),
            P("ep", None),
            P("ep", None),
            P("ep", "tp"),
            P(("ep", "tp"), None),
            P(("ep", "tp"), None),
            P(("ep", "tp")),
        ),
        check_vma=False,
    )
```
